128 devices in a mesh: ep: 64 (over z, y, x), tp: 2 (over core).
Axes of the slice: x: 4, y: 4, z: 4, core: 2. Of those that a mesh axis runs over, the one named last changes fastest.
Arguments:
- tokens: bfloat16 [1024, 2048], P('ep'), may hold values from -6 to 6
- norm_gain: float32 [2048], replicated, may hold values from 0.1 to 1.9
- query_weight: bfloat16 [2048, 1024], P('ep', 'tp'), may hold values from -0.125 to 0.125
- key_weight: bfloat16 [2048, 1024], P('ep', 'tp'), may hold values from -0.125 to 0.125
- value_weight: bfloat16 [2048, 1024], P('ep', 'tp'), may hold values from -0.125 to 0.125
- outgate_weight: bfloat16 [2048, 1024], P('ep', 'tp'), may hold values from -0.125 to 0.125
- input_weight: bfloat16 [2048, 8], P('ep', 'tp'), may hold values from -0.125 to 0.125
- forget_weight: bfloat16 [2048, 8], P('ep', 'tp'), may hold values from -0.125 to 0.125
- forget_bias: float32 [8], P('tp'), may hold values from -1 to 5
- memory: float32 [1024, 8, 128, 128], P('ep', 'tp'), may hold values from -2.4 to 2.4
- stabilizer: float32 [1024, 8], P('ep', 'tp'), may hold values from -3 to 3
- head_gain: float32 [1024], P('tp'), may hold values from 0.1 to 1.9
- mix_weight: bfloat16 [1024, 2048], P('tp', 'ep'), may hold values from -0.1875 to 0.1875
- second_gain: float32 [2048], replicated, may hold values from 0.1 to 1.9
- route_experts: int32 [1024, 4], P('ep'), may hold values from 0 to 63, all different within a row; in each aligned block of 16 rows (0 to 15, 16 to 31, ...) at most 2 rows name the same one
- route_weight: float32 [1024, 4], P('ep'), may hold values from 0.1 to 1
- expert_gate: bfloat16 [64, 2048, 2048], P('ep', None, 'tp'), may hold values from -0.5 to 0.5
- expert_up: bfloat16 [64, 2048, 2048], P('ep', None, 'tp'), may hold values from -0.5 to 0.5
- expert_down: bfloat16 [64, 2048, 2048], P('ep', 'tp'), may hold values from -0.03125 to 0.03125
- dense_gate: bfloat16 [4096, 2048], P(('ep', 'tp')), may hold values from -0.125 to 0.125
- dense_up: bfloat16 [4096, 2048], P(('ep', 'tp')), may hold values from -0.125 to 0.125
- dense_down: bfloat16 [4096, 2048], P(('ep', 'tp')), may hold values from -0.09375 to 0.09375
- branch_scale: float32 [2048], replicated, may hold values from 0.3 to 1.5
Outputs:
- mixed: bfloat16 [1024, 2048], P('ep', 'tp')
- memory_new: float32 [1024, 8, 128, 128], P('ep', 'tp')
- stabilizer_new: float32 [1024, 8], P('ep', 'tp')
The draws below stay inside these ranges and needn't reach their ends.
Inputs may be any that keep to these rules, and one draw needn't show every extreme that they name: `route_experts`: each row names 4 different experts. Within each aligned block of 16 rows no expert is named by more than 2 rows, and in every draw some expert is named by exactly 2 rows of some block.
All inputs are finite; a program needn't handle non-finite values.
Results may differ from the reference program's by a relative error of at most 0.03.
Values may be sent and summed in bfloat16 or wider, within the bound.
A program may use at most 128 MiB of HBM per device.

```python
import math
import jax
import jax.numpy as jnp
import numpy as np
from jax import lax

MODEL = 2048
HEADS = 8
HEAD_SIZE = 128
HIDDEN_SIZE = 2048
DENSE = 4096
TOPK = 4
SEQ_GROUP = 16
BATCH = 1024
EXPERTS = 64
CAPACITY = 2
N_EP = 64
N_TP = 2


def shard_levels(key, dims, shards, least, largest):
    def one(position, parts):
        steps = jax.random.uniform(jax.random.fold_in(jax.random.fold_in(key, 6), position), (parts,), jnp.float32, least / len(shards), largest / len(shards))
        return jnp.repeat(jnp.exp(steps), dims[position] // parts).reshape((-1,) + (1,) * (len(dims) - position - 1))

    level = one(*shards[0])
    for cut in shards[1:]:
        level = level * one(*cut)
    return level


def routed_block(rng, own, number, rows, count, top, most, lean):
    ranking = jax.random.permutation(rng, count)
    crowded, common = portions_of(count, rows * top, most, lean, True), portions_of(count, rows * top, most, lean, False)
    places = jnp.arange(count)

    def named(sizes, offset_by):
        used = int((sizes > 0).sum())
        fixed = max(1, used // 4)
        passed = fixed + (places - fixed + offset_by * (used - fixed)) % max(1, count - fixed)
        return jnp.zeros((count,), jnp.int32).at[ranking[jnp.where(places < fixed, places, passed)]].set(jnp.asarray(sizes, jnp.int32))

    sizes = jnp.where(number % 4 == 0, named(crowded, number // 4), named(common, number - number // 4 - 1))
    mixed = jax.random.permutation(jax.random.fold_in(own, 3), count)
    giver, receiver = mixed[0:count // 2 * 2:2], mixed[1:count // 2 * 2:2]
    margin = jnp.minimum(sizes[giver] - 1, most - sizes[receiver]) // 2
    margin = jnp.where((giver == ranking[0]) | (receiver == ranking[0]) | (sizes[receiver] == 0), 0, jnp.maximum(margin, 0))
    passed = jax.random.randint(jax.random.fold_in(own, 4), (count // 2,), 0, 1 << 20) % (margin + 1)
    sizes = sizes.at[giver].add(-passed).at[receiver].add(passed)
    members = jnp.searchsorted(jnp.cumsum(sizes), jnp.arange(rows * top), side="right").astype(jnp.int32)
    grid = members.reshape(top, rows).T
    grid = grid[jax.random.permutation(jax.random.fold_in(own, 1), rows)]
    offset_by = jax.random.randint(jax.random.fold_in(own, 2), (rows, 1), 0, top)
    return jnp.take_along_axis(grid, (jnp.arange(top)[None, :] + offset_by) % top, axis=1)


def portions_of(number_of, total, limit, slope, full):
    weights = [(1 << 20) // math.isqrt(rank ** slope) + 1 for rank in range(1, number_of + 1)]
    largest = limit if full else min(limit, max(-(-total // number_of), total * weights[0] // sum(weights)))
    least = 1 if total - largest >= number_of - 1 else 0
    given, rest = [largest] + [least] * (number_of - 1), total - largest - least * (number_of - 1)
    while rest > 0:
        candidates = [i for i in range(1, number_of) if given[i] < largest] or [i for i in range(1, number_of) if given[i] < limit]
        whole, budget = sum([weights[i] for i in candidates]), rest
        for i in candidates:
            addition = min(limit - given[i], max(1, budget * weights[i] // whole), rest)
            given[i] = given[i] + addition
            rest = rest - addition
    return np.array(given)


def gaussian(key, dims, scale, limit, shards=(), dtype=jnp.bfloat16):
    result = scale * jax.random.normal(key, dims, jnp.float32)
    if shards:
        result = result * shard_levels(key, dims, shards, -0.22, 0.18)
    return jnp.clip(result, -limit, limit).astype(dtype)


def setup_inputs(seed: int = 0) -> dict:
    arg_keys = jax.random.split(jax.random.key(seed), 24)
    tokens = gaussian(arg_keys[0], (BATCH, MODEL), 1.0, 6.0, ((0, 64),))
    norm_gain = jnp.clip(1.0 + 0.18 * jax.random.normal(arg_keys[1], (MODEL,), jnp.float32), 0.1, 1.9)
    query_weight = gaussian(arg_keys[2], (MODEL, HEADS * HEAD_SIZE), MODEL ** -0.5, 0.125, ((0, 64), (1, 2)))
    key_weight = gaussian(arg_keys[3], (MODEL, HEADS * HEAD_SIZE), MODEL ** -0.5, 0.125, ((0, 64), (1, 2)))
    value_weight = gaussian(arg_keys[4], (MODEL, HEADS * HEAD_SIZE), MODEL ** -0.5, 0.125, ((0, 64), (1, 2)))
    outgate_weight = gaussian(arg_keys[5], (MODEL, HEADS * HEAD_SIZE), MODEL ** -0.5, 0.125, ((0, 64), (1, 2)))
    input_weight = gaussian(arg_keys[6], (MODEL, HEADS), MODEL ** -0.5, 0.125, ((0, 64), (1, 2)))
    forget_weight = gaussian(arg_keys[7], (MODEL, HEADS), MODEL ** -0.5, 0.125, ((0, 64), (1, 2)))
    forget_bias = jnp.clip(-1.0 + 6.0 * jax.random.uniform(arg_keys[8], (HEADS,), jnp.float32) ** shard_levels(arg_keys[8], (HEADS,), ((0, 2),), -0.2, 0.2), -1.0, 5.0)
    memory = gaussian(arg_keys[9], (BATCH, HEADS, HEAD_SIZE, HEAD_SIZE), 0.3, 2.4, ((0, 64), (1, 2)), jnp.float32)
    stabilizer = jnp.clip(jax.random.uniform(arg_keys[10], (BATCH, HEADS), jnp.float32, -3.0, 3.0) * shard_levels(arg_keys[10], (BATCH, HEADS), ((0, 64), (1, 2)), -0.4, 0.0), -3.0, 3.0)
    head_gain = jnp.clip(1.0 + 0.18 * jax.random.normal(arg_keys[11], (HEADS * HEAD_SIZE,), jnp.float32), 0.1, 1.9)
    mix_weight = gaussian(arg_keys[12], (HEADS * HEAD_SIZE, MODEL), (HEADS * HEAD_SIZE) ** -0.5, 0.1875, ((0, 2), (1, 64)))
    second_gain = jnp.clip(1.0 + 0.18 * jax.random.normal(arg_keys[13], (MODEL,), jnp.float32), 0.1, 1.9)
    route_experts_keys = jax.random.split(jax.random.fold_in(arg_keys[14], 1), BATCH // SEQ_GROUP)
    route_experts_turns = jax.random.permutation(jax.random.fold_in(arg_keys[14], 3), BATCH // SEQ_GROUP)
    route_experts = jax.vmap(lambda own, number: routed_block(jax.random.fold_in(arg_keys[14], 2), own, number, SEQ_GROUP, EXPERTS, TOPK, CAPACITY, 2))(route_experts_keys, route_experts_turns).reshape((BATCH, TOPK))
    route_weight = jnp.clip(jnp.exp(math.log(1.0) - 2.3025851 * jax.random.uniform(arg_keys[15], (BATCH, TOPK), jnp.float32) ** shard_levels(arg_keys[15], (BATCH, TOPK), ((0, 64),), -0.2, 0.2)), 0.1, 1.0)
    expert_gate = gaussian(arg_keys[16], (EXPERTS, MODEL, HIDDEN_SIZE), (MODEL // 16) ** -0.5, 0.5, ((0, 64), (2, 2)))
    expert_up = gaussian(arg_keys[17], (EXPERTS, MODEL, HIDDEN_SIZE), (MODEL // 16) ** -0.5, 0.5, ((0, 64), (2, 2)))
    expert_down = gaussian(arg_keys[18], (EXPERTS, HIDDEN_SIZE, MODEL), (16 * HIDDEN_SIZE) ** -0.5, 0.03125, ((0, 64), (1, 2)))
    dense_gate = gaussian(arg_keys[19], (DENSE, MODEL), MODEL ** -0.5, 0.125, ((0, 128),))
    dense_up = gaussian(arg_keys[20], (DENSE, MODEL), MODEL ** -0.5, 0.125, ((0, 128),))
    dense_down = gaussian(arg_keys[21], (DENSE, MODEL), DENSE ** -0.5, 0.09375, ((0, 128),))
    branch_scale = jnp.clip(jax.random.uniform(arg_keys[22], (MODEL,), jnp.float32, 0.3, 1.5), 0.3, 1.5)
    return dict(tokens=tokens, norm_gain=norm_gain, query_weight=query_weight, key_weight=key_weight, value_weight=value_weight, outgate_weight=outgate_weight, input_weight=input_weight, forget_weight=forget_weight, forget_bias=forget_bias, memory=memory, stabilizer=stabilizer, head_gain=head_gain, mix_weight=mix_weight, second_gain=second_gain, route_experts=route_experts, route_weight=route_weight, expert_gate=expert_gate, expert_up=expert_up, expert_down=expert_down, dense_gate=dense_gate, dense_up=dense_up, dense_down=dense_down, branch_scale=branch_scale)


norm_eps = 1e-05
clamp_limit = 7.0
sigmoid_slope = 1.702

def rms_scale(values, gain):
    mean_square = lax.optimization_barrier(jnp.mean(values * values, axis=-1, keepdims=True))
    return values * lax.rsqrt(mean_square + norm_eps) * gain

def round_half(values):
    return lax.optimization_barrier(values.astype(jnp.bfloat16)).astype(jnp.float32)

def clamped_unit(gate_pre, up_pre):
    gate_clamped = jnp.minimum(gate_pre, clamp_limit)
    up_clamped = jnp.clip(up_pre, -clamp_limit, clamp_limit)
    return ((up_clamped + 1.0) * gate_clamped * jax.nn.sigmoid(sigmoid_slope * gate_clamped)).astype(jnp.bfloat16)

def memory_step(projected, forget_bias, memory, stabilizer, head_gain):
    query_rows, key_rows, value_rows, outgate_rows, input_pre, forget_pre = projected
    sequences, head_count = stabilizer.shape
    head_size = memory.shape[-1]
    log_forget = jax.nn.log_sigmoid(forget_pre + forget_bias)
    stab_new = jnp.maximum(log_forget + stabilizer, input_pre)
    carried = jnp.exp(log_forget + stabilizer - stab_new)
    written = jnp.exp(input_pre - stab_new)
    query_heads = query_rows.astype(jnp.float32).reshape(sequences, head_count, head_size)
    key_heads = key_rows.astype(jnp.float32).reshape(sequences, head_count, head_size) * head_size ** (-0.5)
    value_heads = value_rows.astype(jnp.float32).reshape(sequences, head_count, head_size)
    memory_new = carried[:, :, None, None] * memory + written[:, :, None, None] * value_heads[:, :, :, None] * key_heads[:, :, None, :]
    readout = jnp.einsum('bhvk,bhk->bhv', memory_new, query_heads, precision=lax.Precision.HIGHEST)
    out_gate = jax.nn.sigmoid(outgate_rows.astype(jnp.float32).reshape(sequences, head_count, head_size))
    gated = (rms_scale(readout, head_gain.reshape(head_count, head_size)) * out_gate).astype(jnp.bfloat16)
    return (gated.reshape(sequences, head_count * head_size), memory_new, stab_new)

def expert_mix(normed_second, route_experts, route_weight, expert_gate, expert_up, expert_down):
    batch_rows, model_width = normed_second.shape
    expert_count = expert_gate.shape[0]
    hidden_units = expert_gate.shape[2]
    group_units = hidden_units // N_TP
    blocks = normed_second.astype(jnp.float32).reshape(N_EP, batch_rows // N_EP, model_width)
    slots = jnp.arange(CAPACITY).astype(jnp.float32)

    def one_expert(total, index):
        matched = route_experts == index
        hit_mask = jnp.any(matched, axis=1).astype(jnp.float32).reshape(N_EP, -1)
        weights = lax.optimization_barrier(jnp.sum(jnp.where(matched, route_weight, 0.0), axis=1)).reshape(N_EP, -1)
        ranks = jnp.cumsum(hit_mask, axis=1) - 1.0
        select = hit_mask[:, None, :] * (ranks[:, None, :] == slots[None, :, None]).astype(jnp.float32)
        rows = jnp.einsum('jcs,jsd->jcd', select, blocks, precision=lax.Precision.HIGHEST)
        rows = rows.astype(jnp.bfloat16).reshape(-1, model_width)
        gate_pre = jnp.dot(rows, expert_gate[index], preferred_element_type=jnp.float32)
        up_pre = jnp.dot(rows, expert_up[index], preferred_element_type=jnp.float32)
        activity = clamped_unit(gate_pre, up_pre)
        down_weight = expert_down[index]
        outputs = jnp.zeros((rows.shape[0], model_width), jnp.float32)
        for group in range(N_TP):
            lower = group * group_units
            outputs = outputs + round_half(jnp.dot(activity[:, lower:lower + group_units], down_weight[lower:lower + group_units], preferred_element_type=jnp.float32))
        outputs = outputs.reshape(N_EP, CAPACITY, model_width)
        spread = jnp.einsum('jcs,jcd->jsd', select * weights[:, None, :], outputs, precision=lax.Precision.HIGHEST)
        return (total + spread.reshape(batch_rows, model_width), None)
    total, unused = lax.scan(one_expert, jnp.zeros((batch_rows, model_width), jnp.float32), jnp.arange(expert_count).astype(jnp.int32))
    return total

def reference(tokens, norm_gain, query_weight, key_weight, value_weight, outgate_weight, input_weight, forget_weight, forget_bias, memory, stabilizer, head_gain, mix_weight, second_gain, route_experts, route_weight, expert_gate, expert_up, expert_down, dense_gate, dense_up, dense_down, branch_scale):
    inputs_float = tokens.astype(jnp.float32)
    normed = rms_scale(inputs_float, norm_gain).astype(jnp.bfloat16)
    projected = (jnp.dot(normed, query_weight, preferred_element_type=jnp.float32).astype(jnp.bfloat16), jnp.dot(normed, key_weight, preferred_element_type=jnp.float32).astype(jnp.bfloat16), jnp.dot(normed, value_weight, preferred_element_type=jnp.float32).astype(jnp.bfloat16), jnp.dot(normed, outgate_weight, preferred_element_type=jnp.float32).astype(jnp.bfloat16), jnp.dot(normed, input_weight, preferred_element_type=jnp.float32), jnp.dot(normed, forget_weight, preferred_element_type=jnp.float32))
    gated, memory_new, stab_new = memory_step(projected, forget_bias, memory, stabilizer, head_gain)
    group_width = gated.shape[1] // N_TP
    attended = jnp.zeros_like(inputs_float)
    for group in range(N_TP):
        lower = group * group_width
        attended = attended + round_half(jnp.dot(gated[:, lower:lower + group_width], mix_weight[lower:lower + group_width], preferred_element_type=jnp.float32))
    residual = (inputs_float + attended).astype(jnp.bfloat16)
    residual_float = residual.astype(jnp.float32)
    normed_second = rms_scale(residual_float, second_gain).astype(jnp.bfloat16)
    routed = expert_mix(normed_second, route_experts, route_weight, expert_gate, expert_up, expert_down)
    dense_pre = jnp.dot(normed_second, dense_gate.T, preferred_element_type=jnp.float32)
    dense_lift = jnp.dot(normed_second, dense_up.T, preferred_element_type=jnp.float32)
    dense_act = (jax.nn.silu(dense_pre) * dense_lift).astype(jnp.bfloat16)
    dense_out = jnp.dot(dense_act, dense_down, preferred_element_type=jnp.float32)
    mixed = (residual_float + routed + branch_scale * dense_out).astype(jnp.bfloat16)
    return (mixed, memory_new, stab_new)
```

```python
import jax
import jax.numpy as jnp
from jax import lax
from jax.experimental import pallas as pl
from jax.experimental.pallas import tpu as pltpu
from jax.sharding import PartitionSpec as P

norm_eps = 1e-05
clamp_limit = 7.0
sigmoid_slope = 1.702
F32 = jnp.float32
BF16 = jnp.bfloat16
MESH = pl.DeviceIdType.MESH
VMEM_SPEC = pl.BlockSpec(memory_space=pltpu.VMEM)
ANY_SPEC = pl.BlockSpec(memory_space=pl.ANY)
VMEM_LIMIT = 60 * 1024 * 1024

SIDE = 4
PLANE = 16
CHIPS = 64
ROWS = 16


def rms_scale(values, gain):
    mean_square = jnp.mean(values * values, axis=-1, keepdims=True)
    return values * lax.rsqrt(mean_square + norm_eps) * gain


def own_place():
    chip = lax.axis_index("ep")
    core = lax.axis_index("tp")
    return chip, core, chip % SIDE, chip // SIDE


def plane_shift(plane, step):
    z = (plane // SIDE + step // SIDE) % SIDE
    y = (plane % SIDE + step % SIDE) % SIDE
    return z * SIDE + y


def plane_back(plane, step):
    z = (plane // SIDE + SIDE - step // SIDE) % SIDE
    y = (plane % SIDE + SIDE - step % SIDE) % SIDE
    return z * SIDE + y


def chip_shift(chip, step):
    plane = plane_shift(chip // SIDE, step // SIDE)
    return plane * SIDE + (chip % SIDE + step % SIDE) % SIDE


def remote(src, dst, send, recv, device):
    return pltpu.make_async_remote_copy(
        src_ref=src, dst_ref=dst, send_sem=send, recv_sem=recv,
        device_id=device, device_id_type=MESH,
    )


def projection_kernel(
    tok_ref, gain_ref, wq_ref, wk_ref, wv_ref, wo_ref, wi_ref, wf_ref, mix_ref, dg_ref, du_ref, dd_ref,
    rows_ref, gates_ref, mixall_ref, dgall_ref, duall_ref, ddall_ref,
    wbuf, gbuf, nbuf, abuf, pbuf, rbuf,
    load_sem, w_send, w_recv, g_send, g_recv, a_send, a_recv, m_send, m_recv, r_send, r_recv, d_send, d_recv,
):
    chip, core, x, plane = own_place()
    right = plane * SIDE + (x + 1) % SIDE
    left = plane * SIDE + (x + 3) % SIDE
    across = plane * SIDE + (x + 2) % SIDE
    xl, xr, xa = (x + 3) % SIDE, (x + 1) % SIDE, (x + 2) % SIDE
    other = 1 - core

    barrier = pltpu.get_barrier_semaphore()
    for peer in (right, left, across):
        pl.semaphore_signal(barrier, inc=1, device_id=(peer, core), device_id_type=MESH)
    pl.semaphore_signal(barrier, inc=1, device_id=(chip, other), device_id_type=MESH)

    def greet(step, carry):
        peer = plane_shift(plane, step) * SIDE + x
        pl.semaphore_signal(barrier, inc=1, device_id=(peer, core), device_id_type=MESH)
        return carry

    lax.fori_loop(1, PLANE, greet, 0)

    def w_rows(xs):
        return pl.ds(pl.multiple_of(32 * xs, 32), 32)

    def half_rows(xs, half):
        return pl.ds(pl.multiple_of(32 * xs + 16 * half, 16), 16)

    loads = []
    for k, ref in enumerate((wq_ref, wk_ref, wv_ref, wo_ref)):
        load = pltpu.make_async_copy(ref, wbuf.at[w_rows(x), pl.ds(512 * k, 512)], load_sem.at[k])
        load.start()
        loads.append(load)

    normed = rms_scale(tok_ref[...].astype(F32), gain_ref[...])
    nbuf[...] = normed.astype(BF16)
    place = (
        lax.broadcasted_iota(jnp.int32, (32, 128), 1) == lax.broadcasted_iota(jnp.int32, (32, 128), 0) + 32 * x
    ).astype(F32)
    gate_in = jnp.dot(wi_ref[...].astype(F32), place, preferred_element_type=F32)
    gate_fo = jnp.dot(wf_ref[...].astype(F32), place, preferred_element_type=F32)
    gbuf[x] = jnp.concatenate([gate_in, gate_fo], axis=0)
    for load in loads:
        load.wait()
    pl.semaphore_wait(barrier, 3 + 1 + 15)

    own_w = wbuf.at[w_rows(x), :]
    w_right = remote(own_w, own_w, w_send.at[0], w_recv.at[0], (right, core))
    w_left = remote(own_w, own_w, w_send.at[1], w_recv.at[1], (left, core))
    w_right.start()
    w_left.start()
    g_copies = []
    for k, peer in enumerate((right, left, across)):
        copy = remote(gbuf.at[x], gbuf.at[x], g_send.at[k], g_recv.at[k], (peer, core))
        copy.start()
        g_copies.append(copy)

    def token_copy(step):
        peer = plane_shift(plane, step)
        return remote(
            nbuf.at[:, pl.ds(pl.multiple_of(128 * peer, 128), 128)],
            abuf.at[pl.ds(pl.multiple_of(ROWS * plane, ROWS), ROWS), :],
            a_send.at[step], a_recv.at[step], (peer * SIDE + x, core),
        )

    def mix_copy(step):
        peer = plane_shift(plane, step)
        return remote(mix_ref, mixall_ref.at[plane], m_send.at[step], m_recv.at[step], (peer * SIDE + x, core))

    def start_tokens(step, carry):
        token_copy(step).start()
        return carry

    def start_mix(step, carry):
        mix_copy(step).start()
        return carry

    lax.fori_loop(1, PLANE, start_tokens, 0)
    abuf[pl.ds(pl.multiple_of(ROWS * plane, ROWS), ROWS), :] = nbuf[:, pl.ds(pl.multiple_of(128 * plane, 128), 128)]
    lax.fori_loop(1, PLANE, start_mix, 0)
    mix_own = pltpu.make_async_copy(mix_ref, mixall_ref.at[plane], load_sem.at[4])
    mix_own.start()

    dense = ((dg_ref, dgall_ref), (du_ref, duall_ref), (dd_ref, ddall_ref))
    d_first = []
    for k, (src, dst) in enumerate(dense):
        d_first.append(remote(src, dst.at[2 * x + core], d_send.at[k, 0], d_recv.at[k, 0], (right, core)))
        d_first.append(remote(src, dst.at[2 * x + core], d_send.at[k, 1], d_recv.at[k, 1], (left, core)))
        d_first.append(remote(src, dst.at[2 * x + core], d_send.at[k, 4], d_recv.at[k, 4], (chip, other)))

    w_right.wait_recv()
    relay_r = remote(
        wbuf.at[half_rows(xl, 0), :], wbuf.at[half_rows(xl, 0), :], w_send.at[2], w_recv.at[2], (right, core)
    )
    relay_r.start()
    w_left.wait_recv()
    relay_l = remote(
        wbuf.at[half_rows(xr, 1), :], wbuf.at[half_rows(xr, 1), :], w_send.at[3], w_recv.at[3], (left, core)
    )
    relay_l.start()
    for copy in d_first:
        copy.start()

    def wait_tokens(step, carry):
        token_copy(step).wait_recv()
        return carry

    lax.fori_loop(1, PLANE, wait_tokens, 0)
    for copy in g_copies:
        copy.wait_recv()
    gate_w = (gbuf[0] + gbuf[1] + gbuf[2] + gbuf[3]).astype(BF16)
    gate_w = jnp.concatenate([gate_w.astype(F32), jnp.zeros((120, 128), F32)], axis=0).astype(BF16)
    relay_r.wait_recv()
    relay_l.wait_recv()

    def row_copy(step):
        peer = plane_shift(plane, step)
        return remote(
            pbuf.at[pl.ds(pl.multiple_of(ROWS * peer, ROWS), ROWS), :], rbuf.at[plane],
            r_send.at[step], r_recv.at[step], (peer * SIDE + x, core),
        )

    for dz in (2, 1, 3, 0):
        zt = (plane // SIDE + dz) % SIDE
        rows = pl.ds(pl.multiple_of(64 * zt, 64), 64)
        acts = abuf[rows, :]
        for k in range(4):
            cols = slice(512 * k, 512 * k + 512)
            pbuf[rows, cols] = jnp.dot(acts, wbuf[:, cols], preferred_element_type=F32).astype(BF16)
        gates = lax.dot_general(acts, gate_w, (((1,), (1,)), ((), ())), preferred_element_type=F32)
        high = gates.astype(BF16).astype(F32)
        pbuf[rows, 2048:2176] = (high + pltpu.roll(gates - high, 8, 1)).astype(BF16)
        for dy in (2, 1, 3, 0):
            if (dz, dy) != (0, 0):
                row_copy(dz * SIDE + dy).start()
    rbuf[plane] = pbuf[pl.ds(pl.multiple_of(ROWS * plane, ROWS), ROWS), :]

    d_more = []
    for k, (src, dst) in enumerate(dense):
        d_first[3 * k].wait_recv()
        first, second = pl.ds(0, 16), pl.ds(16, 16)
        from_left, from_right = dst.at[2 * xl + core], dst.at[2 * xr + core]
        copy = remote(from_left.at[first], from_left.at[first], d_send.at[k, 2], d_recv.at[k, 2], (right, core))
        copy.start()
        d_more.append(copy)
        d_first[3 * k + 1].wait_recv()
        copy = remote(from_right.at[second], from_right.at[second], d_send.at[k, 3], d_recv.at[k, 3], (left, core))
        copy.start()
        d_more.append(copy)
        copy = remote(from_left, from_left, d_send.at[k, 5], d_recv.at[k, 5], (chip, other))
        copy.start()
        d_more.append(copy)
        copy = remote(from_right, from_right, d_send.at[k, 6], d_recv.at[k, 6], (chip, other))
        copy.start()
        d_more.append(copy)

    def wait_rows(step, carry):
        row_copy(step).wait_recv()
        return carry

    lax.fori_loop(1, PLANE, wait_rows, 0)
    for k in range(4):
        cols = slice(512 * k, 512 * k + 512)
        total = rbuf[0, :, cols].astype(F32)
        for s in range(1, PLANE):
            total = total + rbuf[s, :, cols].astype(F32)
        rows_ref[:, cols] = total.astype(BF16)
    total = rbuf[0, :, 2048:2176].astype(F32)
    for s in range(1, PLANE):
        total = total + rbuf[s, :, 2048:2176].astype(F32)
    gates_ref[...] = total + pltpu.roll(total, 120, 1)

    d_last = []
    for k, (src, dst) in enumerate(dense):
        over = dst.at[2 * xa + core]
        d_more[4 * k].wait_recv()
        copy = remote(over.at[pl.ds(0, 16)], over.at[pl.ds(0, 16)], d_send.at[k, 7], d_recv.at[k, 7], (chip, other))
        copy.start()
        d_last.append(copy)
        d_more[4 * k + 1].wait_recv()
        copy = remote(over.at[pl.ds(16, 16)], over.at[pl.ds(16, 16)], d_send.at[k, 8], d_recv.at[k, 8], (chip, other))
        copy.start()
        d_last.append(copy)

    w_right.wait_send()
    w_left.wait_send()
    relay_r.wait_send()
    relay_l.wait_send()
    for copy in g_copies:
        copy.wait_send()

    def finish(step, carry):
        token_copy(step).wait_send()
        mix_copy(step).wait()
        row_copy(step).wait_send()
        return carry

    lax.fori_loop(1, PLANE, finish, 0)
    mix_own.wait()
    for k in range(3):
        d_first[3 * k].wait_send()
        d_first[3 * k + 1].wait_send()
        d_first[3 * k + 2].wait()
        d_more[4 * k].wait_send()
        d_more[4 * k + 1].wait_send()
        d_more[4 * k + 2].wait()
        d_more[4 * k + 3].wait()
    for copy in d_last:
        copy.wait()


def project(tokens, norm_gain, wq, wk, wv, wo, wi_t, wf_t, mix_t, dg, du, dd):
    dma = pltpu.SemaphoreType.DMA
    return pl.pallas_call(
        projection_kernel,
        out_shape=(
            jax.ShapeDtypeStruct((ROWS, 2048), BF16),
            jax.ShapeDtypeStruct((ROWS, 128), F32),
            jax.ShapeDtypeStruct((PLANE, 32, 512), BF16),
            jax.ShapeDtypeStruct((8, 32, 2048), BF16),
            jax.ShapeDtypeStruct((8, 32, 2048), BF16),
            jax.ShapeDtypeStruct((8, 32, 2048), BF16),
        ),
        in_specs=[VMEM_SPEC] * 2 + [ANY_SPEC] * 4 + [VMEM_SPEC] * 3 + [ANY_SPEC] * 3,
        out_specs=(VMEM_SPEC, VMEM_SPEC, ANY_SPEC, ANY_SPEC, ANY_SPEC, ANY_SPEC),
        scratch_shapes=[
            pltpu.VMEM((128, 2048), BF16),
            pltpu.VMEM((4, 8, 128), F32),
            pltpu.VMEM((ROWS, 2048), BF16),
            pltpu.VMEM((256, 128), BF16),
            pltpu.VMEM((256, 2176), BF16),
            pltpu.VMEM((PLANE, ROWS, 2176), BF16),
            dma((5,)),
            dma((4,)), dma((4,)),
            dma((3,)), dma((3,)),
            dma((16,)), dma((16,)),
            dma((16,)), dma((16,)),
            dma((16,)), dma((16,)),
            dma((3, 9)), dma((3, 9)),
        ],
        compiler_params=pltpu.CompilerParams(
            collective_id=0, has_side_effects=True, vmem_limit_bytes=VMEM_LIMIT
        ),
        name="project",
    )(tokens, norm_gain, wq, wk, wv, wo, wi_t, wf_t, mix_t, dg, du, dd)


def memory_step(rows, gates, forget_bias, memory, stabilizer, head_gain):
    sequences, head_count = stabilizer.shape
    head_size = memory.shape[-1]
    input_pre = gates[:, :head_count]
    forget_pre = gates[:, head_count:2 * head_count]
    log_forget = jax.nn.log_sigmoid(forget_pre + forget_bias)
    stab_new = jnp.maximum(log_forget + stabilizer, input_pre)
    carried = jnp.exp(log_forget + stabilizer - stab_new)
    written = jnp.exp(input_pre - stab_new)
    heads = rows.astype(F32).reshape(sequences, 4, head_count, head_size)
    query_heads = heads[:, 0]
    key_heads = heads[:, 1] * head_size ** (-0.5)
    value_heads = heads[:, 2]
    memory_new = (
        carried[:, :, None, None] * memory
        + written[:, :, None, None] * value_heads[:, :, :, None] * key_heads[:, :, None, :]
    )
    readout = jnp.einsum("bhvk,bhk->bhv", memory_new, query_heads)
    out_gate = jax.nn.sigmoid(heads[:, 3])
    gated = (rms_scale(readout, head_gain.reshape(head_count, head_size)) * out_gate).astype(BF16)
    return gated.reshape(sequences, head_count * head_size), memory_new, stab_new


def expert_kernel(
    gated_ref, mix_ref, tok_ref, gain_ref, route_ref, weight_ref, eg_ref, eu_ref, ed_ref,
    dg_ref, du_ref, dd_ref, dgall_ref, duall_ref, ddall_ref, scale_ref,
    out_ref,
    egv, euv, edv, dgv, duv, ddv, gx, asend, tb, ns, res, n2, sel, comb_hi, comb_lo, obuf, rx, xbuf, hbuf,
    yown, ysend, yrecv, yret, rret, da, dout, dr,
    load_sem, gx_send, gx_recv, tb_send, tb_recv, x_send, x_recv, da_send, da_recv,
    y_send, y_recv, q_send, q_recv, dr_send, dr_recv,
):
    chip, core, x, plane = own_place()
    other = 1 - core

    loads = []
    for k, (src, dst) in enumerate(((eg_ref, egv), (eu_ref, euv), (ed_ref, edv))):
        loads.append(pltpu.make_async_copy(src.at[0], dst, load_sem.at[k]))
    dense_loads = []
    for k, (own, rest, dst) in enumerate(
        ((dg_ref, dgall_ref, dgv), (du_ref, duall_ref, duv), (dd_ref, ddall_ref, ddv))
    ):
        mine = 2 * x + core
        dense_loads.append(pltpu.make_async_copy(own, dst.at[mine], load_sem.at[8 * k + 3]))
        for s in range(1, 8):
            slot = (mine + s) % 8
            dense_loads.append(pltpu.make_async_copy(rest.at[slot], dst.at[slot], load_sem.at[8 * k + 3 + s]))
    for load in loads + dense_loads:
        load.start()

    barrier = pltpu.get_barrier_semaphore()

    def greet(step, carry):
        peer = chip_shift(chip, step)
        pl.semaphore_signal(barrier, inc=1, device_id=(peer, core), device_id_type=MESH)
        return carry

    lax.fori_loop(1, CHIPS, greet, 0)
    pl.semaphore_signal(barrier, inc=1, device_id=(chip, other), device_id_type=MESH)

    def greet_plane(step, carry):
        peer = plane_shift(plane, step) * SIDE + x
        pl.semaphore_signal(barrier, inc=1, device_id=(peer, other), device_id_type=MESH)
        return carry

    lax.fori_loop(1, PLANE, greet_plane, 0)
    for d in range(1, SIDE):
        peer = plane * SIDE + (x + d) % SIDE
        pl.semaphore_signal(barrier, inc=1, device_id=(peer, other), device_id_type=MESH)

    spread = (
        lax.broadcasted_iota(jnp.int32, (ROWS, 128), 1) % ROWS == lax.broadcasted_iota(jnp.int32, (ROWS, 128), 0)
    ).astype(F32)
    route = jnp.dot(route_ref[...].astype(F32), spread, preferred_element_type=F32, precision=lax.Precision.HIGHEST)
    weight = jnp.dot(weight_ref[...], spread, preferred_element_type=F32, precision=lax.Precision.HIGHEST)
    expert = lax.broadcasted_iota(jnp.int32, (CHIPS, 128), 0).astype(F32)
    hit = jnp.zeros((CHIPS, 128), F32)
    chosen = jnp.zeros((CHIPS, 128), F32)
    for k in range(4):
        same = (route[k:k + 1, :] == expert).astype(F32)
        hit = hit + same
        chosen = chosen + same * weight[k:k + 1, :]
    col = lax.broadcasted_iota(jnp.int32, (128, 128), 1) % ROWS
    row = lax.broadcasted_iota(jnp.int32, (128, 128), 0)
    before = ((row < ROWS) & (row < col)).astype(F32)
    rank = jnp.dot(hit, before, preferred_element_type=F32)
    first = hit * (rank == 0.0).astype(F32)
    second = hit * (rank == 1.0).astype(F32)
    block_row = lax.broadcasted_iota(jnp.int32, (8, 128), 0)
    block_col = lax.broadcasted_iota(jnp.int32, (8, 128), 1) // ROWS
    diagonal = (block_row == block_col).astype(F32)

    def widened(top, bottom):
        low = top[:, None, :] * diagonal[None, :, :]
        high = bottom[:, None, :] * diagonal[None, :, :]
        return jnp.concatenate([low, high], axis=1).reshape(1024, 128)

    sel[...] = widened(first, second).astype(BF16)
    comb = widened(first * chosen, second * chosen).T
    comb_top = comb.astype(BF16)
    comb_hi[...] = comb_top
    comb_lo[...] = (comb - comb_top.astype(F32)).astype(BF16)
    gx[pl.ds(pl.multiple_of(ROWS * x, ROWS), ROWS), :] = gated_ref[...]

    pl.semaphore_wait(barrier, 63 + 1 + 15 + 3)

    def gx_copy(d):
        rows = pl.ds(pl.multiple_of(ROWS * x, ROWS), ROWS)
        peer = plane * SIDE + (x + d) % SIDE
        return remote(gated_ref, gx.at[rows, :], gx_send.at[d], gx_recv.at[d], (peer, core))

    for d in range(1, SIDE):
        gx_copy(d).start()
    for d in range(1, SIDE):
        gx_copy(d).wait_recv()
    asend[...] = lax.dot_general(
        gx[...], mix_ref[...], (((1,), (1,)), ((), ())), preferred_element_type=F32
    ).astype(BF16)

    def tb_copy(d, side):
        rows = pl.ds(pl.multiple_of(ROWS * ((x + d) % SIDE), ROWS), ROWS)
        peer = plane * SIDE + (x + d) % SIDE
        return remote(
            asend.at[rows, :], tb.at[core, x], tb_send.at[2 * d + side], tb_recv.at[2 * d + side],
            (peer, (core + side) % 2),
        )

    tb_list = [(0, 1)] + [(d, side) for d in (2, 1, 3) for side in (0, 1)]
    for d, side in tb_list:
        tb_copy(d, side).start()
    tb[core, x] = asend[pl.ds(pl.multiple_of(ROWS * x, ROWS), ROWS), :]
    for d, side in tb_list:
        tb_copy(d, side).wait_recv()
    attended = [tb[0, k].astype(F32) + tb[1, k].astype(F32) for k in range(SIDE)]
    lane = lax.broadcasted_iota(jnp.int32, (ROWS, 128), 1) // 32
    tiles = []
    for t in range(PLANE):
        tile = None
        for k in range(SIDE):
            part = attended[k][:, 128 * (t // 4):128 * (t // 4) + 128]
            shift = (32 * k - 32 * (t % 4)) % 128
            if shift:
                part = pltpu.roll(part, shift, 1)
            tile = part if tile is None else jnp.where(lane == k, part, tile)
        tiles.append(tile)
    residual = (tok_ref[...].astype(F32) + jnp.concatenate(tiles, axis=1)).astype(BF16)
    res[...] = residual
    normed = rms_scale(residual.astype(F32), gain_ref[...]).astype(BF16)
    ns[...] = normed
    for b in range(8):
        n2[16 * b:16 * b + 16, :] = normed[:, 256 * b:256 * b + 256]
    for k in range(4):
        obuf[256 * k:256 * k + 256, :] = jnp.dot(
            sel[256 * k:256 * k + 256, :], n2[...], preferred_element_type=F32
        ).astype(BF16)

    def tile_rows(index):
        return pl.ds(pl.multiple_of(ROWS * index, ROWS), ROWS)

    def x_copy(step):
        peer = chip_shift(chip, step)
        return remote(
            obuf.at[tile_rows(peer), :], rx.at[tile_rows(chip), :], x_send.at[step], x_recv.at[step], (peer, core)
        )

    def start_x(step, carry):
        x_copy(step).start()
        return carry

    lax.fori_loop(1, CHIPS, start_x, 0)
    rx[tile_rows(chip), :] = obuf[tile_rows(chip), :]

    parity = plane % 2
    half = plane // 2

    def da_send_copy(step):
        peer = plane_shift(plane, step)
        return remote(ns, da.at[half], da_send.at[step], da_recv.at[half], (peer * SIDE + x, parity))

    def da_recv_copy(index):
        return remote(ns, da.at[index], da_send.at[0], da_recv.at[index], (chip, other))

    def start_da(index, carry):
        da_send_copy(2 * index + core).start()
        return carry

    lax.fori_loop(1 - core, 8, start_da, 0)

    @pl.when(parity == core)
    def _():
        da[half] = ns[...]

    def wait_x(step, carry):
        x_copy(step).wait_recv()
        return carry

    lax.fori_loop(1, CHIPS, wait_x, 0)
    row = lax.broadcasted_iota(jnp.int32, (256, 256), 0)
    col = lax.broadcasted_iota(jnp.int32, (256, 256), 1)
    gather = (col == ((row % 32) // 2) * 16 + (row % 2) * 8 + row // 32).astype(F32).astype(BF16)
    scatter = (row == ((col % 32) // 2) * 16 + (col % 2) * 8 + col // 32).astype(F32).astype(BF16)
    for g in range(4):
        mixed_up = jnp.dot(gather, rx[256 * g:256 * g + 256, :], preferred_element_type=F32).astype(BF16)
        for b in range(8):
            xbuf[32 * g:32 * g + 32, 256 * b:256 * b + 256] = mixed_up[32 * b:32 * b + 32, :]
    loads[0].wait()
    loads[1].wait()

    def expert_up(t, carry):
        cols = pl.ds(pl.multiple_of(256 * t, 256), 256)
        gate_pre = jnp.dot(xbuf[...], egv[:, cols], preferred_element_type=F32)
        up_pre = jnp.dot(xbuf[...], euv[:, cols], preferred_element_type=F32)
        gate_clamped = jnp.minimum(gate_pre, clamp_limit)
        up_clamped = jnp.clip(up_pre, -clamp_limit, clamp_limit)
        hbuf[:, cols] = (
            (up_clamped + 1.0) * gate_clamped * jax.nn.sigmoid(sigmoid_slope * gate_clamped)
        ).astype(BF16)
        return carry

    lax.fori_loop(0, 4, expert_up, 0)
    loads[2].wait()

    def y_copy(t):
        return remote(ysend.at[t], yrecv.at[t], y_send.at[t], y_recv.at[t], (chip, other))

    def expert_down_far(t, carry):
        cols = pl.ds(pl.multiple_of(1024 * other + 256 * t, 256), 256)
        ysend[t] = jnp.dot(hbuf[...], edv[:, cols], preferred_element_type=F32).astype(BF16)
        y_copy(t).start()
        return carry

    def expert_down_near(t, carry):
        cols = pl.ds(pl.multiple_of(1024 * core + 256 * t, 256), 256)
        yown[t] = jnp.dot(hbuf[...], edv[:, cols], preferred_element_type=F32).astype(BF16)
        return carry

    lax.fori_loop(0, 4, expert_down_far, 0)
    lax.fori_loop(0, 4, expert_down_near, 0)

    for load in dense_loads:
        load.wait()

    def wait_da(index, carry):
        @pl.when(2 * index + core != plane)
        def _():
            da_recv_copy(index).wait_recv()
        return carry

    lax.fori_loop(0, 8, wait_da, 0)
    dense_rows = da[...].reshape(128, 2048)
    over_last = (((1,), (1,)), ((), ()))
    gate_rows = lax.dot_general(dense_rows, dgv[...].reshape(256, 2048), over_last, preferred_element_type=F32)
    lift_rows = lax.dot_general(dense_rows, duv[...].reshape(256, 2048), over_last, preferred_element_type=F32)
    activity = (gate_rows / (1.0 + jnp.exp(-gate_rows)) * lift_rows).astype(BF16)
    down = ddv[...].reshape(256, 2048)
    for h in range(2):
        for t in range(2):
            lower = 1024 * h + 512 * t
            part = jnp.dot(activity, down[:, lower:lower + 512], preferred_element_type=F32).astype(BF16)
            dout[h, :, 512 * t:512 * t + 512] = part

    def dr_copy(index, h):
        target = 2 * index + core
        return remote(
            dout.at[h, tile_rows(index), :], dr.at[plane], dr_send.at[2 * index + h], dr_recv.at[plane],
            (target * SIDE + x, h),
        )

    def start_dr(index, carry):
        for h in range(2):
            @pl.when((2 * index + core != plane) | (core != h))
            def _():
                dr_copy(index, h).start()
        return carry

    lax.fori_loop(0, 8, start_dr, 0)

    @pl.when(parity == core)
    def _():
        dr[plane] = dout[core, tile_rows(half), :]

    for t in range(4):
        y_copy(t).wait_recv()
    for g in range(4):
        rows = slice(32 * g, 32 * g + 32)
        stacked = []
        for t in range(4):
            both = (yown[t, rows, :].astype(F32) + yrecv[t, rows, :].astype(F32)).astype(BF16)
            stacked += [both[:, :128], both[:, 128:]]
        yret[256 * g:256 * g + 256, :] = jnp.dot(
            scatter, jnp.concatenate(stacked, axis=0), preferred_element_type=F32
        ).astype(BF16)

    def q_copy(step):
        peer = chip_shift(chip, step)
        return remote(
            yret.at[tile_rows(peer), :], rret.at[tile_rows(chip), :], q_send.at[step], q_recv.at[step], (peer, core)
        )

    def start_q(step, carry):
        q_copy(step).start()
        return carry

    lax.fori_loop(1, CHIPS, start_q, 0)
    rret[tile_rows(chip), :] = yret[tile_rows(chip), :]

    def dr_recv_copy(source):
        return remote(
            dout.at[0, pl.ds(0, ROWS), :], dr.at[source], dr_send.at[0], dr_recv.at[source], (chip, other)
        )

    def wait_dr(source, carry):
        @pl.when((source != plane) | (parity != core))
        def _():
            dr_recv_copy(source).wait_recv()
        return carry

    lax.fori_loop(0, PLANE, wait_dr, 0)
    branch = dr[0].astype(F32)
    for s in range(1, PLANE):
        branch = branch + dr[s].astype(F32)

    def wait_q(step, carry):
        q_copy(step).wait_recv()
        return carry

    lax.fori_loop(1, CHIPS, wait_q, 0)
    returned = rret[...]
    routed = jnp.dot(comb_hi[...], returned, preferred_element_type=F32) + jnp.dot(
        comb_lo[...], returned, preferred_element_type=F32
    )
    routed = jnp.concatenate([routed[16 * b:16 * b + 16, :] for b in range(8)], axis=1)
    own_cols = pl.ds(pl.multiple_of(1024 * core, 1024), 1024)
    out_ref[...] = (res[:, own_cols].astype(F32) + routed + branch * scale_ref[:, own_cols]).astype(BF16)

    for d in range(1, SIDE):
        gx_copy(d).wait_send()
    for d, side in tb_list:
        tb_copy(d, side).wait_send()

    def finish(step, carry):
        x_copy(step).wait_send()
        q_copy(step).wait_send()
        return carry

    lax.fori_loop(1, CHIPS, finish, 0)

    def finish_da(index, carry):
        da_send_copy(2 * index + core).wait_send()
        return carry

    lax.fori_loop(1 - core, 8, finish_da, 0)
    for t in range(4):
        y_copy(t).wait_send()

    def finish_dr(index, carry):
        for h in range(2):
            @pl.when((2 * index + core != plane) | (core != h))
            def _():
                dr_copy(index, h).wait_send()
        return carry

    lax.fori_loop(0, 8, finish_dr, 0)


def feed_forward(*operands):
    dma = pltpu.SemaphoreType.DMA
    vm = pltpu.VMEM
    return pl.pallas_call(
        expert_kernel,
        out_shape=jax.ShapeDtypeStruct((ROWS, 1024), BF16),
        in_specs=[VMEM_SPEC] * 6 + [ANY_SPEC] * 9 + [VMEM_SPEC],
        out_specs=VMEM_SPEC,
        scratch_shapes=[
            vm((2048, 1024), BF16), vm((2048, 1024), BF16), vm((1024, 2048), BF16),
            vm((8, 32, 2048), BF16), vm((8, 32, 2048), BF16), vm((8, 32, 2048), BF16),
            vm((64, 512), BF16), vm((64, 512), BF16), vm((2, 4, ROWS, 512), BF16),
            vm((ROWS, 2048), BF16), vm((ROWS, 2048), BF16), vm((128, 256), BF16),
            vm((1024, 128), BF16), vm((128, 1024), BF16), vm((128, 1024), BF16),
            vm((1024, 256), BF16), vm((1024, 256), BF16), vm((128, 2048), BF16), vm((128, 1024), BF16),
            vm((4, 128, 256), BF16), vm((4, 128, 256), BF16), vm((4, 128, 256), BF16),
            vm((1024, 128), BF16), vm((1024, 128), BF16),
            vm((8, ROWS, 2048), BF16), vm((2, 128, 1024), BF16), vm((PLANE, ROWS, 1024), BF16),
            dma((27,)),
            dma((4,)), dma((4,)),
            dma((8,)), dma((8,)),
            dma((64,)), dma((64,)),
            dma((16,)), dma((8,)),
            dma((4,)), dma((4,)),
            dma((64,)), dma((64,)),
            dma((16,)), dma((16,)),
        ],
        compiler_params=pltpu.CompilerParams(
            collective_id=1, has_side_effects=True, vmem_limit_bytes=VMEM_LIMIT
        ),
        name="feed_forward",
    )(*operands)


def body(
    tokens, norm_gain, query_weight, key_weight, value_weight, outgate_weight, input_weight, forget_weight,
    forget_bias, memory, stabilizer, head_gain, mix_weight, second_gain, route_experts, route_weight,
    expert_gate, expert_up, expert_down, dense_gate, dense_up, dense_down, branch_scale,
):
    rows, gates, mix_all, dg_all, du_all, dd_all = project(
        tokens, norm_gain.reshape(1, -1), query_weight, key_weight, value_weight, outgate_weight,
        input_weight.T, forget_weight.T, mix_weight.T, dense_gate, dense_up, dense_down,
    )
    gated, memory_new, stab_new = memory_step(rows, gates, forget_bias, memory, stabilizer, head_gain)
    mixed = feed_forward(
        gated, mix_all.reshape(512, 512), tokens, second_gain.reshape(1, -1), route_experts.T, route_weight.T,
        expert_gate, expert_up, expert_down, dense_gate, dense_up, dense_down, dg_all, du_all, dd_all,
        branch_scale.reshape(1, -1),
    )
    return mixed, memory_new, stab_new


def solution(mesh):
    in_specs = (
        P("ep", None), P(),
        P("ep", "tp"), P("ep", "tp"), P("ep", "tp"), P("ep", "tp"), P("ep", "tp"), P("ep", "tp"),
        P("tp"), P("ep", "tp", None, None), P("ep", "tp"), P("tp"), P("tp", "ep"), P(),
        P("ep", None), P("ep", None),
        P("ep", None, "tp"), P("ep", None, "tp"), P("ep", "tp", None),
        P(("ep", "tp"), None), P(("ep", "tp"), None), P(("ep", "tp"), None), P(),
    )
    out_specs = (P("ep", "tp"), P("ep", "tp", None, None), P("ep", "tp"))
    return jax.shard_map(body, mesh=mesh, in_specs=in_specs, out_specs=out_specs, check_vma=False)
```

```python
import jax
import jax.numpy as jnp
from jax import lax
from jax.experimental import pallas as pl
from jax.experimental.pallas import tpu as pltpu
from jax.sharding import PartitionSpec as P

norm_eps = 1e-05
clamp_limit = 7.0
sigmoid_slope = 1.702
F32 = jnp.float32
BF16 = jnp.bfloat16
MESH = pl.DeviceIdType.MESH
VMEM_SPEC = pl.BlockSpec(memory_space=pltpu.VMEM)
ANY_SPEC = pl.BlockSpec(memory_space=pl.ANY)
VMEM_LIMIT = 60 * 1024 * 1024

SIDE = 4
PLANE = 16
CHIPS = 64
ROWS = 16
SEQS = 2


def rms_scale(values, gain):
    mean_square = jnp.mean(values * values, axis=-1, keepdims=True)
    return values * lax.rsqrt(mean_square + norm_eps) * gain


def own_place():
    chip = lax.axis_index("ep")
    core = lax.axis_index("tp")
    return chip, core, chip % SIDE, chip // SIDE


def plane_shift(plane, step):
    z = (plane // SIDE + step // SIDE) % SIDE
    y = (plane % SIDE + step % SIDE) % SIDE
    return z * SIDE + y


def plane_back(plane, step):
    z = (plane // SIDE + SIDE - step // SIDE) % SIDE
    y = (plane % SIDE + SIDE - step % SIDE) % SIDE
    return z * SIDE + y


def chip_shift(chip, step):
    plane = plane_shift(chip // SIDE, step // SIDE)
    return plane * SIDE + (chip % SIDE + step % SIDE) % SIDE


def remote(src, dst, send, recv, device):
    return pltpu.make_async_remote_copy(
        src_ref=src, dst_ref=dst, send_sem=send, recv_sem=recv,
        device_id=device, device_id_type=MESH,
    )


def drain(ref, sem):
    pltpu.make_async_copy(ref, ref, sem).wait()


def projection_kernel(
    tok_ref, gain_ref, wq_ref, wk_ref, wv_ref, wo_ref, wi_ref, wf_ref, mix_ref, dg_ref, du_ref, dd_ref,
    rows_ref, gates_ref, mixall_ref, dgall_ref, duall_ref, ddall_ref,
    tokv, gainv, wiv, wfv, wbuf, gbuf, nbuf, abuf, pbuf, rbuf,
    load_sem, w_send, w_recv, g_send, g_recv, a_send, a_recv, m_send, m_recv, r_send, r_recv, d_send, d_recv,
):
    chip, core, x, plane = own_place()
    right = plane * SIDE + (x + 1) % SIDE
    left = plane * SIDE + (x + 3) % SIDE
    across = plane * SIDE + (x + 2) % SIDE
    xl, xr = (x + 3) % SIDE, (x + 1) % SIDE

    barrier = pltpu.get_barrier_semaphore()
    for peer in (right, left, across):
        pl.semaphore_signal(barrier, inc=1, device_id=(peer, core), device_id_type=MESH)

    def greet(step, carry):
        peer = plane_shift(plane, step) * SIDE + x
        pl.semaphore_signal(barrier, inc=1, device_id=(peer, core), device_id_type=MESH)
        return carry

    lax.fori_loop(1, PLANE, greet, 0)

    def w_rows(xs):
        return pl.ds(pl.multiple_of(32 * xs, 32), 32)

    def half_rows(xs, half):
        return pl.ds(pl.multiple_of(32 * xs + 16 * half, 16), 16)

    for k, ref in enumerate((wq_ref, wk_ref, wv_ref, wo_ref)):
        load = pltpu.make_async_copy(ref, wbuf.at[w_rows(x), pl.ds(512 * k, 512)], load_sem.at[0])
        load.start()
    small = [
        pltpu.make_async_copy(src, dst, load_sem.at[2 + k])
        for k, (src, dst) in enumerate(((tok_ref, tokv), (gain_ref, gainv), (wi_ref, wiv), (wf_ref, wfv)))
    ]
    for load in small:
        load.start()
    for load in small:
        load.wait()

    normed = rms_scale(tokv[...].astype(F32), gainv[...])
    nbuf[...] = normed.astype(BF16)
    place = (
        lax.broadcasted_iota(jnp.int32, (32, 128), 1) == lax.broadcasted_iota(jnp.int32, (32, 128), 0) + 32 * x
    ).astype(F32)
    gate_in = jnp.dot(wiv[...].astype(F32), place, preferred_element_type=F32)
    gate_fo = jnp.dot(wfv[...].astype(F32), place, preferred_element_type=F32)
    gbuf[x] = jnp.concatenate([gate_in, gate_fo], axis=0)
    drain(wbuf.at[w_rows(x), :], load_sem.at[0])
    pl.semaphore_wait(barrier, 3 + 15)

    def w_copy(kind, xs, part, device):
        rows = wbuf.at[half_rows(xs, part), :]
        return remote(rows, rows, w_send, w_recv.at[kind], (device, core))

    w_copy(0, x, 0, right).start()
    w_copy(1, x, 1, left).start()
    w_copy(2, x, 1, right).start()
    w_copy(3, x, 0, left).start()
    for peer in (right, left, across):
        remote(gbuf.at[x], gbuf.at[x], g_send, g_recv, (peer, core)).start()

    def token_copy(step):
        peer = plane_shift(plane, step)
        return remote(
            nbuf.at[:, pl.ds(pl.multiple_of(128 * peer, 128), 128)],
            abuf.at[pl.ds(pl.multiple_of(ROWS * plane, ROWS), ROWS), :],
            a_send, a_recv, (peer * SIDE + x, core),
        )

    def mix_copy(step):
        peer = plane_shift(plane, step)
        return remote(mix_ref, mixall_ref.at[plane], m_send, m_recv, (peer * SIDE + x, core))

    def start_tokens(step, carry):
        token_copy(step).start()
        return carry

    def start_mix(step, carry):
        mix_copy(step).start()
        return carry

    lax.fori_loop(1, PLANE, start_tokens, 0)
    abuf[pl.ds(pl.multiple_of(ROWS * plane, ROWS), ROWS), :] = nbuf[:, pl.ds(pl.multiple_of(128 * plane, 128), 128)]
    lax.fori_loop(1, PLANE, start_mix, 0)
    mix_own = pltpu.make_async_copy(mix_ref, mixall_ref.at[plane], load_sem.at[1])
    mix_own.start()

    dense = ((dg_ref, dgall_ref), (du_ref, duall_ref), (dd_ref, ddall_ref))

    def dense_copy(k, kind, xs, part, device):
        block = dense[k][1].at[xs]
        if part is not None:
            block = block.at[pl.ds(16 * part, 16)]
        source = dense[k][0] if kind in (0, 1) else block
        return remote(source, block, d_send.at[k], d_recv.at[kind], device)

    w_copy(0, x, 0, right).wait_recv()
    w_copy(4, xl, 0, right).start()
    w_copy(1, x, 1, left).wait_recv()
    w_copy(5, xr, 1, left).start()
    for k in range(3):
        dense_copy(k, 0, x, None, (right, core)).start()
        dense_copy(k, 1, x, None, (left, core)).start()
    drain(abuf.at[pl.ds(0, 240), :], a_recv)
    drain(gbuf.at[pl.ds(0, 3)], g_recv)
    gate_w = (gbuf[0] + gbuf[1] + gbuf[2] + gbuf[3]).astype(BF16)
    gate_w = jnp.concatenate([gate_w.astype(F32), jnp.zeros((120, 128), F32)], axis=0).astype(BF16)
    for kind in (2, 3, 4, 5):
        w_copy(kind, x, 0, right).wait_recv()

    def row_copy(step):
        peer = plane_shift(plane, step)
        return remote(
            pbuf.at[pl.ds(pl.multiple_of(ROWS * peer, ROWS), ROWS), :], rbuf.at[plane],
            r_send, r_recv, (peer * SIDE + x, core),
        )

    for dz in (2, 1, 3, 0):
        zt = (plane // SIDE + dz) % SIDE
        rows = pl.ds(pl.multiple_of(64 * zt, 64), 64)
        acts = abuf[rows, :]
        for k in range(4):
            cols = slice(512 * k, 512 * k + 512)
            pbuf[rows, cols] = jnp.dot(acts, wbuf[:, cols], preferred_element_type=F32).astype(BF16)
        gates = lax.dot_general(acts, gate_w, (((1,), (1,)), ((), ())), preferred_element_type=F32)
        high = gates.astype(BF16).astype(F32)
        pbuf[rows, 2048:2176] = (high + pltpu.roll(gates - high, 8, 1)).astype(BF16)
        for dy in (2, 1, 3, 0):
            if (dz, dy) != (0, 0):
                row_copy(dz * SIDE + dy).start()
    rbuf[plane] = pbuf[pl.ds(pl.multiple_of(ROWS * plane, ROWS), ROWS), :]

    three, threehalf = dgall_ref.at[pl.ds(0, 3)], dgall_ref.at[pl.ds(0, 3), pl.ds(0, 16)]
    drain(three, d_recv.at[0])
    for k in range(3):
        dense_copy(k, 2, xl, 0, (right, core)).start()
    drain(three, d_recv.at[1])
    for k in range(3):
        dense_copy(k, 3, xr, 1, (left, core)).start()

    drain(rbuf.at[pl.ds(0, 15)], r_recv)
    for k in range(4):
        cols = slice(512 * k, 512 * k + 512)
        total = rbuf[0, :, cols].astype(F32)
        for s in range(1, PLANE):
            total = total + rbuf[s, :, cols].astype(F32)
        rows_ref[:, cols] = total.astype(BF16)
    total = rbuf[0, :, 2048:2176].astype(F32)
    for s in range(1, PLANE):
        total = total + rbuf[s, :, 2048:2176].astype(F32)
    gates_ref[...] = total + pltpu.roll(total, 120, 1)

    drain(threehalf, d_recv.at[2])
    drain(threehalf, d_recv.at[3])

    drain(wbuf.at[pl.ds(0, 96), :], w_send)
    drain(gbuf.at[pl.ds(0, 3)], g_send)
    drain(abuf.at[pl.ds(0, 240), :], a_send)
    drain(mixall_ref.at[pl.ds(0, 15)], m_send)
    drain(rbuf.at[pl.ds(0, 15)], r_send)
    for k in range(3):
        drain(dense[k][1].at[pl.ds(0, 3)], d_send.at[k])
    drain(mixall_ref.at[pl.ds(0, 15)], m_recv)
    mix_own.wait()


def project(tokens, norm_gain, wq, wk, wv, wo, wi_t, wf_t, mix_t, dg, du, dd):
    dma = pltpu.SemaphoreType.DMA
    return pl.pallas_call(
        projection_kernel,
        out_shape=(
            jax.ShapeDtypeStruct((ROWS, 2048), BF16),
            jax.ShapeDtypeStruct((ROWS, 128), F32),
            jax.ShapeDtypeStruct((PLANE, 32, 512), BF16),
            jax.ShapeDtypeStruct((4, 32, 2048), BF16),
            jax.ShapeDtypeStruct((4, 32, 2048), BF16),
            jax.ShapeDtypeStruct((4, 32, 2048), BF16),
        ),
        in_specs=[ANY_SPEC] * 12,
        out_specs=(VMEM_SPEC, VMEM_SPEC, ANY_SPEC, ANY_SPEC, ANY_SPEC, ANY_SPEC),
        scratch_shapes=[
            pltpu.VMEM((ROWS, 2048), BF16),
            pltpu.VMEM((1, 2048), F32),
            pltpu.VMEM((4, 32), BF16),
            pltpu.VMEM((4, 32), BF16),
            pltpu.VMEM((128, 2048), BF16),
            pltpu.VMEM((4, 8, 128), F32),
            pltpu.VMEM((ROWS, 2048), BF16),
            pltpu.VMEM((256, 128), BF16),
            pltpu.VMEM((256, 2176), BF16),
            pltpu.VMEM((PLANE, ROWS, 2176), BF16),
            dma((6,)),
            dma, dma((6,)),
            dma, dma,
            dma, dma,
            dma, dma,
            dma, dma,
            dma((3,)), dma((4,)),
        ],
        compiler_params=pltpu.CompilerParams(
            collective_id=0, has_side_effects=True, vmem_limit_bytes=VMEM_LIMIT
        ),
        name="project",
    )(tokens, norm_gain, wq, wk, wv, wo, wi_t, wf_t, mix_t, dg, du, dd)


def memory_kernel(
    bias_ref, rows_ref, gates_ref, stab_ref, gain_ref, mem_ref,
    new_ref, stab_new_ref, gated_ref,
    carr, keys, queries, vt, rt,
):
    step = pl.program_id(0)
    over_last = (((1,), (1,)), ((), ()))
    exact = lax.Precision.HIGHEST

    def identity(n):
        row = lax.broadcasted_iota(jnp.int32, (n, n), 0)
        return (row == lax.broadcasted_iota(jnp.int32, (n, n), 1)).astype(F32)

    @pl.when(step == 0)
    def _():
        stab = lax.dot_general(
            identity(ROWS), stab_ref[...], over_last, preferred_element_type=F32, precision=exact
        )
        gates = gates_ref[...]
        input_pre = gates[:, 0:4]
        forget = pltpu.roll(gates, 124, 1)[:, 0:4] + bias_ref[...]
        log_forget = jnp.minimum(forget, 0.0) - jnp.log1p(jnp.exp(-jnp.abs(forget)))
        stab_new = jnp.maximum(log_forget + stab, input_pre)
        carried = jnp.exp(log_forget + stab - stab_new)
        written = jnp.exp(input_pre - stab_new)
        stab_new_ref[...] = lax.dot_general(
            identity(4), stab_new, over_last, preferred_element_type=F32, precision=exact
        )
        for h in range(4):
            carr[h] = jnp.broadcast_to(carried[:, h:h + 1], (ROWS, 128))
            query = rows_ref[:, 128 * h:128 * h + 128].astype(F32)
            queries[h] = jnp.concatenate([query, jnp.zeros((112, 128), F32)], axis=0).T.astype(BF16)
            key = rows_ref[:, 512 + 128 * h:512 + 128 * h + 128].astype(F32)
            keys[h] = key * (128 ** (-0.5)) * written[:, h:h + 1]
            value = rows_ref[:, 1024 + 128 * h:1024 + 128 * h + 128].astype(F32)
            vt[h] = jnp.concatenate([value, jnp.zeros((112, 128), F32)], axis=0).T
            rt[h] = jnp.zeros((128, 128), F32)

    lane = lax.broadcasted_iota(jnp.int32, (128, 128), 1)
    for h in range(4):
        values = vt[h]
        reads = rt[h]
        for j in range(SEQS):
            place = pl.ds(SEQS * step + j, 1)
            fresh = carr[h, place, :] * mem_ref[j, h] + values[:, j:j + 1] * keys[h, place, :]
            new_ref[j, h] = fresh
            read = jnp.dot(fresh.astype(BF16), queries[h], preferred_element_type=F32)
            reads = jnp.where(lane == SEQS * step + j, read, reads)
        rt[h] = reads
        vt[h] = pltpu.roll(values, 128 - SEQS, 1)

    @pl.when(step == ROWS // SEQS - 1)
    def _():
        for h in range(4):
            cols = slice(128 * h, 128 * h + 128)
            readout = rt[h].T[0:ROWS, :]
            gate = jax.nn.sigmoid(rows_ref[:, 1536 + 128 * h:1536 + 128 * h + 128].astype(F32))
            gated_ref[:, cols] = (rms_scale(readout, gain_ref[:, cols]) * gate).astype(BF16)


def memory_step(forget_bias, rows, gates, stabilizer_t, head_gain, memory):
    def whole(*shape):
        return pl.BlockSpec(shape, lambda i: (0,) * len(shape))

    block = pl.BlockSpec((SEQS, 4, 128, 128), lambda i: (i, 0, 0, 0))
    return pl.pallas_call(
        memory_kernel,
        grid=(ROWS // SEQS,),
        out_shape=(
            jax.ShapeDtypeStruct((ROWS, 4, 128, 128), F32),
            jax.ShapeDtypeStruct((4, ROWS), F32),
            jax.ShapeDtypeStruct((ROWS, 512), BF16),
        ),
        in_specs=[whole(1, 4), whole(ROWS, 2048), whole(ROWS, 128), whole(4, ROWS), whole(1, 512), block],
        out_specs=(block, whole(4, ROWS), whole(ROWS, 512)),
        scratch_shapes=[
            pltpu.VMEM((4, ROWS, 128), F32), pltpu.VMEM((4, ROWS, 128), F32), pltpu.VMEM((4, 128, 128), BF16),
            pltpu.VMEM((4, 128, 128), F32), pltpu.VMEM((4, 128, 128), F32),
        ],
        compiler_params=pltpu.CompilerParams(vmem_limit_bytes=VMEM_LIMIT),
        name="memory_update",
    )(forget_bias, rows, gates, stabilizer_t, head_gain, memory)


def expert_kernel(
    gated_hbm, mix_ref, tok_hbm, gain_hbm, route_hbm, weight_hbm, eg_ref, eu_ref, ed_ref,
    dg_ref, du_ref, dd_ref, dgall_ref, duall_ref, ddall_ref, scale_hbm,
    out_ref,
    gated_ref, tok_ref, gain_ref, route_ref, weight_ref, scale_ref,
    egv, euv, edv, dgv, duv, ddv, mixv, gx, asend, tb, ns, res, n2, sel, comb_hi, comb_lo, obuf, rx, xbuf, gacc, uacc, hbuf,
    yown, ysend, yrecv, yret, rret, da, dout, dr,
    load_sem, gx_send, gx_recv, tb_send, tb_recv, x_send, x_recv, da_send, da_recv,
    y_send, y_recv, q_send, q_recv, dr_send, dr_recv, xo_send, xo_recv, d_send, d_recv,
):
    chip, core, x, plane = own_place()
    other = 1 - core

    barrier = pltpu.get_barrier_semaphore()

    def greet(step, carry):
        peer = chip_shift(chip, step)
        pl.semaphore_signal(barrier, inc=1, device_id=(peer, core), device_id_type=MESH)
        return carry

    lax.fori_loop(1, CHIPS, greet, 0)
    pl.semaphore_signal(barrier, inc=1, device_id=(chip, other), device_id_type=MESH)

    def greet_plane(step, carry):
        peer = plane_shift(plane, step) * SIDE + x
        pl.semaphore_signal(barrier, inc=1, device_id=(peer, other), device_id_type=MESH)
        return carry

    lax.fori_loop(1, PLANE, greet_plane, 0)
    for d in range(1, SIDE):
        peer = plane * SIDE + (x + d) % SIDE
        pl.semaphore_signal(barrier, inc=1, device_id=(peer, other), device_id_type=MESH)

    loads = []
    for k, (src, dst) in enumerate(((eg_ref, egv), (eu_ref, euv), (ed_ref, edv))):
        loads.append(pltpu.make_async_copy(src.at[0], dst, load_sem.at[k]))
    dense_loads, dense_sends = [], []
    for k, (own, rest, dst) in enumerate(
        ((dg_ref, dgall_ref, dgv), (du_ref, duall_ref, duv), (dd_ref, ddall_ref, ddv))
    ):
        for s in range(SIDE):
            xs = (x + s) % SIDE
            src = rest.at[xs] if s else own
            slot = dst.at[2 * xs + core]
            dense_loads.append(pltpu.make_async_copy(src, slot, load_sem.at[3 + k]))
            dense_sends.append(remote(src, slot, d_send.at[k], d_recv.at[k], (chip, other)))
    small = [
        pltpu.make_async_copy(src, dst, load_sem.at[7 + k])
        for k, (src, dst) in enumerate((
            (route_hbm, route_ref), (weight_hbm, weight_ref), (gated_hbm, gated_ref), (tok_hbm, tok_ref),
            (gain_hbm, gain_ref), (scale_hbm, scale_ref),
        ))
    ]
    mix_load = pltpu.make_async_copy(mix_ref, mixv, load_sem.at[6])
    for load in small + [mix_load] + loads + dense_loads:
        load.start()
    for load in small:
        load.wait()

    spread = (
        lax.broadcasted_iota(jnp.int32, (ROWS, 128), 1) % ROWS == lax.broadcasted_iota(jnp.int32, (ROWS, 128), 0)
    ).astype(F32)
    route = jnp.dot(route_ref[...].astype(F32), spread, preferred_element_type=F32, precision=lax.Precision.HIGHEST)
    weight = jnp.dot(weight_ref[...], spread, preferred_element_type=F32, precision=lax.Precision.HIGHEST)
    expert = lax.broadcasted_iota(jnp.int32, (CHIPS, 128), 0).astype(F32)
    hit = jnp.zeros((CHIPS, 128), F32)
    chosen = jnp.zeros((CHIPS, 128), F32)
    for k in range(4):
        same = (route[k:k + 1, :] == expert).astype(F32)
        hit = hit + same
        chosen = chosen + same * weight[k:k + 1, :]
    col = lax.broadcasted_iota(jnp.int32, (128, 128), 1) % ROWS
    row = lax.broadcasted_iota(jnp.int32, (128, 128), 0)
    before = ((row < ROWS) & (row < col)).astype(F32)
    rank = jnp.dot(hit, before, preferred_element_type=F32)
    first = hit * (rank == 0.0).astype(F32)
    second = hit * (rank == 1.0).astype(F32)
    block_row = lax.broadcasted_iota(jnp.int32, (8, 128), 0)
    block_col = lax.broadcasted_iota(jnp.int32, (8, 128), 1) // ROWS
    diagonal = (block_row == block_col).astype(F32)

    def widened(top, bottom):
        low = top[:, None, :] * diagonal[None, :, :]
        high = bottom[:, None, :] * diagonal[None, :, :]
        return jnp.concatenate([low, high], axis=1).reshape(1024, 128)

    sel[...] = widened(first, second).astype(BF16)
    comb = widened(first * chosen, second * chosen).T
    comb_top = comb.astype(BF16)
    comb_hi[...] = comb_top
    comb_lo[...] = (comb - comb_top.astype(F32)).astype(BF16)
    gx[pl.ds(pl.multiple_of(ROWS * x, ROWS), ROWS), :] = gated_ref[...]

    pl.semaphore_wait(barrier, 63 + 1 + 15 + 3)

    def gx_copy(d):
        rows = pl.ds(pl.multiple_of(ROWS * x, ROWS), ROWS)
        peer = plane * SIDE + (x + d) % SIDE
        return remote(gated_ref, gx.at[rows, :], gx_send, gx_recv, (peer, core))

    for d in range(1, SIDE):
        gx_copy(d).start()
    for copy in dense_sends:
        copy.start()
    mix_load.wait()
    drain(gx.at[pl.ds(0, 48), :], gx_recv)
    asend[...] = lax.dot_general(
        gx[...], mixv[...], (((1,), (1,)), ((), ())), preferred_element_type=F32
    ).astype(BF16)

    def tb_copy(d, side):
        rows = pl.ds(pl.multiple_of(ROWS * ((x + d) % SIDE), ROWS), ROWS)
        peer = plane * SIDE + (x + d) % SIDE
        return remote(
            asend.at[rows, :], tb.at[core, x], tb_send, tb_recv,
            (peer, (core + side) % 2),
        )

    tb_list = [(0, 1)] + [(d, side) for d in (2, 1, 3) for side in (0, 1)]
    for d, side in tb_list:
        tb_copy(d, side).start()
    tb[core, x] = asend[pl.ds(pl.multiple_of(ROWS * x, ROWS), ROWS), :]
    tb_bytes = rx.at[pl.ds(0, 448), :]
    drain(tb_bytes, tb_recv)
    attended = [tb[0, k].astype(F32) + tb[1, k].astype(F32) for k in range(SIDE)]
    lane = lax.broadcasted_iota(jnp.int32, (ROWS, 128), 1) // 32
    tiles = []
    for t in range(PLANE):
        tile = None
        for k in range(SIDE):
            part = attended[k][:, 128 * (t // 4):128 * (t // 4) + 128]
            shift = (32 * k - 32 * (t % 4)) % 128
            if shift:
                part = pltpu.roll(part, shift, 1)
            tile = part if tile is None else jnp.where(lane == k, part, tile)
        tiles.append(tile)
    residual = (tok_ref[...].astype(F32) + jnp.concatenate(tiles, axis=1)).astype(BF16)
    res[...] = residual
    normed = rms_scale(residual.astype(F32), gain_ref[...]).astype(BF16)
    ns[...] = normed
    for b in range(8):
        cols = pl.ds(pl.multiple_of(1024 * core + 128 * b, 128), 128)
        n2[16 * b:16 * b + 16, :] = ns[:, cols]
    for k in range(4):
        obuf[256 * k:256 * k + 256, :] = jnp.dot(
            sel[256 * k:256 * k + 256, :], n2[...], preferred_element_type=F32
        ).astype(BF16)

    def tile_rows(index):
        return pl.ds(pl.multiple_of(ROWS * index, ROWS), ROWS)

    def x_copy(step):
        peer = chip_shift(chip, step)
        return remote(
            obuf.at[tile_rows(peer), :], rx.at[tile_rows(chip), :], x_send, x_recv, (peer, core)
        )

    def start_x(step, carry):
        x_copy(step).start()
        return carry

    lax.fori_loop(1, CHIPS, start_x, 0)
    rx[tile_rows(chip), :] = obuf[tile_rows(chip), :]

    parity = plane % 2
    half = plane // 2

    def da_send_copy(step):
        peer = plane_shift(plane, step)
        return remote(ns, da.at[half], da_send, da_recv, (peer * SIDE + x, parity))

    def start_da(index, carry):
        da_send_copy(2 * index + core).start()
        return carry

    lax.fori_loop(1 - core, 8, start_da, 0)

    @pl.when(parity == core)
    def _():
        da[half] = ns[...]

    drain(rx.at[pl.ds(0, 1008), :], x_recv)
    row = lax.broadcasted_iota(jnp.int32, (256, 256), 0)
    col = lax.broadcasted_iota(jnp.int32, (256, 256), 1)
    gather = (col == ((row % 32) // 2) * 16 + (row % 2) * 8 + row // 32).astype(F32).astype(BF16)
    scatter = (row == ((col % 32) // 2) * 16 + (col % 2) * 8 + col // 32).astype(F32).astype(BF16)
    for g in range(4):
        mixed_up = jnp.dot(gather, rx[256 * g:256 * g + 256, :], preferred_element_type=F32).astype(BF16)
        for b in range(8):
            xbuf[core, 32 * g:32 * g + 32, 128 * b:128 * b + 128] = mixed_up[32 * b:32 * b + 32, :]
    swap = remote(xbuf.at[core], xbuf.at[core], xo_send, xo_recv, (chip, other))
    swap.start()
    loads[0].wait()
    loads[1].wait()

    def expert_up_near(t, carry):
        cols = pl.ds(pl.multiple_of(256 * t, 256), 256)
        depth = pl.ds(pl.multiple_of(1024 * core, 1024), 1024)
        gacc[:, cols] = jnp.dot(xbuf[core], egv[depth, cols], preferred_element_type=F32)
        uacc[:, cols] = jnp.dot(xbuf[core], euv[depth, cols], preferred_element_type=F32)
        return carry

    def expert_up_far(t, carry):
        cols = pl.ds(pl.multiple_of(256 * t, 256), 256)
        depth = pl.ds(pl.multiple_of(1024 * other, 1024), 1024)
        gate_pre = gacc[:, cols] + jnp.dot(xbuf[other], egv[depth, cols], preferred_element_type=F32)
        up_pre = uacc[:, cols] + jnp.dot(xbuf[other], euv[depth, cols], preferred_element_type=F32)
        gate_clamped = jnp.minimum(gate_pre, clamp_limit)
        up_clamped = jnp.clip(up_pre, -clamp_limit, clamp_limit)
        hbuf[:, cols] = (
            (up_clamped + 1.0) * gate_clamped * jax.nn.sigmoid(sigmoid_slope * gate_clamped)
        ).astype(BF16)
        return carry

    lax.fori_loop(0, 4, expert_up_near, 0)
    swap.wait_recv()
    lax.fori_loop(0, 4, expert_up_far, 0)
    loads[2].wait()

    def y_copy(t):
        return remote(ysend.at[t], yrecv.at[t], y_send, y_recv, (chip, other))

    def expert_down_far(t, carry):
        cols = pl.ds(pl.multiple_of(1024 * other + 256 * t, 256), 256)
        ysend[t] = jnp.dot(hbuf[...], edv[:, cols], preferred_element_type=F32).astype(BF16)
        y_copy(t).start()
        return carry

    def expert_down_near(t, carry):
        cols = pl.ds(pl.multiple_of(1024 * core + 256 * t, 256), 256)
        yown[t] = jnp.dot(hbuf[...], edv[:, cols], preferred_element_type=F32).astype(BF16)
        return carry

    lax.fori_loop(0, 4, expert_down_far, 0)
    lax.fori_loop(0, 4, expert_down_near, 0)

    for k, dst in enumerate((dgv, duv, ddv)):
        drain(dst.at[pl.ds(0, 4)], load_sem.at[3 + k])
        drain(dst.at[pl.ds(0, 4)], d_recv.at[k])

    @pl.when(parity == core)
    def _():
        drain(da.at[pl.ds(0, 7)], da_recv)

    @pl.when(parity != core)
    def _():
        drain(da, da_recv)

    dense_rows = da[...].reshape(128, 2048)
    over_last = (((1,), (1,)), ((), ()))
    gate_rows = lax.dot_general(dense_rows, dgv[...].reshape(256, 2048), over_last, preferred_element_type=F32)
    lift_rows = lax.dot_general(dense_rows, duv[...].reshape(256, 2048), over_last, preferred_element_type=F32)
    activity = (gate_rows / (1.0 + jnp.exp(-gate_rows)) * lift_rows).astype(BF16)
    down = ddv[...].reshape(256, 2048)
    for h in range(2):
        for t in range(2):
            lower = 1024 * h + 512 * t
            part = jnp.dot(activity, down[:, lower:lower + 512], preferred_element_type=F32).astype(BF16)
            dout[h, :, 512 * t:512 * t + 512] = part

    def dr_copy(index, h):
        target = 2 * index + core
        return remote(
            dout.at[h, tile_rows(index), :], dr.at[plane], dr_send, dr_recv,
            (target * SIDE + x, h),
        )

    def start_dr(index, carry):
        for h in range(2):
            @pl.when((2 * index + core != plane) | (core != h))
            def _():
                dr_copy(index, h).start()
        return carry

    lax.fori_loop(0, 8, start_dr, 0)

    @pl.when(parity == core)
    def _():
        dr[plane] = dout[core, tile_rows(half), :]

    drain(yrecv, y_recv)
    for g in range(4):
        rows = slice(32 * g, 32 * g + 32)
        stacked = []
        for t in range(4):
            both = (yown[t, rows, :].astype(F32) + yrecv[t, rows, :].astype(F32)).astype(BF16)
            stacked += [both[:, :128], both[:, 128:]]
        yret[256 * g:256 * g + 256, :] = jnp.dot(
            scatter, jnp.concatenate(stacked, axis=0), preferred_element_type=F32
        ).astype(BF16)

    def q_copy(step):
        peer = chip_shift(chip, step)
        return remote(
            yret.at[tile_rows(peer), :], rret.at[tile_rows(chip), :], q_send, q_recv, (peer, core)
        )

    def start_q(step, carry):
        q_copy(step).start()
        return carry

    lax.fori_loop(1, CHIPS, start_q, 0)
    rret[tile_rows(chip), :] = yret[tile_rows(chip), :]

    @pl.when(parity == core)
    def _():
        drain(dr.at[pl.ds(0, 15)], dr_recv)

    @pl.when(parity != core)
    def _():
        drain(dr, dr_recv)

    branch = dr[0].astype(F32)
    for s in range(1, PLANE):
        branch = branch + dr[s].astype(F32)

    drain(rret.at[pl.ds(0, 1008), :], q_recv)
    returned = rret[...]
    routed = jnp.dot(comb_hi[...], returned, preferred_element_type=F32) + jnp.dot(
        comb_lo[...], returned, preferred_element_type=F32
    )
    routed = jnp.concatenate([routed[16 * b:16 * b + 16, :] for b in range(8)], axis=1)
    own_cols = pl.ds(pl.multiple_of(1024 * core, 1024), 1024)
    out_ref[...] = (res[:, own_cols].astype(F32) + routed + branch * scale_ref[:, own_cols]).astype(BF16)

    drain(gx.at[pl.ds(0, 48), :], gx_send)
    drain(tb_bytes, tb_send)
    drain(rx.at[pl.ds(0, 1008), :], x_send)
    drain(rret.at[pl.ds(0, 1008), :], q_send)
    drain(yrecv, y_send)
    drain(xbuf.at[0], xo_send)
    for k, dst in enumerate((dgv, duv, ddv)):
        drain(dst.at[pl.ds(0, 4)], d_send.at[k])

    @pl.when(core == 0)
    def _():
        drain(da.at[pl.ds(0, 7)], da_send)

    @pl.when(core != 0)
    def _():
        drain(da, da_send)

    @pl.when(parity == core)
    def _():
        drain(dr.at[pl.ds(0, 15)], dr_send)

    @pl.when(parity != core)
    def _():
        drain(dr, dr_send)


def feed_forward(*operands):
    dma = pltpu.SemaphoreType.DMA
    vm = pltpu.VMEM
    return pl.pallas_call(
        expert_kernel,
        out_shape=jax.ShapeDtypeStruct((ROWS, 1024), BF16),
        in_specs=[ANY_SPEC] * 16,
        out_specs=VMEM_SPEC,
        scratch_shapes=[
            vm((ROWS, 512), BF16), vm((ROWS, 2048), BF16), vm((1, 2048), F32),
            vm((4, ROWS), jnp.int32), vm((4, ROWS), F32), vm((1, 2048), F32),
            vm((2048, 1024), BF16), vm((2048, 1024), BF16), vm((1024, 2048), BF16),
            vm((8, 32, 2048), BF16), vm((8, 32, 2048), BF16), vm((8, 32, 2048), BF16),
            vm((512, 512), BF16),
            vm((64, 512), BF16), vm((64, 512), BF16), vm((2, 4, ROWS, 512), BF16),
            vm((ROWS, 2048), BF16), vm((ROWS, 2048), BF16), vm((128, 128), BF16),
            vm((1024, 128), BF16), vm((128, 1024), BF16), vm((128, 1024), BF16),
            vm((1024, 128), BF16), vm((1024, 128), BF16), vm((2, 128, 1024), BF16),
            vm((128, 1024), F32), vm((128, 1024), F32), vm((128, 1024), BF16),
            vm((4, 128, 256), BF16), vm((4, 128, 256), BF16), vm((4, 128, 256), BF16),
            vm((1024, 128), BF16), vm((1024, 128), BF16),
            vm((8, ROWS, 2048), BF16), vm((2, 128, 1024), BF16), vm((PLANE, ROWS, 1024), BF16),
            dma((13,)),
            dma, dma,
            dma, dma,
            dma, dma,
            dma, dma,
            dma, dma,
            dma, dma,
            dma, dma,
            dma, dma,
            dma((3,)), dma((3,)),
        ],
        compiler_params=pltpu.CompilerParams(
            collective_id=1, has_side_effects=True, vmem_limit_bytes=VMEM_LIMIT
        ),
        name="feed_forward",
    )(*operands)


def body(
    tokens, norm_gain, query_weight, key_weight, value_weight, outgate_weight, input_weight, forget_weight,
    forget_bias, memory, stabilizer, head_gain, mix_weight, second_gain, route_experts, route_weight,
    expert_gate, expert_up, expert_down, dense_gate, dense_up, dense_down, branch_scale,
):
    rows, gates, mix_all, dg_all, du_all, dd_all = project(
        tokens, norm_gain.reshape(1, -1), query_weight, key_weight, value_weight, outgate_weight,
        input_weight.T, forget_weight.T, mix_weight.T, dense_gate, dense_up, dense_down,
    )
    memory_new, stab_new, gated = memory_step(
        forget_bias.reshape(1, -1), rows, gates, stabilizer.T, head_gain.reshape(1, -1), memory
    )
    mixed = feed_forward(
        gated, mix_all.reshape(512, 512), tokens, second_gain.reshape(1, -1), route_experts.T, route_weight.T,
        expert_gate, expert_up, expert_down, dense_gate, dense_up, dense_down, dg_all, du_all, dd_all,
        branch_scale.reshape(1, -1),
    )
    return mixed, memory_new, stab_new.T


def solution(mesh):
    in_specs = (
        P("ep", None), P(),
        P("ep", "tp"), P("ep", "tp"), P("ep", "tp"), P("ep", "tp"), P("ep", "tp"), P("ep", "tp"),
        P("tp"), P("ep", "tp", None, None), P("ep", "tp"), P("tp"), P("tp", "ep"), P(),
        P("ep", None), P("ep", None),
        P("ep", None, "tp"), P("ep", None, "tp"), P("ep", "tp", None),
        P(("ep", "tp"), None), P(("ep", "tp"), None), P(("ep", "tp"), None), P(),
    )
    out_specs = (P("ep", "tp"), P("ep", "tp", None, None), P("ep", "tp"))
    return jax.shard_map(body, mesh=mesh, in_specs=in_specs, out_specs=out_specs, check_vma=False)
```

```python
import jax
import jax.numpy as jnp
from jax import lax
from jax.experimental import pallas as pl
from jax.experimental.pallas import tpu as pltpu
from jax.sharding import PartitionSpec as P

norm_eps = 1e-05
clamp_limit = 7.0
sigmoid_slope = 1.702
F32 = jnp.float32
BF16 = jnp.bfloat16
MESH = pl.DeviceIdType.MESH
VMEM_SPEC = pl.BlockSpec(memory_space=pltpu.VMEM)
ANY_SPEC = pl.BlockSpec(memory_space=pl.ANY)
VMEM_LIMIT = 60 * 1024 * 1024

SIDE = 4
PLANE = 16
CHIPS = 64
ROWS = 16
SEQS = 2


def rms_scale(values, gain):
    mean_square = jnp.mean(values * values, axis=-1, keepdims=True)
    return values * lax.rsqrt(mean_square + norm_eps) * gain


def own_place():
    chip = lax.axis_index("ep")
    core = lax.axis_index("tp")
    return chip, core, chip % SIDE, chip // SIDE


def plane_shift(plane, step):
    z = (plane // SIDE + step // SIDE) % SIDE
    y = (plane % SIDE + step % SIDE) % SIDE
    return z * SIDE + y


def each_chip(plane, x, act):
    xs = [(x + d) % SIDE for d in range(SIDE)]

    def on_plane(step, carry):
        base = plane_shift(plane, step) * SIDE
        for d in range(SIDE):
            act(base + xs[d])
        return carry

    lax.fori_loop(1, PLANE, on_plane, 0)
    for d in range(1, SIDE):
        act(plane * SIDE + xs[d])


def remote(src, dst, send, recv, device):
    return pltpu.make_async_remote_copy(
        src_ref=src, dst_ref=dst, send_sem=send, recv_sem=recv,
        device_id=device, device_id_type=MESH,
    )


def drain(ref, sem):
    pltpu.make_async_copy(ref, ref, sem).wait()


def projection_kernel(
    tok_ref, gain_ref, wq_ref, wk_ref, wv_ref, wo_ref, wi_ref, wf_ref, mix_ref, dg_ref, du_ref,
    rows_ref, gates_ref, mixall_ref, dgall_ref, duall_ref,
    tokv, gainv, wiv, wfv, wbuf, gbuf, nbuf, abuf, pbuf, sbuf, tbuf, rbuf,
    load_sem, w_send, w_recv, g_send, g_recv, a_send, a_recv, m_send, m_recv, p_send, p_recv, r_send, r_recv,
    d_send, d_recv,
):
    chip, core, x, plane = own_place()
    z, y = plane // SIDE, plane % SIDE
    right = plane * SIDE + (x + 1) % SIDE
    left = plane * SIDE + (x + 3) % SIDE
    across = plane * SIDE + (x + 2) % SIDE
    xl, xr = (x + 3) % SIDE, (x + 1) % SIDE

    barrier = pltpu.get_barrier_semaphore()
    for peer in (right, left, across):
        pl.semaphore_signal(barrier, inc=1, device_id=(peer, core), device_id_type=MESH)

    def greet(step, carry):
        peer = plane_shift(plane, step) * SIDE + x
        pl.semaphore_signal(barrier, inc=1, device_id=(peer, core), device_id_type=MESH)
        return carry

    lax.fori_loop(1, PLANE, greet, 0)

    def w_rows(xs):
        return pl.ds(pl.multiple_of(32 * xs, 32), 32)

    def half_rows(xs, half):
        return pl.ds(pl.multiple_of(32 * xs + 16 * half, 16), 16)

    for k, ref in enumerate((wq_ref, wk_ref, wv_ref, wo_ref)):
        load = pltpu.make_async_copy(ref, wbuf.at[w_rows(x), pl.ds(512 * k, 512)], load_sem.at[0])
        load.start()
    small = [
        pltpu.make_async_copy(src, dst, load_sem.at[2 + k])
        for k, (src, dst) in enumerate(((tok_ref, tokv), (gain_ref, gainv), (wi_ref, wiv), (wf_ref, wfv)))
    ]
    for load in small:
        load.start()
    for load in small:
        load.wait()

    normed = rms_scale(tokv[...].astype(F32), gainv[...])
    nbuf[...] = normed.astype(BF16)
    place = (
        lax.broadcasted_iota(jnp.int32, (32, 128), 1) == lax.broadcasted_iota(jnp.int32, (32, 128), 0) + 32 * x
    ).astype(F32)
    gate_in = jnp.dot(wiv[...].astype(F32), place, preferred_element_type=F32)
    gate_fo = jnp.dot(wfv[...].astype(F32), place, preferred_element_type=F32)
    gbuf[x] = jnp.concatenate([gate_in, gate_fo], axis=0)
    drain(wbuf.at[w_rows(x), :], load_sem.at[0])
    pl.semaphore_wait(barrier, 3 + 15)

    def w_copy(k, kind, xs, part, device):
        rows = w_rows(xs) if part is None else half_rows(xs, part)
        block = wbuf.at[rows, pl.ds(512 * k, 512)]
        return remote(block, block, w_send, w_recv.at[k, kind], (device, core))

    for k in range(4):
        w_copy(k, 0, x, None, right).start()
        w_copy(k, 1, x, None, left).start()
    for peer in (right, left, across):
        remote(gbuf.at[x], gbuf.at[x], g_send, g_recv, (peer, core)).start()

    def token_copy(step):
        peer = plane_shift(plane, step)
        return remote(
            nbuf.at[:, pl.ds(pl.multiple_of(128 * peer, 128), 128)],
            abuf.at[pl.ds(pl.multiple_of(ROWS * plane, ROWS), ROWS), :],
            a_send, a_recv, (peer * SIDE + x, core),
        )

    def plane_peer(axis, step):
        if axis == 0:
            return (z + step) % SIDE, y
        return z, (y + step) % SIDE

    def device_of(zt, yt):
        return ((zt * SIDE + yt) * SIDE + x, core)

    def mix_first(axis, step):
        part = pl.ds(16 * axis, 16)
        return remote(
            mix_ref.at[part], mixall_ref.at[z, y, part], m_send, m_recv.at[axis], device_of(*plane_peer(axis, step))
        )

    def mix_second(axis, step):
        part = pl.ds(16 * (1 - axis), 16)
        block = mixall_ref.at[z, :, part] if axis == 0 else mixall_ref.at[:, y, part]
        return remote(block, block, m_send, m_recv.at[2 + axis], device_of(*plane_peer(axis, step)))

    def start_tokens(step, carry):
        token_copy(step).start()
        return carry

    lax.fori_loop(1, PLANE, start_tokens, 0)
    abuf[pl.ds(pl.multiple_of(ROWS * plane, ROWS), ROWS), :] = nbuf[:, pl.ds(pl.multiple_of(128 * plane, 128), 128)]
    for axis in range(2):
        for d in (2, 1, 3):
            mix_first(axis, d).start()
    mix_own = pltpu.make_async_copy(mix_ref, mixall_ref.at[z, y], load_sem.at[1])
    mix_own.start()

    dense = ((dg_ref, dgall_ref), (du_ref, duall_ref))

    def dense_copy(k, kind, xs, part, device):
        block = dense[k][1].at[xs]
        if part is not None:
            block = block.at[pl.ds(16 * part, 16)]
        source = dense[k][0] if kind in (0, 1) else block
        return remote(source, block, d_send.at[k], d_recv.at[kind], device)

    def w_relay(k):
        w_copy(k, 0, x, None, right).wait_recv()
        w_copy(k, 2, xl, 0, right).start()
        w_copy(k, 1, x, None, left).wait_recv()
        w_copy(k, 3, xr, 1, left).start()

    for k in range(4):
        w_relay(k)
    for k in range(2):
        dense_copy(k, 0, x, None, (right, core)).start()
        dense_copy(k, 1, x, None, (left, core)).start()
    drain(abuf.at[pl.ds(0, 240), :], a_recv)
    drain(gbuf.at[pl.ds(0, 3)], g_recv)
    gate_w = (gbuf[0] + gbuf[1] + gbuf[2] + gbuf[3]).astype(BF16)
    gate_w = jnp.concatenate([gate_w.astype(F32), jnp.zeros((120, 128), F32)], axis=0).astype(BF16)
    def columns(k):
        return pl.ds(512 * k, 640 if k == 3 else 512)

    def first_sum(k, step):
        axis = (k + 1) % 2
        zt, yt = plane_peer(axis, step)
        src = pbuf.at[zt, :, :, columns(k)] if axis == 0 else pbuf.at[:, yt, :, columns(k)]
        own = z if axis == 0 else y
        return remote(src, sbuf.at[own, :, :, columns(k)], p_send, p_recv.at[k], device_of(zt, yt))

    def second_sum(k, step):
        axis = k % 2
        zt, yt = plane_peer(axis, step)
        target, own = (zt, z) if axis == 0 else (yt, y)
        return remote(
            tbuf.at[target, :, columns(k)], rbuf.at[own, :, columns(k)], r_send, r_recv.at[k], device_of(zt, yt)
        )

    for k in range(4):
        w_copy(k, 2, xl, 0, right).wait_recv()
        w_copy(k, 3, xr, 1, left).wait_recv()
        cols = slice(512 * k, 512 * k + 512)
        part = jnp.dot(abuf[...], wbuf[:, cols], preferred_element_type=F32).astype(BF16)
        pbuf[:, :, :, cols] = part.reshape(SIDE, SIDE, ROWS, 512)
        if k == 3:
            gates = lax.dot_general(abuf[...], gate_w, (((1,), (1,)), ((), ())), preferred_element_type=F32)
            high = gates.astype(BF16).astype(F32)
            part = (high + pltpu.roll(gates - high, 8, 1)).astype(BF16)
            pbuf[:, :, :, 2048:2176] = part.reshape(SIDE, SIDE, ROWS, 128)
        for d in (2, 1, 3):
            first_sum(k, d).start()
    mix_own.wait()
    for axis in range(2):
        drain(mixall_ref.at[0, pl.ds(0, 3), pl.ds(0, 16)], m_recv.at[1 - axis])
        for d in (2, 1, 3):
            mix_second(axis, d).start()
    first_lanes = lax.broadcasted_iota(jnp.int32, (ROWS, 128), 1) < 8
    for k in range(4):
        cols = slice(512 * k, 2176 if k == 3 else 512 * k + 512)
        if k % 2 == 0:
            sbuf[y, :, :, cols] = pbuf[:, y, :, cols]
        else:
            sbuf[z, :, :, cols] = pbuf[z, :, :, cols]
        drain(sbuf.at[pl.ds(0, 3), :, :, columns(k)], p_recv.at[k])
        for t in range(SIDE):
            total = sbuf[0, t, :, cols].astype(F32)
            for s in range(1, SIDE):
                total = total + sbuf[s, t, :, cols].astype(F32)
            if k == 3:
                gates = total[:, 512:640]
                gates = jnp.where(first_lanes, gates + pltpu.roll(gates, 120, 1), 0.0)
                high = gates.astype(BF16).astype(F32)
                total = jnp.concatenate([total[:, :512], high + pltpu.roll(gates - high, 8, 1)], axis=1)
            tbuf[t, :, cols] = total.astype(BF16)
        for d in (2, 1, 3):
            second_sum(k, d).start()
        if k % 2 == 0:
            rbuf[z, :, cols] = tbuf[z, :, cols]
        else:
            rbuf[y, :, cols] = tbuf[y, :, cols]

    two, twohalf = dgall_ref.at[pl.ds(0, 2)], dgall_ref.at[pl.ds(0, 2), pl.ds(0, 16)]
    drain(two, d_recv.at[0])
    for k in range(2):
        dense_copy(k, 2, xl, 0, (right, core)).start()
    drain(two, d_recv.at[1])
    for k in range(2):
        dense_copy(k, 3, xr, 1, (left, core)).start()
    for k in range(4):
        cols = slice(512 * k, 512 * k + 512)
        drain(rbuf.at[pl.ds(0, 3), :, columns(k)], r_recv.at[k])
        total = rbuf[0, :, cols].astype(F32)
        for s in range(1, SIDE):
            total = total + rbuf[s, :, cols].astype(F32)
        rows_ref[:, cols] = total.astype(BF16)
    total = rbuf[0, :, 2048:2176].astype(F32)
    for s in range(1, SIDE):
        total = total + rbuf[s, :, 2048:2176].astype(F32)
    gates_ref[...] = total + pltpu.roll(total, 120, 1)

    drain(twohalf, d_recv.at[2])
    drain(twohalf, d_recv.at[3])

    drain(wbuf.at[pl.ds(0, 96), :], w_send)
    drain(gbuf.at[pl.ds(0, 3)], g_send)
    drain(abuf.at[pl.ds(0, 240), :], a_send)
    drain(mixall_ref.at[pl.ds(0, 3), :, :], m_send)
    drain(mixall_ref.at[0, pl.ds(0, 3)], m_send)
    drain(sbuf.at[pl.ds(0, 3)], p_send)
    drain(rbuf.at[pl.ds(0, 3)], r_send)
    for k in range(2):
        drain(dense[k][1].at[pl.ds(0, 3)], d_send.at[k])
    for axis in range(2):
        drain(mixall_ref.at[pl.ds(0, 3), :, pl.ds(0, 16)], m_recv.at[2 + axis])


def project(tokens, norm_gain, wq, wk, wv, wo, wi_t, wf_t, mix_t, dg, du):
    dma = pltpu.SemaphoreType.DMA
    return pl.pallas_call(
        projection_kernel,
        out_shape=(
            jax.ShapeDtypeStruct((ROWS, 2048), BF16),
            jax.ShapeDtypeStruct((ROWS, 128), F32),
            jax.ShapeDtypeStruct((SIDE, SIDE, 32, 512), BF16),
            jax.ShapeDtypeStruct((4, 32, 2048), BF16),
            jax.ShapeDtypeStruct((4, 32, 2048), BF16),
        ),
        in_specs=[ANY_SPEC] * 11,
        out_specs=(VMEM_SPEC, VMEM_SPEC, ANY_SPEC, ANY_SPEC, ANY_SPEC),
        scratch_shapes=[
            pltpu.VMEM((ROWS, 2048), BF16),
            pltpu.VMEM((1, 2048), F32),
            pltpu.VMEM((4, 32), BF16),
            pltpu.VMEM((4, 32), BF16),
            pltpu.VMEM((128, 2048), BF16),
            pltpu.VMEM((4, 8, 128), F32),
            pltpu.VMEM((ROWS, 2048), BF16),
            pltpu.VMEM((256, 128), BF16),
            pltpu.VMEM((SIDE, SIDE, ROWS, 2176), BF16),
            pltpu.VMEM((SIDE, SIDE, ROWS, 2176), BF16),
            pltpu.VMEM((SIDE, ROWS, 2176), BF16),
            pltpu.VMEM((SIDE, ROWS, 2176), BF16),
            dma((6,)),
            dma, dma((4, 4)),
            dma, dma,
            dma, dma,
            dma, dma((4,)),
            dma, dma((4,)),
            dma, dma((4,)),
            dma((2,)), dma((4,)),
        ],
        compiler_params=pltpu.CompilerParams(
            collective_id=0, has_side_effects=True, vmem_limit_bytes=VMEM_LIMIT
        ),
        name="project",
    )(tokens, norm_gain, wq, wk, wv, wo, wi_t, wf_t, mix_t, dg, du)


def identity(n):
    row = lax.broadcasted_iota(jnp.int32, (n, n), 0)
    return (row == lax.broadcasted_iota(jnp.int32, (n, n), 1)).astype(F32)


def turned(values):
    rows = values.shape[0]
    return lax.dot_general(
        identity(values.shape[1]), values, (((1,), (1,)), ((), ())),
        preferred_element_type=F32, precision=lax.Precision.HIGHEST,
    ).reshape(values.shape[1], rows)


def memory_gates(gates, bias, stab_t):
    stab = turned(stab_t)
    input_pre = gates[:, 0:4]
    forget = pltpu.roll(gates, 124, 1)[:, 0:4] + bias
    log_forget = jnp.minimum(forget, 0.0) - jnp.log1p(jnp.exp(-jnp.abs(forget)))
    stab_new = jnp.maximum(log_forget + stab, input_pre)
    return stab_new, jnp.exp(log_forget + stab - stab_new), jnp.exp(input_pre - stab_new)


def head_cols(part, h):
    return slice(512 * part + 128 * h, 512 * part + 128 * h + 128)


def upright(rows):
    return jnp.concatenate([rows, jnp.zeros((112, 128), F32)], axis=0).T


def memory_kernel(
    carr_hbm, keys_hbm, vt_hbm, stab_hbm, mem_ref, mixed_hbm,
    new_ref, stab_new_ref, mixed_ref,
    memv, carr, keys, vt, small_sem, load_sem, store_sem,
):
    small = [
        pltpu.make_async_copy(src, dst, small_sem.at[k])
        for k, (src, dst) in enumerate((
            (carr_hbm, carr), (keys_hbm, keys), (vt_hbm, vt), (stab_hbm, stab_new_ref), (mixed_hbm, mixed_ref),
        ))
    ]
    for copy in small:
        copy.start()

    def part(i):
        return pl.ds(SEQS * i, SEQS)

    def load(i):
        return pltpu.make_async_copy(mem_ref.at[part(i)], memv.at[part(i)], load_sem.at[i])

    def store(i):
        return pltpu.make_async_copy(memv.at[part(i)], new_ref.at[part(i)], store_sem)

    for i in range(ROWS // SEQS):
        load(i).start()
    for copy in small:
        copy.wait()
    def advance(i, carry):
        load(i).wait()
        for h in range(4):
            values = vt[h]
            for j in range(SEQS):
                place = pl.ds(SEQS * i + j, 1)
                memv[SEQS * i + j, h] = (
                    carr[h, place, :] * memv[SEQS * i + j, h] + values[:, j:j + 1] * keys[h, place, :]
                )
            vt[h] = pltpu.roll(values, 128 - SEQS, 1)
        store(i).start()
        return carry

    lax.fori_loop(0, ROWS // SEQS, advance, 0)
    drain(memv, store_sem)


def memory_update(carried, keys, values, stab_new, memory, mixed):
    dma = pltpu.SemaphoreType.DMA
    vm = pltpu.VMEM
    return pl.pallas_call(
        memory_kernel,
        out_shape=(
            jax.ShapeDtypeStruct((ROWS, 4, 128, 128), F32),
            jax.ShapeDtypeStruct((4, ROWS), F32),
            jax.ShapeDtypeStruct((ROWS, 1024), BF16),
        ),
        in_specs=[ANY_SPEC] * 6,
        out_specs=(ANY_SPEC, VMEM_SPEC, VMEM_SPEC),
        scratch_shapes=[
            vm((ROWS, 4, 128, 128), F32), vm((4, ROWS, 128), F32), vm((4, ROWS, 128), F32), vm((4, 128, 128), F32),
            dma((5,)), dma((ROWS // SEQS,)), dma,
        ],
        compiler_params=pltpu.CompilerParams(vmem_limit_bytes=VMEM_LIMIT),
        name="memory_update",
    )(carried, keys, values, stab_new, memory, mixed)


def expert_kernel(
    mem_ref, rows_hbm, gates_hbm, bias_hbm, stab_hbm, hgain_hbm, mix_ref, tok_hbm, gain_hbm, route_hbm, weight_hbm, eg_ref, eu_ref, ed_ref,
    dg_ref, du_ref, dd_ref, dgall_ref, duall_ref, scale_hbm,
    out_ref, carr_ref, keys_ref, vt_ref, stab_new_ref,
    memv, rows_ref, gates_ref, bias_ref, stab_ref, hgain_ref, rt, queries, gated_ref,
    tok_ref, gain_ref, route_ref, weight_ref, scale_ref,
    egv, euv, edv, dgv, duv, ddv, mixv, gx, asend, tb, ns, res, n2, sel, comb_hi, comb_lo, obuf, rx, xbuf, gacc, uacc, hbuf,
    yown, ysend, yrecv, yret, rret, da, dout, dr,
    load_sem, gx_send, gx_recv, tb_send, tb_recv, x_send, x_recv, da_send, da_recv,
    y_send, y_recv, q_send, q_recv, dr_send, dr_recv, xo_send, xo_recv, d_send, d_recv, mem_sem, down_send, down_recv,
):
    chip, core, x, plane = own_place()
    other = 1 - core

    barrier = pltpu.get_barrier_semaphore()

    def greet(peer):
        pl.semaphore_signal(barrier, inc=1, device_id=(peer, core), device_id_type=MESH)

    each_chip(plane, x, greet)
    pl.semaphore_signal(barrier, inc=1, device_id=(chip, other), device_id_type=MESH)

    def greet_plane(step, carry):
        peer = plane_shift(plane, step) * SIDE + x
        pl.semaphore_signal(barrier, inc=1, device_id=(peer, other), device_id_type=MESH)
        return carry

    lax.fori_loop(1, PLANE, greet_plane, 0)
    for d in range(1, SIDE):
        peer = plane * SIDE + (x + d) % SIDE
        pl.semaphore_signal(barrier, inc=1, device_id=(peer, other), device_id_type=MESH)

    loads = []
    for k, (src, dst) in enumerate(((eg_ref, egv), (eu_ref, euv), (ed_ref, edv))):
        loads.append(pltpu.make_async_copy(src.at[0], dst, load_sem.at[k]))
    dense_loads, dense_sends = [], []
    for k, (own, rest, dst) in enumerate(
        ((dg_ref, dgall_ref, dgv), (du_ref, duall_ref, duv), (dd_ref, None, ddv))
    ):
        for s in range(SIDE if k < 2 else 1):
            xs = (x + s) % SIDE
            src = rest.at[xs] if s else own
            slot = dst.at[2 * xs + core]
            dense_loads.append(pltpu.make_async_copy(src, slot, load_sem.at[3 + k]))
            dense_sends.append(remote(src, slot, d_send.at[k], d_recv.at[k], (chip, other)))
    small = [
        pltpu.make_async_copy(src, dst, load_sem.at[7 + k])
        for k, (src, dst) in enumerate((
            (rows_hbm, rows_ref), (gates_hbm, gates_ref), (bias_hbm, bias_ref), (stab_hbm, stab_ref),
            (hgain_hbm, hgain_ref), (route_hbm, route_ref), (weight_hbm, weight_ref), (tok_hbm, tok_ref),
            (gain_hbm, gain_ref), (scale_hbm, scale_ref),
        ))
    ]
    mix_load = pltpu.make_async_copy(mix_ref, mixv, load_sem.at[6])
    def mem_load(i):
        part = pl.ds(4 * i, 4)
        return pltpu.make_async_copy(mem_ref.at[part], memv.at[part], mem_sem.at[i])

    for load in small:
        load.start()
    for i in range(4):
        mem_load(i).start()
    mix_load.start()
    for load in small:
        load.wait()

    stab_new, carried, written = memory_gates(gates_ref[...], bias_ref[...], stab_ref[...])
    stab_new_ref[...] = turned(stab_new)
    for h in range(4):
        query = upright(rows_ref[:, head_cols(0, h)].astype(F32)).astype(BF16)
        queries[h] = jnp.concatenate([query, query], axis=0)
    lane_index = lax.broadcasted_iota(jnp.int32, (128, 128), 1)

    def read_part(i, carry):
        mem_load(i).wait()
        for h in range(4):
            stored = memv[pl.ds(4 * i, 4), h].reshape(512, 128)
            top = stored.astype(BF16)
            rest = (stored - top.astype(F32)).astype(BF16)
            read = jnp.dot(jnp.concatenate([top, rest], axis=1), queries[h], preferred_element_type=F32)
            reads = rt[h]
            for j in range(4):
                reads = jnp.where(lane_index == 4 * i + j, read[128 * j:128 * j + 128, :], reads)
            rt[h] = reads
        return carry

    rt[...] = jnp.zeros(rt.shape, F32)
    lax.fori_loop(0, 4, read_part, 0)
    for load in dense_loads + loads:
        load.start()
    for h in range(4):
        query = rows_ref[:, head_cols(0, h)].astype(F32)
        key = rows_ref[:, head_cols(1, h)].astype(F32) * (128 ** (-0.5))
        value = rows_ref[:, head_cols(2, h)].astype(F32)
        match = jnp.sum(key * query, axis=1, keepdims=True) * written[:, h:h + 1]
        carr_ref[h] = jnp.broadcast_to(carried[:, h:h + 1], (ROWS, 128))
        keys_ref[h] = key * written[:, h:h + 1]
        vt_ref[h] = upright(value)
        readout = carried[:, h:h + 1] * rt[h].T[0:ROWS, :] + match * value
        gate = jax.nn.sigmoid(rows_ref[:, head_cols(3, h)].astype(F32))
        scaled = rms_scale(readout, hgain_ref[:, head_cols(0, h)])
        gated_ref[:, head_cols(0, h)] = (scaled * gate).astype(BF16)

    spread = (
        lax.broadcasted_iota(jnp.int32, (ROWS, 128), 1) % ROWS == lax.broadcasted_iota(jnp.int32, (ROWS, 128), 0)
    ).astype(F32)
    route = jnp.dot(route_ref[...].astype(F32), spread, preferred_element_type=F32, precision=lax.Precision.HIGHEST)
    weight = jnp.dot(weight_ref[...], spread, preferred_element_type=F32, precision=lax.Precision.HIGHEST)
    expert = lax.broadcasted_iota(jnp.int32, (CHIPS, 128), 0).astype(F32)
    hit = jnp.zeros((CHIPS, 128), F32)
    chosen = jnp.zeros((CHIPS, 128), F32)
    for k in range(4):
        same = (route[k:k + 1, :] == expert).astype(F32)
        hit = hit + same
        chosen = chosen + same * weight[k:k + 1, :]
    col = lax.broadcasted_iota(jnp.int32, (128, 128), 1) % ROWS
    row = lax.broadcasted_iota(jnp.int32, (128, 128), 0)
    before = ((row < ROWS) & (row < col)).astype(F32)
    rank = jnp.dot(hit, before, preferred_element_type=F32)
    first = hit * (rank == 0.0).astype(F32)
    second = hit * (rank == 1.0).astype(F32)
    block_row = lax.broadcasted_iota(jnp.int32, (8, 128), 0)
    block_col = lax.broadcasted_iota(jnp.int32, (8, 128), 1) // ROWS
    diagonal = (block_row == block_col).astype(F32)

    def widened(top, bottom):
        low = top[:, None, :] * diagonal[None, :, :]
        high = bottom[:, None, :] * diagonal[None, :, :]
        return jnp.concatenate([low, high], axis=1).reshape(1024, 128)

    sel[...] = widened(first, second).astype(BF16)
    comb = widened(first * chosen, second * chosen).T
    comb_top = comb.astype(BF16)
    comb_hi[...] = comb_top
    comb_lo[...] = (comb - comb_top.astype(F32)).astype(BF16)
    gx[pl.ds(pl.multiple_of(ROWS * x, ROWS), ROWS), :] = gated_ref[...]

    pl.semaphore_wait(barrier, 63 + 1 + 15 + 3)

    def gx_copy(d):
        rows = pl.ds(pl.multiple_of(ROWS * x, ROWS), ROWS)
        peer = plane * SIDE + (x + d) % SIDE
        return remote(gated_ref, gx.at[rows, :], gx_send, gx_recv, (peer, core))

    for d in range(1, SIDE):
        gx_copy(d).start()
    def down_copy(kind, xs, part, device):
        block = ddv.at[2 * xs + core]
        if part is not None:
            block = block.at[pl.ds(16 * part, 16)]
        if kind == 4:
            return remote(block, block, d_send.at[2], d_recv.at[2], (chip, other))
        return remote(dd_ref if kind < 2 else block, block, down_send, down_recv.at[kind], (device, core))

    right, left = plane * SIDE + (x + 1) % SIDE, plane * SIDE + (x + 3) % SIDE
    xl, xr, xa = (x + 3) % SIDE, (x + 1) % SIDE, (x + 2) % SIDE
    mix_load.wait()
    drain(gx.at[pl.ds(0, 48), :], gx_recv)
    asend[...] = lax.dot_general(
        gx[...], mixv[...], (((1,), (1,)), ((), ())), preferred_element_type=F32
    ).astype(BF16)

    def tb_copy(d, side):
        rows = pl.ds(pl.multiple_of(ROWS * ((x + d) % SIDE), ROWS), ROWS)
        peer = plane * SIDE + (x + d) % SIDE
        return remote(
            asend.at[rows, :], tb.at[core, x], tb_send, tb_recv,
            (peer, (core + side) % 2),
        )

    tb_list = [(0, 1)] + [(d, side) for d in (2, 1, 3) for side in (0, 1)]
    for d, side in tb_list:
        tb_copy(d, side).start()
    tb[core, x] = asend[pl.ds(pl.multiple_of(ROWS * x, ROWS), ROWS), :]
    down_copy(0, x, None, right).start()
    down_copy(1, x, None, left).start()
    for copy in dense_sends:
        copy.start()
    tb_bytes = rx.at[pl.ds(0, 448), :]
    drain(tb_bytes, tb_recv)
    attended = [tb[0, k].astype(F32) + tb[1, k].astype(F32) for k in range(SIDE)]
    lane = lax.broadcasted_iota(jnp.int32, (ROWS, 128), 1) // 32
    tiles = []
    for t in range(PLANE):
        tile = None
        for k in range(SIDE):
            part = attended[k][:, 128 * (t // 4):128 * (t // 4) + 128]
            shift = (32 * k - 32 * (t % 4)) % 128
            if shift:
                part = pltpu.roll(part, shift, 1)
            tile = part if tile is None else jnp.where(lane == k, part, tile)
        tiles.append(tile)
    residual = (tok_ref[...].astype(F32) + jnp.concatenate(tiles, axis=1)).astype(BF16)
    res[...] = residual
    normed = rms_scale(residual.astype(F32), gain_ref[...]).astype(BF16)
    ns[...] = normed
    def tile_rows(index):
        return pl.ds(pl.multiple_of(ROWS * index, ROWS), ROWS)

    parity = plane % 2
    half = plane // 2

    def da_send_copy(step):
        peer = plane_shift(plane, step)
        return remote(ns, da.at[half], da_send, da_recv, (peer * SIDE + x, parity))

    def start_da(index, carry):
        da_send_copy(2 * index + core).start()
        return carry

    lax.fori_loop(1 - core, 8, start_da, 0)

    @pl.when(parity == core)
    def _():
        da[half] = ns[...]

    for b in range(8):
        cols = pl.ds(pl.multiple_of(1024 * core + 128 * b, 128), 128)
        n2[16 * b:16 * b + 16, :] = ns[:, cols]
    for k in range(4):
        obuf[256 * k:256 * k + 256, :] = jnp.dot(
            sel[256 * k:256 * k + 256, :], n2[...], preferred_element_type=F32
        ).astype(BF16)

    def x_copy(peer):
        return remote(
            obuf.at[tile_rows(peer), :], rx.at[tile_rows(chip), :], x_send, x_recv, (peer, core)
        )

    each_chip(plane, x, lambda peer: x_copy(peer).start())
    rx[tile_rows(chip), :] = obuf[tile_rows(chip), :]

    down_copy(0, x, None, right).wait_recv()
    down_copy(2, xl, 0, right).start()
    down_copy(1, x, None, left).wait_recv()
    down_copy(3, xr, 1, left).start()
    down_copy(4, xl, None, chip).start()
    down_copy(4, xr, None, chip).start()
    for k, dst in enumerate((dgv, duv)):
        drain(dst.at[pl.ds(0, 4)], load_sem.at[3 + k])
        drain(dst.at[pl.ds(0, 4)], d_recv.at[k])

    @pl.when(parity == core)
    def _():
        drain(da.at[pl.ds(0, 7)], da_recv)

    @pl.when(parity != core)
    def _():
        drain(da, da_recv)

    down_copy(2, xa, 0, right).wait_recv()
    down_copy(3, xa, 1, left).wait_recv()
    down_copy(4, xa, None, chip).start()
    dense_rows = da[...].reshape(128, 2048)
    over_last = (((1,), (1,)), ((), ()))
    gate_rows = lax.dot_general(dense_rows, dgv[...].reshape(256, 2048), over_last, preferred_element_type=F32)
    lift_rows = lax.dot_general(dense_rows, duv[...].reshape(256, 2048), over_last, preferred_element_type=F32)
    activity = (gate_rows / (1.0 + jnp.exp(-gate_rows)) * lift_rows).astype(BF16)
    drain(ddv.at[pl.ds(0, 1)], load_sem.at[5])
    drain(ddv.at[pl.ds(0, 4)], d_recv.at[2])
    down = ddv[...].reshape(256, 2048)
    for h in range(2):
        for t in range(2):
            lower = 1024 * h + 512 * t
            part = jnp.dot(activity, down[:, lower:lower + 512], preferred_element_type=F32).astype(BF16)
            dout[h, :, 512 * t:512 * t + 512] = part

    def dr_copy(index, h):
        target = 2 * index + core
        return remote(
            dout.at[h, tile_rows(index), :], dr.at[plane], dr_send, dr_recv,
            (target * SIDE + x, h),
        )

    def start_dr(index, carry):
        for h in range(2):
            @pl.when((2 * index + core != plane) | (core != h))
            def _():
                dr_copy(index, h).start()
        return carry

    lax.fori_loop(0, 8, start_dr, 0)

    @pl.when(parity == core)
    def _():
        dr[plane] = dout[core, tile_rows(half), :]

    drain(rx.at[pl.ds(0, 1008), :], x_recv)
    row = lax.broadcasted_iota(jnp.int32, (256, 256), 0)
    col = lax.broadcasted_iota(jnp.int32, (256, 256), 1)
    gather = (col == ((row % 32) // 2) * 16 + (row % 2) * 8 + row // 32).astype(F32).astype(BF16)
    scatter = (row == ((col % 32) // 2) * 16 + (col % 2) * 8 + col // 32).astype(F32).astype(BF16)
    for g in range(4):
        mixed_up = jnp.dot(gather, rx[256 * g:256 * g + 256, :], preferred_element_type=F32).astype(BF16)
        for b in range(8):
            xbuf[core, 32 * g:32 * g + 32, 128 * b:128 * b + 128] = mixed_up[32 * b:32 * b + 32, :]
    swap = remote(xbuf.at[core], xbuf.at[core], xo_send, xo_recv, (chip, other))
    swap.start()
    loads[0].wait()
    loads[1].wait()

    def expert_up_near(t, carry):
        cols = pl.ds(pl.multiple_of(256 * t, 256), 256)
        depth = pl.ds(pl.multiple_of(1024 * core, 1024), 1024)
        gacc[:, cols] = jnp.dot(xbuf[core], egv[depth, cols], preferred_element_type=F32)
        uacc[:, cols] = jnp.dot(xbuf[core], euv[depth, cols], preferred_element_type=F32)
        return carry

    def expert_up_far(t, carry):
        cols = pl.ds(pl.multiple_of(256 * t, 256), 256)
        depth = pl.ds(pl.multiple_of(1024 * other, 1024), 1024)
        gate_pre = gacc[:, cols] + jnp.dot(xbuf[other], egv[depth, cols], preferred_element_type=F32)
        up_pre = uacc[:, cols] + jnp.dot(xbuf[other], euv[depth, cols], preferred_element_type=F32)
        gate_clamped = jnp.minimum(gate_pre, clamp_limit)
        up_clamped = jnp.clip(up_pre, -clamp_limit, clamp_limit)
        hbuf[:, cols] = (
            (up_clamped + 1.0) * gate_clamped * jax.nn.sigmoid(sigmoid_slope * gate_clamped)
        ).astype(BF16)
        return carry

    lax.fori_loop(0, 4, expert_up_near, 0)
    swap.wait_recv()
    lax.fori_loop(0, 4, expert_up_far, 0)
    loads[2].wait()

    def y_copy(t):
        return remote(ysend.at[t], yrecv.at[t], y_send, y_recv, (chip, other))

    def expert_down_far(t, carry):
        cols = pl.ds(pl.multiple_of(1024 * other + 256 * t, 256), 256)
        ysend[t] = jnp.dot(hbuf[...], edv[:, cols], preferred_element_type=F32).astype(BF16)
        y_copy(t).start()
        return carry

    def expert_down_near(t, carry):
        cols = pl.ds(pl.multiple_of(1024 * core + 256 * t, 256), 256)
        yown[t] = jnp.dot(hbuf[...], edv[:, cols], preferred_element_type=F32).astype(BF16)
        return carry

    lax.fori_loop(0, 4, expert_down_far, 0)
    lax.fori_loop(0, 4, expert_down_near, 0)

    drain(yrecv, y_recv)
    for g in range(4):
        rows = slice(32 * g, 32 * g + 32)
        stacked = []
        for t in range(4):
            both = (yown[t, rows, :].astype(F32) + yrecv[t, rows, :].astype(F32)).astype(BF16)
            stacked += [both[:, :128], both[:, 128:]]
        yret[256 * g:256 * g + 256, :] = jnp.dot(
            scatter, jnp.concatenate(stacked, axis=0), preferred_element_type=F32
        ).astype(BF16)

    def q_copy(peer):
        return remote(
            yret.at[tile_rows(peer), :], rret.at[tile_rows(chip), :], q_send, q_recv, (peer, core)
        )

    each_chip(plane, x, lambda peer: q_copy(peer).start())
    rret[tile_rows(chip), :] = yret[tile_rows(chip), :]

    @pl.when(parity == core)
    def _():
        drain(dr.at[pl.ds(0, 15)], dr_recv)

    @pl.when(parity != core)
    def _():
        drain(dr, dr_recv)

    branch = dr[0].astype(F32)
    for s in range(1, PLANE):
        branch = branch + dr[s].astype(F32)

    drain(rret.at[pl.ds(0, 1008), :], q_recv)
    returned = rret[...]
    routed = jnp.dot(comb_hi[...], returned, preferred_element_type=F32) + jnp.dot(
        comb_lo[...], returned, preferred_element_type=F32
    )
    routed = jnp.concatenate([routed[16 * b:16 * b + 16, :] for b in range(8)], axis=1)
    own_cols = pl.ds(pl.multiple_of(1024 * core, 1024), 1024)
    out_ref[...] = (res[:, own_cols].astype(F32) + routed + branch * scale_ref[:, own_cols]).astype(BF16)

    drain(gx.at[pl.ds(0, 48), :], gx_send)
    drain(tb_bytes, tb_send)
    drain(rx.at[pl.ds(0, 1008), :], x_send)
    drain(rret.at[pl.ds(0, 1008), :], q_send)
    drain(yrecv, y_send)
    drain(xbuf.at[0], xo_send)
    for k, dst in enumerate((dgv, duv, ddv)):
        drain(dst.at[pl.ds(0, 4)], d_send.at[k])
    drain(ddv.at[pl.ds(0, 3)], down_send)

    @pl.when(core == 0)
    def _():
        drain(da.at[pl.ds(0, 7)], da_send)

    @pl.when(core != 0)
    def _():
        drain(da, da_send)

    @pl.when(parity == core)
    def _():
        drain(dr.at[pl.ds(0, 15)], dr_send)

    @pl.when(parity != core)
    def _():
        drain(dr, dr_send)


def feed_forward(*operands):
    dma = pltpu.SemaphoreType.DMA
    vm = pltpu.VMEM
    return pl.pallas_call(
        expert_kernel,
        out_shape=(
            jax.ShapeDtypeStruct((ROWS, 1024), BF16),
            jax.ShapeDtypeStruct((4, ROWS, 128), F32),
            jax.ShapeDtypeStruct((4, ROWS, 128), F32),
            jax.ShapeDtypeStruct((4, 128, 128), F32),
            jax.ShapeDtypeStruct((4, ROWS), F32),
        ),
        in_specs=[ANY_SPEC] * 20,
        out_specs=(VMEM_SPEC,) * 5,
        scratch_shapes=[
            vm((ROWS, 4, 128, 128), F32), vm((ROWS, 2048), BF16), vm((ROWS, 128), F32), vm((1, 4), F32),
            vm((4, ROWS), F32), vm((1, 512), F32), vm((4, 128, 128), F32), vm((4, 256, 128), BF16),
            vm((ROWS, 512), BF16), vm((ROWS, 2048), BF16), vm((1, 2048), F32),
            vm((4, ROWS), jnp.int32), vm((4, ROWS), F32), vm((1, 2048), F32),
            vm((2048, 1024), BF16), vm((2048, 1024), BF16), vm((1024, 2048), BF16),
            vm((8, 32, 2048), BF16), vm((8, 32, 2048), BF16), vm((8, 32, 2048), BF16),
            vm((512, 512), BF16),
            vm((64, 512), BF16), vm((64, 512), BF16), vm((2, 4, ROWS, 512), BF16),
            vm((ROWS, 2048), BF16), vm((ROWS, 2048), BF16), vm((128, 128), BF16),
            vm((1024, 128), BF16), vm((128, 1024), BF16), vm((128, 1024), BF16),
            vm((1024, 128), BF16), vm((1024, 128), BF16), vm((2, 128, 1024), BF16),
            vm((128, 1024), F32), vm((128, 1024), F32), vm((128, 1024), BF16),
            vm((4, 128, 256), BF16), vm((4, 128, 256), BF16), vm((4, 128, 256), BF16),
            vm((1024, 128), BF16), vm((1024, 128), BF16),
            vm((8, ROWS, 2048), BF16), vm((2, 128, 1024), BF16), vm((PLANE, ROWS, 1024), BF16),
            dma((17,)),
            dma, dma,
            dma, dma,
            dma, dma,
            dma, dma,
            dma, dma,
            dma, dma,
            dma, dma,
            dma, dma,
            dma((3,)), dma((3,)),
            dma((4,)),
            dma, dma((4,)),
        ],
        compiler_params=pltpu.CompilerParams(
            collective_id=1, has_side_effects=True, vmem_limit_bytes=VMEM_LIMIT
        ),
        name="feed_forward",
    )(*operands)


def body(
    tokens, norm_gain, query_weight, key_weight, value_weight, outgate_weight, input_weight, forget_weight,
    forget_bias, memory, stabilizer, head_gain, mix_weight, second_gain, route_experts, route_weight,
    expert_gate, expert_up, expert_down, dense_gate, dense_up, dense_down, branch_scale,
):
    rows, gates, mix_all, dg_all, du_all = project(
        tokens, norm_gain.reshape(1, -1), query_weight, key_weight, value_weight, outgate_weight,
        input_weight.T, forget_weight.T, mix_weight.T, dense_gate, dense_up,
    )
    bias, stab_t = forget_bias.reshape(1, -1), stabilizer.T
    mixed, carried, keys, values, stab_new = feed_forward(
        memory, rows, gates, bias, stab_t, head_gain.reshape(1, -1), mix_all.reshape(512, 512), tokens, second_gain.reshape(1, -1), route_experts.T, route_weight.T,
        expert_gate, expert_up, expert_down, dense_gate, dense_up, dense_down, dg_all, du_all,
        branch_scale.reshape(1, -1),
    )
    memory_new, stab_new, mixed = memory_update(carried, keys, values, stab_new, memory, mixed)
    return mixed, memory_new, stab_new.T


def solution(mesh):
    in_specs = (
        P("ep", None), P(),
        P("ep", "tp"), P("ep", "tp"), P("ep", "tp"), P("ep", "tp"), P("ep", "tp"), P("ep", "tp"),
        P("tp"), P("ep", "tp", None, None), P("ep", "tp"), P("tp"), P("tp", "ep"), P(),
        P("ep", None), P("ep", None),
        P("ep", None, "tp"), P("ep", None, "tp"), P("ep", "tp", None),
        P(("ep", "tp"), None), P(("ep", "tp"), None), P(("ep", "tp"), None), P(),
    )
    out_specs = (P("ep", "tp"), P("ep", "tp", None, None), P("ep", "tp"))
    return jax.shard_map(body, mesh=mesh, in_specs=in_specs, out_specs=out_specs, check_vma=False)
```

```python
import jax
import jax.numpy as jnp
from jax import lax
from jax.experimental import pallas as pl
from jax.experimental.pallas import tpu as pltpu
from jax.sharding import PartitionSpec as P

norm_eps = 1e-05
clamp_limit = 7.0
sigmoid_slope = 1.702
F32 = jnp.float32
BF16 = jnp.bfloat16
MESH = pl.DeviceIdType.MESH
VMEM_SPEC = pl.BlockSpec(memory_space=pltpu.VMEM)
ANY_SPEC = pl.BlockSpec(memory_space=pl.ANY)
VMEM_LIMIT = 60 * 1024 * 1024

SIDE = 4
PLANE = 16
CHIPS = 64
ROWS = 16
SEQS = 2


def rms_scale(values, gain):
    mean_square = jnp.mean(values * values, axis=-1, keepdims=True)
    return values * lax.rsqrt(mean_square + norm_eps) * gain


def own_place():
    chip = lax.axis_index("ep")
    core = lax.axis_index("tp")
    return chip, core, chip % SIDE, chip // SIDE


def plane_shift(plane, step):
    z = (plane // SIDE + step // SIDE) % SIDE
    y = (plane % SIDE + step % SIDE) % SIDE
    return z * SIDE + y


def axis_peers(plane, x):
    z, y = plane // SIDE, plane % SIDE
    along_y = [((z * SIDE + (y + d) % SIDE) * SIDE + x) for d in range(1, SIDE)]
    along_z = [((((z + d) % SIDE) * SIDE + y) * SIDE + x) for d in range(1, SIDE)]
    along_x = [(plane * SIDE + (x + d) % SIDE) for d in range(1, SIDE)]
    return along_x, along_y, along_z


def each_chip(plane, x, act):
    xs = [(x + d) % SIDE for d in range(SIDE)]

    def on_plane(step, carry):
        base = plane_shift(plane, step) * SIDE
        for d in range(SIDE):
            act(base + xs[d])
        return carry

    lax.fori_loop(1, PLANE, on_plane, 0)
    for d in range(1, SIDE):
        act(plane * SIDE + xs[d])


def remote(src, dst, send, recv, device):
    return pltpu.make_async_remote_copy(
        src_ref=src, dst_ref=dst, send_sem=send, recv_sem=recv,
        device_id=device, device_id_type=MESH,
    )


def drain(ref, sem):
    pltpu.make_async_copy(ref, ref, sem).wait()


def projection_kernel(
    tok_ref, gain_ref, wq_ref, wk_ref, wv_ref, wo_ref, wi_ref, wf_ref, mix_ref, dg_ref, du_ref,
    rows_ref, gates_ref, mixall_ref, dgall_ref, duall_ref,
    tokv, gainv, wiv, wfv, wbuf, gbuf, nbuf, abuf, pbuf, sbuf, tbuf, rbuf,
    load_sem, w_send, w_recv, g_send, g_recv, a_send, a_recv, m_send, m_recv, p_send, p_recv, r_send, r_recv,
    d_send, d_recv, near_sem,
):
    chip, core, x, plane = own_place()
    z, y = plane // SIDE, plane % SIDE
    right = plane * SIDE + (x + 1) % SIDE
    left = plane * SIDE + (x + 3) % SIDE
    across = plane * SIDE + (x + 2) % SIDE
    xl, xr = (x + 3) % SIDE, (x + 1) % SIDE

    barrier = pltpu.get_barrier_semaphore()
    along_x, along_y, along_z = axis_peers(plane, x)
    for peer in along_z + along_x + along_y:
        pl.semaphore_signal(barrier, inc=1, device_id=(peer, core), device_id_type=MESH)

    def w_rows(xs):
        return pl.ds(pl.multiple_of(32 * xs, 32), 32)

    def half_rows(xs, half):
        return pl.ds(pl.multiple_of(32 * xs + 16 * half, 16), 16)

    for k, ref in enumerate((wq_ref, wk_ref, wv_ref, wo_ref)):
        load = pltpu.make_async_copy(ref, wbuf.at[w_rows(x), pl.ds(512 * k, 512)], load_sem.at[0])
        load.start()
    small = [
        pltpu.make_async_copy(src, dst, load_sem.at[2 + k])
        for k, (src, dst) in enumerate(((tok_ref, tokv), (gain_ref, gainv), (wi_ref, wiv), (wf_ref, wfv)))
    ]
    for load in small:
        load.start()
    for load in small:
        load.wait()

    normed = rms_scale(tokv[...].astype(F32), gainv[...])
    nbuf[...] = normed.astype(BF16)
    place = (
        lax.broadcasted_iota(jnp.int32, (32, 128), 1) == lax.broadcasted_iota(jnp.int32, (32, 128), 0) + 32 * x
    ).astype(F32)
    gate_in = jnp.dot(wiv[...].astype(F32), place, preferred_element_type=F32)
    gate_fo = jnp.dot(wfv[...].astype(F32), place, preferred_element_type=F32)
    gbuf[x] = jnp.concatenate([gate_in, gate_fo], axis=0)
    drain(wbuf.at[w_rows(x), :], load_sem.at[0])
    pl.semaphore_wait(barrier, 9)
    for peer in along_y:
        pl.semaphore_signal(near_sem, inc=1, device_id=(peer, core), device_id_type=MESH)

    def w_copy(k, kind, xs, part, device):
        rows = w_rows(xs) if part is None else half_rows(xs, part)
        block = wbuf.at[rows, pl.ds(512 * k, 512)]
        return remote(block, block, w_send, w_recv.at[k, kind], (device, core))

    for k in range(4):
        w_copy(k, 0, x, None, right).start()
        w_copy(k, 1, x, None, left).start()
    for peer in (right, left, across):
        remote(gbuf.at[x], gbuf.at[x], g_send, g_recv, (peer, core)).start()

    def token_copy(step):
        peer = plane_shift(plane, step)
        return remote(
            nbuf.at[:, pl.ds(pl.multiple_of(128 * peer, 128), 128)],
            abuf.at[pl.ds(pl.multiple_of(ROWS * plane, ROWS), ROWS), :],
            a_send, a_recv, (peer * SIDE + x, core),
        )

    def plane_peer(axis, step):
        if axis == 0:
            return (z + step) % SIDE, y
        return z, (y + step) % SIDE

    def device_of(zt, yt):
        return ((zt * SIDE + yt) * SIDE + x, core)

    def mix_first(axis, step):
        part = pl.ds(16 * axis, 16)
        return remote(
            mix_ref.at[part], mixall_ref.at[z, y, part], m_send, m_recv.at[axis], device_of(*plane_peer(axis, step))
        )

    def mix_second(axis, step):
        part = pl.ds(16 * (1 - axis), 16)
        block = mixall_ref.at[z, :, part] if axis == 0 else mixall_ref.at[:, y, part]
        return remote(block, block, m_send, m_recv.at[2 + axis], device_of(*plane_peer(axis, step)))

    def start_tokens(step, carry):
        token_copy(step).start()
        return carry

    pl.semaphore_wait(near_sem, 3)
    lax.fori_loop(1, PLANE, start_tokens, 0)
    abuf[pl.ds(pl.multiple_of(ROWS * plane, ROWS), ROWS), :] = nbuf[:, pl.ds(pl.multiple_of(128 * plane, 128), 128)]
    for axis in range(2):
        for d in (2, 1, 3):
            mix_first(axis, d).start()
    mix_own = pltpu.make_async_copy(mix_ref, mixall_ref.at[z, y], load_sem.at[1])
    mix_own.start()

    dense = ((dg_ref, dgall_ref), (du_ref, duall_ref))

    def dense_copy(k, kind, xs, part, device):
        block = dense[k][1].at[xs]
        if part is not None:
            block = block.at[pl.ds(16 * part, 16)]
        source = dense[k][0] if kind in (0, 1) else block
        return remote(source, block, d_send.at[k], d_recv.at[kind], device)

    def w_relay(k):
        w_copy(k, 0, x, None, right).wait_recv()
        w_copy(k, 2, xl, 0, right).start()
        w_copy(k, 1, x, None, left).wait_recv()
        w_copy(k, 3, xr, 1, left).start()

    for k in range(4):
        w_relay(k)
    for k in range(2):
        dense_copy(k, 0, x, None, (right, core)).start()
        dense_copy(k, 1, x, None, (left, core)).start()
    drain(abuf.at[pl.ds(0, 240), :], a_recv)
    drain(gbuf.at[pl.ds(0, 3)], g_recv)
    gate_w = (gbuf[0] + gbuf[1] + gbuf[2] + gbuf[3]).astype(BF16)
    gate_w = jnp.concatenate([gate_w.astype(F32), jnp.zeros((120, 128), F32)], axis=0).astype(BF16)
    def columns(k):
        return pl.ds(512 * k, 640 if k == 3 else 512)

    def first_sum(k, step):
        axis = (k + 1) % 2
        zt, yt = plane_peer(axis, step)
        src = pbuf.at[zt, :, :, columns(k)] if axis == 0 else pbuf.at[:, yt, :, columns(k)]
        own = z if axis == 0 else y
        return remote(src, sbuf.at[own, :, :, columns(k)], p_send, p_recv.at[k], device_of(zt, yt))

    def second_sum(k, step):
        axis = k % 2
        zt, yt = plane_peer(axis, step)
        target, own = (zt, z) if axis == 0 else (yt, y)
        return remote(
            tbuf.at[target, :, columns(k)], rbuf.at[own, :, columns(k)], r_send, r_recv.at[k], device_of(zt, yt)
        )

    for k in range(4):
        w_copy(k, 2, xl, 0, right).wait_recv()
        w_copy(k, 3, xr, 1, left).wait_recv()
        cols = slice(512 * k, 512 * k + 512)
        part = jnp.dot(abuf[...], wbuf[:, cols], preferred_element_type=F32).astype(BF16)
        pbuf[:, :, :, cols] = part.reshape(SIDE, SIDE, ROWS, 512)
        if k == 3:
            gates = lax.dot_general(abuf[...], gate_w, (((1,), (1,)), ((), ())), preferred_element_type=F32)
            high = gates.astype(BF16).astype(F32)
            part = (high + pltpu.roll(gates - high, 8, 1)).astype(BF16)
            pbuf[:, :, :, 2048:2176] = part.reshape(SIDE, SIDE, ROWS, 128)
        for d in (2, 1, 3):
            first_sum(k, d).start()
    mix_own.wait()
    for axis in range(2):
        drain(mixall_ref.at[0, pl.ds(0, 3), pl.ds(0, 16)], m_recv.at[1 - axis])
        for d in (2, 1, 3):
            mix_second(axis, d).start()
    first_lanes = lax.broadcasted_iota(jnp.int32, (ROWS, 128), 1) < 8
    for k in range(4):
        cols = slice(512 * k, 2176 if k == 3 else 512 * k + 512)
        if k % 2 == 0:
            sbuf[y, :, :, cols] = pbuf[:, y, :, cols]
        else:
            sbuf[z, :, :, cols] = pbuf[z, :, :, cols]
        drain(sbuf.at[pl.ds(0, 3), :, :, columns(k)], p_recv.at[k])
        for t in range(SIDE):
            total = sbuf[0, t, :, cols].astype(F32)
            for s in range(1, SIDE):
                total = total + sbuf[s, t, :, cols].astype(F32)
            if k == 3:
                gates = total[:, 512:640]
                gates = jnp.where(first_lanes, gates + pltpu.roll(gates, 120, 1), 0.0)
                high = gates.astype(BF16).astype(F32)
                total = jnp.concatenate([total[:, :512], high + pltpu.roll(gates - high, 8, 1)], axis=1)
            tbuf[t, :, cols] = total.astype(BF16)
        for d in (2, 1, 3):
            second_sum(k, d).start()
        if k % 2 == 0:
            rbuf[z, :, cols] = tbuf[z, :, cols]
        else:
            rbuf[y, :, cols] = tbuf[y, :, cols]

    two, twohalf = dgall_ref.at[pl.ds(0, 2)], dgall_ref.at[pl.ds(0, 2), pl.ds(0, 16)]
    drain(two, d_recv.at[0])
    for k in range(2):
        dense_copy(k, 2, xl, 0, (right, core)).start()
    drain(two, d_recv.at[1])
    for k in range(2):
        dense_copy(k, 3, xr, 1, (left, core)).start()
    for k in range(4):
        cols = slice(512 * k, 512 * k + 512)
        drain(rbuf.at[pl.ds(0, 3), :, columns(k)], r_recv.at[k])
        total = rbuf[0, :, cols].astype(F32)
        for s in range(1, SIDE):
            total = total + rbuf[s, :, cols].astype(F32)
        rows_ref[:, cols] = total.astype(BF16)
    total = rbuf[0, :, 2048:2176].astype(F32)
    for s in range(1, SIDE):
        total = total + rbuf[s, :, 2048:2176].astype(F32)
    gates_ref[...] = total + pltpu.roll(total, 120, 1)

    drain(twohalf, d_recv.at[2])
    drain(twohalf, d_recv.at[3])

    drain(wbuf.at[pl.ds(0, 96), :], w_send)
    drain(gbuf.at[pl.ds(0, 3)], g_send)
    drain(abuf.at[pl.ds(0, 240), :], a_send)
    drain(mixall_ref.at[pl.ds(0, 3), :, :], m_send)
    drain(mixall_ref.at[0, pl.ds(0, 3)], m_send)
    drain(sbuf.at[pl.ds(0, 3)], p_send)
    drain(rbuf.at[pl.ds(0, 3)], r_send)
    for k in range(2):
        drain(dense[k][1].at[pl.ds(0, 3)], d_send.at[k])
    for axis in range(2):
        drain(mixall_ref.at[pl.ds(0, 3), :, pl.ds(0, 16)], m_recv.at[2 + axis])


def project(tokens, norm_gain, wq, wk, wv, wo, wi_t, wf_t, mix_t, dg, du):
    dma = pltpu.SemaphoreType.DMA
    return pl.pallas_call(
        projection_kernel,
        out_shape=(
            jax.ShapeDtypeStruct((ROWS, 2048), BF16),
            jax.ShapeDtypeStruct((ROWS, 128), F32),
            jax.ShapeDtypeStruct((SIDE, SIDE, 32, 512), BF16),
            jax.ShapeDtypeStruct((4, 32, 2048), BF16),
            jax.ShapeDtypeStruct((4, 32, 2048), BF16),
        ),
        in_specs=[ANY_SPEC] * 11,
        out_specs=(VMEM_SPEC, VMEM_SPEC, ANY_SPEC, ANY_SPEC, ANY_SPEC),
        scratch_shapes=[
            pltpu.VMEM((ROWS, 2048), BF16),
            pltpu.VMEM((1, 2048), F32),
            pltpu.VMEM((4, 32), BF16),
            pltpu.VMEM((4, 32), BF16),
            pltpu.VMEM((128, 2048), BF16),
            pltpu.VMEM((4, 8, 128), F32),
            pltpu.VMEM((ROWS, 2048), BF16),
            pltpu.VMEM((256, 128), BF16),
            pltpu.VMEM((SIDE, SIDE, ROWS, 2176), BF16),
            pltpu.VMEM((SIDE, SIDE, ROWS, 2176), BF16),
            pltpu.VMEM((SIDE, ROWS, 2176), BF16),
            pltpu.VMEM((SIDE, ROWS, 2176), BF16),
            dma((6,)),
            dma, dma((4, 4)),
            dma, dma,
            dma, dma,
            dma, dma((4,)),
            dma, dma((4,)),
            dma, dma((4,)),
            dma((2,)), dma((4,)),
            pltpu.SemaphoreType.REGULAR,
        ],
        compiler_params=pltpu.CompilerParams(
            collective_id=0, has_side_effects=True, vmem_limit_bytes=VMEM_LIMIT
        ),
        name="project",
    )(tokens, norm_gain, wq, wk, wv, wo, wi_t, wf_t, mix_t, dg, du)


def identity(n):
    row = lax.broadcasted_iota(jnp.int32, (n, n), 0)
    return (row == lax.broadcasted_iota(jnp.int32, (n, n), 1)).astype(F32)


def turned(values):
    rows = values.shape[0]
    return lax.dot_general(
        identity(values.shape[1]), values, (((1,), (1,)), ((), ())),
        preferred_element_type=F32, precision=lax.Precision.HIGHEST,
    ).reshape(values.shape[1], rows)


def memory_gates(gates, bias, stab_t):
    stab = turned(stab_t)
    input_pre = gates[:, 0:4]
    forget = pltpu.roll(gates, 124, 1)[:, 0:4] + bias
    log_forget = jnp.minimum(forget, 0.0) - jnp.log1p(jnp.exp(-jnp.abs(forget)))
    stab_new = jnp.maximum(log_forget + stab, input_pre)
    return stab_new, jnp.exp(log_forget + stab - stab_new), jnp.exp(input_pre - stab_new)


def head_cols(part, h):
    return slice(512 * part + 128 * h, 512 * part + 128 * h + 128)


def upright(rows):
    return jnp.concatenate([rows, jnp.zeros((112, 128), F32)], axis=0).T


def memory_kernel(
    carr_hbm, keys_hbm, vt_hbm, stab_hbm, mem_ref, mixed_hbm,
    new_ref, stab_new_ref, mixed_ref,
    memv, carr, keys, vt, small_sem, load_sem, store_sem,
):
    small = [
        pltpu.make_async_copy(src, dst, small_sem.at[k])
        for k, (src, dst) in enumerate((
            (carr_hbm, carr), (keys_hbm, keys), (vt_hbm, vt), (stab_hbm, stab_new_ref), (mixed_hbm, mixed_ref),
        ))
    ]
    for copy in small:
        copy.start()

    def part(i):
        return pl.ds(SEQS * i, SEQS)

    def load(i):
        return pltpu.make_async_copy(mem_ref.at[part(i)], memv.at[part(i)], load_sem.at[i])

    def store(i):
        return pltpu.make_async_copy(memv.at[part(i)], new_ref.at[part(i)], store_sem)

    for i in range(3):
        load(i).start()
    for copy in small:
        copy.wait()
    def advance(i, carry):
        load(i).wait()

        @pl.when(i + 3 < ROWS // SEQS)
        def _():
            load(i + 3).start()

        for h in range(4):
            values = vt[h]
            for j in range(SEQS):
                place = pl.ds(SEQS * i + j, 1)
                memv[SEQS * i + j, h] = (
                    carr[h, place, :] * memv[SEQS * i + j, h] + values[:, j:j + 1] * keys[h, place, :]
                )
            vt[h] = pltpu.roll(values, 128 - SEQS, 1)
        store(i).start()
        return carry

    lax.fori_loop(0, ROWS // SEQS, advance, 0)
    drain(memv, store_sem)


def memory_update(carried, keys, values, stab_new, memory, mixed):
    dma = pltpu.SemaphoreType.DMA
    vm = pltpu.VMEM
    return pl.pallas_call(
        memory_kernel,
        out_shape=(
            jax.ShapeDtypeStruct((ROWS, 4, 128, 128), F32),
            jax.ShapeDtypeStruct((4, ROWS), F32),
            jax.ShapeDtypeStruct((ROWS, 1024), BF16),
        ),
        in_specs=[ANY_SPEC] * 6,
        out_specs=(ANY_SPEC, VMEM_SPEC, VMEM_SPEC),
        scratch_shapes=[
            vm((ROWS, 4, 128, 128), F32), vm((4, ROWS, 128), F32), vm((4, ROWS, 128), F32), vm((4, 128, 128), F32),
            dma((5,)), dma((ROWS // SEQS,)), dma,
        ],
        compiler_params=pltpu.CompilerParams(vmem_limit_bytes=VMEM_LIMIT),
        name="memory_update",
    )(carried, keys, values, stab_new, memory, mixed)


def expert_kernel(
    mem_ref, rows_hbm, gates_hbm, bias_hbm, stab_hbm, hgain_hbm, mix_ref, tok_hbm, gain_hbm, route_hbm, weight_hbm, eg_ref, eu_ref, ed_ref,
    dg_ref, du_ref, dd_ref, dgall_ref, duall_ref, scale_hbm,
    out_ref, carr_ref, keys_ref, vt_ref, stab_new_ref,
    memv, rows_ref, gates_ref, bias_ref, stab_ref, hgain_ref, rt, queries, gated_ref,
    tok_ref, gain_ref, route_ref, weight_ref, scale_ref,
    egv, euv, edv, dgv, duv, ddv, mixv, gx, asend, tb, ns, res, n2, sel, comb_hi, comb_lo, obuf, rx, xbuf, gacc, uacc, hbuf,
    yown, ysend, yrecv, yret, rret, da, dout, dr,
    load_sem, gx_send, gx_recv, tb_send, tb_recv, x_send, x_recv, da_send, da_recv,
    y_send, y_recv, q_send, q_recv, dr_send, dr_recv, xo_send, xo_recv, d_send, d_recv, mem_sem, down_send, down_recv, near_sem,
):
    chip, core, x, plane = own_place()
    other = 1 - core

    barrier = pltpu.get_barrier_semaphore()

    along_x, along_y, along_z = axis_peers(plane, x)
    for peer in along_z + along_y + along_x:
        pl.semaphore_signal(barrier, inc=1, device_id=(peer, core), device_id_type=MESH)
    pl.semaphore_signal(barrier, inc=1, device_id=(chip, other), device_id_type=MESH)

    loads = []
    for k, (src, dst) in enumerate(((eg_ref, egv), (eu_ref, euv), (ed_ref, edv))):
        loads.append(pltpu.make_async_copy(src.at[0], dst, load_sem.at[k]))
    dense_loads, dense_sends = [], []
    for k, (own, rest, dst) in enumerate(
        ((dg_ref, dgall_ref, dgv), (du_ref, duall_ref, duv), (dd_ref, None, ddv))
    ):
        for s in range(SIDE if k < 2 else 1):
            xs = (x + s) % SIDE
            src = rest.at[xs] if s else own
            slot = dst.at[2 * xs + core]
            dense_loads.append(pltpu.make_async_copy(src, slot, load_sem.at[3 + k]))
            dense_sends.append(remote(src, slot, d_send.at[k], d_recv.at[k], (chip, other)))
    small = [
        pltpu.make_async_copy(src, dst, load_sem.at[7 + k])
        for k, (src, dst) in enumerate((
            (rows_hbm, rows_ref), (gates_hbm, gates_ref), (bias_hbm, bias_ref), (stab_hbm, stab_ref),
            (hgain_hbm, hgain_ref), (route_hbm, route_ref), (weight_hbm, weight_ref), (tok_hbm, tok_ref),
            (gain_hbm, gain_ref), (scale_hbm, scale_ref),
        ))
    ]
    mix_load = pltpu.make_async_copy(mix_ref, mixv, load_sem.at[6])
    def mem_load(i):
        part = pl.ds(4 * i, 4)
        return pltpu.make_async_copy(mem_ref.at[part], memv.at[part], mem_sem.at[i])

    for load in small:
        load.start()
    for i in range(4):
        mem_load(i).start()
    mix_load.start()
    for load in small:
        load.wait()

    stab_new, carried, written = memory_gates(gates_ref[...], bias_ref[...], stab_ref[...])
    stab_new_ref[...] = turned(stab_new)
    for h in range(4):
        query = upright(rows_ref[:, head_cols(0, h)].astype(F32)).astype(BF16)
        queries[h] = jnp.concatenate([query, query], axis=0)
    lane_index = lax.broadcasted_iota(jnp.int32, (128, 128), 1)

    def read_part(i, carry):
        mem_load(i).wait()
        for h in range(4):
            stored = memv[pl.ds(4 * i, 4), h].reshape(512, 128)
            top = stored.astype(BF16)
            rest = (stored - top.astype(F32)).astype(BF16)
            read = jnp.dot(jnp.concatenate([top, rest], axis=1), queries[h], preferred_element_type=F32)
            reads = rt[h]
            for j in range(4):
                reads = jnp.where(lane_index == 4 * i + j, read[128 * j:128 * j + 128, :], reads)
            rt[h] = reads
        return carry

    rt[...] = jnp.zeros(rt.shape, F32)
    lax.fori_loop(0, 4, read_part, 0)
    for load in dense_loads + loads:
        load.start()
    for h in range(4):
        query = rows_ref[:, head_cols(0, h)].astype(F32)
        key = rows_ref[:, head_cols(1, h)].astype(F32) * (128 ** (-0.5))
        value = rows_ref[:, head_cols(2, h)].astype(F32)
        match = jnp.sum(key * query, axis=1, keepdims=True) * written[:, h:h + 1]
        carr_ref[h] = jnp.broadcast_to(carried[:, h:h + 1], (ROWS, 128))
        keys_ref[h] = key * written[:, h:h + 1]
        vt_ref[h] = upright(value)
        readout = carried[:, h:h + 1] * rt[h].T[0:ROWS, :] + match * value
        gate = jax.nn.sigmoid(rows_ref[:, head_cols(3, h)].astype(F32))
        scaled = rms_scale(readout, hgain_ref[:, head_cols(0, h)])
        gated_ref[:, head_cols(0, h)] = (scaled * gate).astype(BF16)

    spread = (
        lax.broadcasted_iota(jnp.int32, (ROWS, 128), 1) % ROWS == lax.broadcasted_iota(jnp.int32, (ROWS, 128), 0)
    ).astype(F32)
    route = jnp.dot(route_ref[...].astype(F32), spread, preferred_element_type=F32, precision=lax.Precision.HIGHEST)
    weight = jnp.dot(weight_ref[...], spread, preferred_element_type=F32, precision=lax.Precision.HIGHEST)
    expert = lax.broadcasted_iota(jnp.int32, (CHIPS, 128), 0).astype(F32)
    hit = jnp.zeros((CHIPS, 128), F32)
    chosen = jnp.zeros((CHIPS, 128), F32)
    for k in range(4):
        same = (route[k:k + 1, :] == expert).astype(F32)
        hit = hit + same
        chosen = chosen + same * weight[k:k + 1, :]
    col = lax.broadcasted_iota(jnp.int32, (128, 128), 1) % ROWS
    row = lax.broadcasted_iota(jnp.int32, (128, 128), 0)
    before = ((row < ROWS) & (row < col)).astype(F32)
    rank = jnp.dot(hit, before, preferred_element_type=F32)
    first = hit * (rank == 0.0).astype(F32)
    second = hit * (rank == 1.0).astype(F32)
    block_row = lax.broadcasted_iota(jnp.int32, (8, 128), 0)
    block_col = lax.broadcasted_iota(jnp.int32, (8, 128), 1) // ROWS
    diagonal = (block_row == block_col).astype(F32)

    def widened(top, bottom):
        low = top[:, None, :] * diagonal[None, :, :]
        high = bottom[:, None, :] * diagonal[None, :, :]
        return jnp.concatenate([low, high], axis=1).reshape(1024, 128)

    sel[...] = widened(first, second).astype(BF16)
    comb = widened(first * chosen, second * chosen).T
    comb_top = comb.astype(BF16)
    comb_hi[...] = comb_top
    comb_lo[...] = (comb - comb_top.astype(F32)).astype(BF16)
    gx[pl.ds(pl.multiple_of(ROWS * x, ROWS), ROWS), :] = gated_ref[...]

    pl.semaphore_wait(barrier, 9 + 1)

    def gx_copy(d):
        rows = pl.ds(pl.multiple_of(ROWS * x, ROWS), ROWS)
        peer = plane * SIDE + (x + d) % SIDE
        return remote(gated_ref, gx.at[rows, :], gx_send, gx_recv, (peer, core))

    for d in range(1, SIDE):
        gx_copy(d).start()
    def down_copy(kind, xs, part, device):
        block = ddv.at[2 * xs + core]
        if part is not None:
            block = block.at[pl.ds(16 * part, 16)]
        if kind == 4:
            return remote(block, block, d_send.at[2], d_recv.at[2], (chip, other))
        return remote(dd_ref if kind < 2 else block, block, down_send, down_recv.at[kind], (device, core))

    right, left = plane * SIDE + (x + 1) % SIDE, plane * SIDE + (x + 3) % SIDE
    xl, xr, xa = (x + 3) % SIDE, (x + 1) % SIDE, (x + 2) % SIDE
    mix_load.wait()
    drain(gx.at[pl.ds(0, 48), :], gx_recv)
    for peer in along_y:
        pl.semaphore_signal(near_sem, inc=1, device_id=(peer, core), device_id_type=MESH)
    asend[...] = lax.dot_general(
        gx[...], mixv[...], (((1,), (1,)), ((), ())), preferred_element_type=F32
    ).astype(BF16)

    def tb_copy(d, side):
        rows = pl.ds(pl.multiple_of(ROWS * ((x + d) % SIDE), ROWS), ROWS)
        peer = plane * SIDE + (x + d) % SIDE
        return remote(
            asend.at[rows, :], tb.at[core, x], tb_send, tb_recv,
            (peer, (core + side) % 2),
        )

    tb_list = [(0, 1)] + [(d, side) for d in (2, 1, 3) for side in (0, 1)]
    for d, side in tb_list:
        tb_copy(d, side).start()
    tb[core, x] = asend[pl.ds(pl.multiple_of(ROWS * x, ROWS), ROWS), :]
    down_copy(0, x, None, right).start()
    down_copy(1, x, None, left).start()
    tb_bytes = rx.at[pl.ds(0, 448), :]
    drain(tb_bytes, tb_recv)
    pl.semaphore_wait(near_sem, 3)
    for copy in dense_sends:
        copy.start()
    attended = [tb[0, k].astype(F32) + tb[1, k].astype(F32) for k in range(SIDE)]
    lane = lax.broadcasted_iota(jnp.int32, (ROWS, 128), 1) // 32
    tiles = []
    for t in range(PLANE):
        tile = None
        for k in range(SIDE):
            part = attended[k][:, 128 * (t // 4):128 * (t // 4) + 128]
            shift = (32 * k - 32 * (t % 4)) % 128
            if shift:
                part = pltpu.roll(part, shift, 1)
            tile = part if tile is None else jnp.where(lane == k, part, tile)
        tiles.append(tile)
    residual = (tok_ref[...].astype(F32) + jnp.concatenate(tiles, axis=1)).astype(BF16)
    res[...] = residual
    normed = rms_scale(residual.astype(F32), gain_ref[...]).astype(BF16)
    ns[...] = normed
    def tile_rows(index):
        return pl.ds(pl.multiple_of(ROWS * index, ROWS), ROWS)

    parity = plane % 2
    half = plane // 2

    z, y = plane // SIDE, plane % SIDE
    own_row = y // 2
    low, high = pl.ds(0, 1024), pl.ds(1024, 1024)

    def acts_first(axis, d):
        peer = (along_z, along_y)[axis][d]
        cols = (low, high)[axis]
        return remote(
            ns.at[:, cols], da.at[z, own_row, :, cols], da_send.at[0], da_recv.at[axis], (peer, parity)
        )

    def acts_second(axis, d):
        peer = (along_z, along_y)[axis][d]
        block = da.at[z, :, :, high] if axis == 0 else da.at[:, own_row, :, low]
        return remote(block, block, da_send.at[1 + axis], da_recv.at[2 + axis], (peer, core))

    for axis in range(2):
        @pl.when(core == axis)
        def _():
            for d in (1, 0, 2):
                acts_first(axis, d).start()

    @pl.when(parity == core)
    def _():
        da[z, own_row] = ns[...]

    for b in range(8):
        cols = pl.ds(pl.multiple_of(1024 * core + 128 * b, 128), 128)
        n2[16 * b:16 * b + 16, :] = ns[:, cols]
    for k in range(4):
        obuf[256 * k:256 * k + 256, :] = jnp.dot(
            sel[256 * k:256 * k + 256, :], n2[...], preferred_element_type=F32
        ).astype(BF16)

    def x_copy(peer):
        return remote(
            obuf.at[tile_rows(peer), :], rx.at[tile_rows(chip), :], x_send, x_recv, (peer, core)
        )

    each_chip(plane, x, lambda peer: x_copy(peer).start())
    rx[tile_rows(chip), :] = obuf[tile_rows(chip), :]

    down_copy(0, x, None, right).wait_recv()
    down_copy(2, xl, 0, right).start()
    down_copy(1, x, None, left).wait_recv()
    down_copy(3, xr, 1, left).start()
    down_copy(4, xl, None, chip).start()
    down_copy(4, xr, None, chip).start()
    row_of = da.at[0, 0, :, low]

    @pl.when(parity == core)
    def _():
        drain(row_of, da_recv.at[1])
        drain(da.at[pl.ds(0, 3), 0, :, low], da_recv.at[0])
        for d in (1, 0, 2):
            acts_second(1, d).start()

    @pl.when(parity != core)
    def _():
        drain(da.at[pl.ds(0, 2), 0, :, low], da_recv.at[1])

    for d in (1, 0, 2):
        acts_second(0, d).start()

    for k, dst in enumerate((dgv, duv)):
        drain(dst.at[pl.ds(0, 4)], load_sem.at[3 + k])
        drain(dst.at[pl.ds(0, 4)], d_recv.at[k])

    @pl.when(parity == core)
    def _():
        drain(da.at[:, 0, :, low], da_recv.at[3])

    @pl.when(parity != core)
    def _():
        drain(da.at[:, :, :, low], da_recv.at[3])

    drain(da.at[pl.ds(0, 3), :, :, low], da_recv.at[2])

    down_copy(2, xa, 0, right).wait_recv()
    down_copy(3, xa, 1, left).wait_recv()
    down_copy(4, xa, None, chip).start()
    dense_rows = da[...].reshape(128, 2048)
    over_last = (((1,), (1,)), ((), ()))
    gate_rows = lax.dot_general(dense_rows, dgv[...].reshape(256, 2048), over_last, preferred_element_type=F32)
    lift_rows = lax.dot_general(dense_rows, duv[...].reshape(256, 2048), over_last, preferred_element_type=F32)
    activity = (gate_rows / (1.0 + jnp.exp(-gate_rows)) * lift_rows).astype(BF16)
    drain(ddv.at[pl.ds(0, 1)], load_sem.at[5])
    drain(ddv.at[pl.ds(0, 4)], d_recv.at[2])
    down = ddv[...].reshape(256, 2048)
    for h in range(2):
        for t in range(2):
            lower = 1024 * h + 512 * t
            part = jnp.dot(activity, down[:, lower:lower + 512], preferred_element_type=F32).astype(BF16)
            dout[h, :, 512 * t:512 * t + 512] = part

    def dr_copy(index, h):
        target = 2 * index + core
        return remote(
            dout.at[h, tile_rows(index), :], dr.at[plane], dr_send, dr_recv,
            (target * SIDE + x, h),
        )

    def start_dr(index, carry):
        for h in range(2):
            @pl.when((2 * index + core != plane) | (core != h))
            def _():
                dr_copy(index, h).start()
        return carry

    lax.fori_loop(0, 8, start_dr, 0)

    @pl.when(parity == core)
    def _():
        dr[plane] = dout[core, tile_rows(half), :]

    drain(rx.at[pl.ds(0, 1008), :], x_recv)
    row = lax.broadcasted_iota(jnp.int32, (256, 256), 0)
    col = lax.broadcasted_iota(jnp.int32, (256, 256), 1)
    gather = (col == ((row % 32) // 2) * 16 + (row % 2) * 8 + row // 32).astype(F32).astype(BF16)
    scatter = (row == ((col % 32) // 2) * 16 + (col % 2) * 8 + col // 32).astype(F32).astype(BF16)
    for g in range(4):
        mixed_up = jnp.dot(gather, rx[256 * g:256 * g + 256, :], preferred_element_type=F32).astype(BF16)
        for b in range(8):
            xbuf[core, 32 * g:32 * g + 32, 128 * b:128 * b + 128] = mixed_up[32 * b:32 * b + 32, :]
    swap = remote(xbuf.at[core], xbuf.at[core], xo_send, xo_recv, (chip, other))
    swap.start()
    loads[0].wait()
    loads[1].wait()

    def expert_up_near(t, carry):
        cols = pl.ds(pl.multiple_of(256 * t, 256), 256)
        depth = pl.ds(pl.multiple_of(1024 * core, 1024), 1024)
        gacc[:, cols] = jnp.dot(xbuf[core], egv[depth, cols], preferred_element_type=F32)
        uacc[:, cols] = jnp.dot(xbuf[core], euv[depth, cols], preferred_element_type=F32)
        return carry

    def expert_up_far(t, carry):
        cols = pl.ds(pl.multiple_of(256 * t, 256), 256)
        depth = pl.ds(pl.multiple_of(1024 * other, 1024), 1024)
        gate_pre = gacc[:, cols] + jnp.dot(xbuf[other], egv[depth, cols], preferred_element_type=F32)
        up_pre = uacc[:, cols] + jnp.dot(xbuf[other], euv[depth, cols], preferred_element_type=F32)
        gate_clamped = jnp.minimum(gate_pre, clamp_limit)
        up_clamped = jnp.clip(up_pre, -clamp_limit, clamp_limit)
        hbuf[:, cols] = (
            (up_clamped + 1.0) * gate_clamped * jax.nn.sigmoid(sigmoid_slope * gate_clamped)
        ).astype(BF16)
        return carry

    lax.fori_loop(0, 4, expert_up_near, 0)
    swap.wait_recv()
    lax.fori_loop(0, 4, expert_up_far, 0)
    loads[2].wait()

    def y_copy(t):
        return remote(ysend.at[t], yrecv.at[t], y_send, y_recv, (chip, other))

    def expert_down_far(t, carry):
        cols = pl.ds(pl.multiple_of(1024 * other + 256 * t, 256), 256)
        ysend[t] = jnp.dot(hbuf[...], edv[:, cols], preferred_element_type=F32).astype(BF16)
        y_copy(t).start()
        return carry

    def expert_down_near(t, carry):
        cols = pl.ds(pl.multiple_of(1024 * core + 256 * t, 256), 256)
        yown[t] = jnp.dot(hbuf[...], edv[:, cols], preferred_element_type=F32).astype(BF16)
        return carry

    lax.fori_loop(0, 4, expert_down_far, 0)
    lax.fori_loop(0, 4, expert_down_near, 0)

    drain(yrecv, y_recv)
    for g in range(4):
        rows = slice(32 * g, 32 * g + 32)
        stacked = []
        for t in range(4):
            both = (yown[t, rows, :].astype(F32) + yrecv[t, rows, :].astype(F32)).astype(BF16)
            stacked += [both[:, :128], both[:, 128:]]
        yret[256 * g:256 * g + 256, :] = jnp.dot(
            scatter, jnp.concatenate(stacked, axis=0), preferred_element_type=F32
        ).astype(BF16)

    def q_copy(peer):
        return remote(
            yret.at[tile_rows(peer), :], rret.at[tile_rows(chip), :], q_send, q_recv, (peer, core)
        )

    each_chip(plane, x, lambda peer: q_copy(peer).start())
    rret[tile_rows(chip), :] = yret[tile_rows(chip), :]

    @pl.when(parity == core)
    def _():
        drain(dr.at[pl.ds(0, 15)], dr_recv)

    @pl.when(parity != core)
    def _():
        drain(dr, dr_recv)

    branch = dr[0].astype(F32)
    for s in range(1, PLANE):
        branch = branch + dr[s].astype(F32)

    drain(rret.at[pl.ds(0, 1008), :], q_recv)
    returned = rret[...]
    routed = jnp.dot(comb_hi[...], returned, preferred_element_type=F32) + jnp.dot(
        comb_lo[...], returned, preferred_element_type=F32
    )
    routed = jnp.concatenate([routed[16 * b:16 * b + 16, :] for b in range(8)], axis=1)
    own_cols = pl.ds(pl.multiple_of(1024 * core, 1024), 1024)
    out_ref[...] = (res[:, own_cols].astype(F32) + routed + branch * scale_ref[:, own_cols]).astype(BF16)

    drain(gx.at[pl.ds(0, 48), :], gx_send)
    drain(tb_bytes, tb_send)
    drain(rx.at[pl.ds(0, 1008), :], x_send)
    drain(rret.at[pl.ds(0, 1008), :], q_send)
    drain(yrecv, y_send)
    drain(xbuf.at[0], xo_send)
    for k, dst in enumerate((dgv, duv, ddv)):
        drain(dst.at[pl.ds(0, 4)], d_send.at[k])
    drain(ddv.at[pl.ds(0, 3)], down_send)

    drain(da.at[pl.ds(0, 3), 0, :, low], da_send.at[0])
    drain(da.at[pl.ds(0, 3), :, :, low], da_send.at[1])

    @pl.when(parity == core)
    def _():
        drain(da.at[pl.ds(0, 3)], da_send.at[2])

    @pl.when(parity == core)
    def _():
        drain(dr.at[pl.ds(0, 15)], dr_send)

    @pl.when(parity != core)
    def _():
        drain(dr, dr_send)


def feed_forward(*operands):
    dma = pltpu.SemaphoreType.DMA
    vm = pltpu.VMEM
    return pl.pallas_call(
        expert_kernel,
        out_shape=(
            jax.ShapeDtypeStruct((ROWS, 1024), BF16),
            jax.ShapeDtypeStruct((4, ROWS, 128), F32),
            jax.ShapeDtypeStruct((4, ROWS, 128), F32),
            jax.ShapeDtypeStruct((4, 128, 128), F32),
            jax.ShapeDtypeStruct((4, ROWS), F32),
        ),
        in_specs=[ANY_SPEC] * 20,
        out_specs=(VMEM_SPEC,) * 5,
        scratch_shapes=[
            vm((ROWS, 4, 128, 128), F32), vm((ROWS, 2048), BF16), vm((ROWS, 128), F32), vm((1, 4), F32),
            vm((4, ROWS), F32), vm((1, 512), F32), vm((4, 128, 128), F32), vm((4, 256, 128), BF16),
            vm((ROWS, 512), BF16), vm((ROWS, 2048), BF16), vm((1, 2048), F32),
            vm((4, ROWS), jnp.int32), vm((4, ROWS), F32), vm((1, 2048), F32),
            vm((2048, 1024), BF16), vm((2048, 1024), BF16), vm((1024, 2048), BF16),
            vm((8, 32, 2048), BF16), vm((8, 32, 2048), BF16), vm((8, 32, 2048), BF16),
            vm((512, 512), BF16),
            vm((64, 512), BF16), vm((64, 512), BF16), vm((2, 4, ROWS, 512), BF16),
            vm((ROWS, 2048), BF16), vm((ROWS, 2048), BF16), vm((128, 128), BF16),
            vm((1024, 128), BF16), vm((128, 1024), BF16), vm((128, 1024), BF16),
            vm((1024, 128), BF16), vm((1024, 128), BF16), vm((2, 128, 1024), BF16),
            vm((128, 1024), F32), vm((128, 1024), F32), vm((128, 1024), BF16),
            vm((4, 128, 256), BF16), vm((4, 128, 256), BF16), vm((4, 128, 256), BF16),
            vm((1024, 128), BF16), vm((1024, 128), BF16),
            vm((SIDE, 2, ROWS, 2048), BF16), vm((2, 128, 1024), BF16), vm((PLANE, ROWS, 1024), BF16),
            dma((17,)),
            dma, dma,
            dma, dma,
            dma, dma,
            dma((3,)), dma((4,)),
            dma, dma,
            dma, dma,
            dma, dma,
            dma, dma,
            dma((3,)), dma((3,)),
            dma((4,)),
            dma, dma((4,)),
            pltpu.SemaphoreType.REGULAR,
        ],
        compiler_params=pltpu.CompilerParams(
            collective_id=1, has_side_effects=True, vmem_limit_bytes=VMEM_LIMIT
        ),
        name="feed_forward",
    )(*operands)


def body(
    tokens, norm_gain, query_weight, key_weight, value_weight, outgate_weight, input_weight, forget_weight,
    forget_bias, memory, stabilizer, head_gain, mix_weight, second_gain, route_experts, route_weight,
    expert_gate, expert_up, expert_down, dense_gate, dense_up, dense_down, branch_scale,
):
    rows, gates, mix_all, dg_all, du_all = project(
        tokens, norm_gain.reshape(1, -1), query_weight, key_weight, value_weight, outgate_weight,
        input_weight.T, forget_weight.T, mix_weight.T, dense_gate, dense_up,
    )
    bias, stab_t = forget_bias.reshape(1, -1), stabilizer.T
    mixed, carried, keys, values, stab_new = feed_forward(
        memory, rows, gates, bias, stab_t, head_gain.reshape(1, -1), mix_all.reshape(512, 512), tokens, second_gain.reshape(1, -1), route_experts.T, route_weight.T,
        expert_gate, expert_up, expert_down, dense_gate, dense_up, dense_down, dg_all, du_all,
        branch_scale.reshape(1, -1),
    )
    memory_new, stab_new, mixed = memory_update(carried, keys, values, stab_new, memory, mixed)
    return mixed, memory_new, stab_new.T


def solution(mesh):
    in_specs = (
        P("ep", None), P(),
        P("ep", "tp"), P("ep", "tp"), P("ep", "tp"), P("ep", "tp"), P("ep", "tp"), P("ep", "tp"),
        P("tp"), P("ep", "tp", None, None), P("ep", "tp"), P("tp"), P("tp", "ep"), P(),
        P("ep", None), P("ep", None),
        P("ep", None, "tp"), P("ep", None, "tp"), P("ep", "tp", None),
        P(("ep", "tp"), None), P(("ep", "tp"), None), P(("ep", "tp"), None), P(),
    )
    out_specs = (P("ep", "tp"), P("ep", "tp", None, None), P("ep", "tp"))
    return jax.shard_map(body, mesh=mesh, in_specs=in_specs, out_specs=out_specs, check_vma=False)
```

```python
import jax
import jax.numpy as jnp
from jax import lax
from jax.experimental import pallas as pl
from jax.experimental.pallas import tpu as pltpu
from jax.sharding import PartitionSpec as P

norm_eps = 1e-05
clamp_limit = 7.0
sigmoid_slope = 1.702
F32 = jnp.float32
BF16 = jnp.bfloat16
MESH = pl.DeviceIdType.MESH
VMEM_SPEC = pl.BlockSpec(memory_space=pltpu.VMEM)
ANY_SPEC = pl.BlockSpec(memory_space=pl.ANY)
VMEM_LIMIT = 60 * 1024 * 1024

SIDE = 4
PLANE = 16
CHIPS = 64
ROWS = 16
SEQS = 2


def rms_scale(values, gain):
    mean_square = jnp.mean(values * values, axis=-1, keepdims=True)
    return values * lax.rsqrt(mean_square + norm_eps) * gain


def own_place():
    chip = lax.axis_index("ep")
    core = lax.axis_index("tp")
    return chip, core, chip % SIDE, chip // SIDE


def plane_shift(plane, step):
    z = (plane // SIDE + step // SIDE) % SIDE
    y = (plane % SIDE + step % SIDE) % SIDE
    return z * SIDE + y


def axis_peers(plane, x):
    z, y = plane // SIDE, plane % SIDE
    along_y = [((z * SIDE + (y + d) % SIDE) * SIDE + x) for d in range(1, SIDE)]
    along_z = [((((z + d) % SIDE) * SIDE + y) * SIDE + x) for d in range(1, SIDE)]
    along_x = [(plane * SIDE + (x + d) % SIDE) for d in range(1, SIDE)]
    return along_x, along_y, along_z


def each_chip(plane, x, act):
    xs = [(x + d) % SIDE for d in range(SIDE)]

    def on_plane(step, carry):
        base = plane_shift(plane, step) * SIDE
        for d in range(SIDE):
            act(base + xs[d])
        return carry

    lax.fori_loop(1, PLANE, on_plane, 0)
    for d in range(1, SIDE):
        act(plane * SIDE + xs[d])


def remote(src, dst, send, recv, device):
    return pltpu.make_async_remote_copy(
        src_ref=src, dst_ref=dst, send_sem=send, recv_sem=recv,
        device_id=device, device_id_type=MESH,
    )


def drain(ref, sem):
    pltpu.make_async_copy(ref, ref, sem).wait()


def identity(n):
    row = lax.broadcasted_iota(jnp.int32, (n, n), 0)
    return (row == lax.broadcasted_iota(jnp.int32, (n, n), 1)).astype(F32)


def turned(values):
    rows = values.shape[0]
    return lax.dot_general(
        identity(values.shape[1]), values, (((1,), (1,)), ((), ())),
        preferred_element_type=F32, precision=lax.Precision.HIGHEST,
    ).reshape(values.shape[1], rows)


def memory_gates(gates, bias, stab_t):
    stab = turned(stab_t)
    input_pre = gates[:, 0:4]
    forget = pltpu.roll(gates, 124, 1)[:, 0:4] + bias
    log_forget = jnp.minimum(forget, 0.0) - jnp.log1p(jnp.exp(-jnp.abs(forget)))
    stab_new = jnp.maximum(log_forget + stab, input_pre)
    return stab_new, jnp.exp(log_forget + stab - stab_new), jnp.exp(input_pre - stab_new)


def head_cols(part, h):
    return slice(512 * part + 128 * h, 512 * part + 128 * h + 128)


def upright(rows):
    return jnp.concatenate([rows, jnp.zeros((112, 128), F32)], axis=0).T


def memory_kernel(
    carr_hbm, keys_hbm, vt_hbm, stab_hbm, mem_ref, mixed_hbm,
    new_ref, stab_new_ref, mixed_ref,
    memv, carr, keys, vt, small_sem, load_sem, store_sem,
):
    small = [
        pltpu.make_async_copy(src, dst, small_sem.at[k])
        for k, (src, dst) in enumerate((
            (carr_hbm, carr), (keys_hbm, keys), (vt_hbm, vt), (stab_hbm, stab_new_ref), (mixed_hbm, mixed_ref),
        ))
    ]
    for copy in small:
        copy.start()

    def part(i):
        return pl.ds(SEQS * i, SEQS)

    def load(i):
        return pltpu.make_async_copy(mem_ref.at[part(i)], memv.at[part(i)], load_sem.at[i])

    def store(i):
        return pltpu.make_async_copy(memv.at[part(i)], new_ref.at[part(i)], store_sem)

    for i in range(3):
        load(i).start()
    for copy in small:
        copy.wait()
    def advance(i, carry):
        load(i).wait()

        @pl.when(i + 3 < ROWS // SEQS)
        def _():
            load(i + 3).start()

        for h in range(4):
            values = vt[h]
            for j in range(SEQS):
                place = pl.ds(SEQS * i + j, 1)
                memv[SEQS * i + j, h] = (
                    carr[h, place, :] * memv[SEQS * i + j, h] + values[:, j:j + 1] * keys[h, place, :]
                )
            vt[h] = pltpu.roll(values, 128 - SEQS, 1)
        store(i).start()
        return carry

    lax.fori_loop(0, ROWS // SEQS, advance, 0)
    drain(memv, store_sem)


def memory_update(carried, keys, values, stab_new, memory, mixed):
    dma = pltpu.SemaphoreType.DMA
    vm = pltpu.VMEM
    return pl.pallas_call(
        memory_kernel,
        out_shape=(
            jax.ShapeDtypeStruct((ROWS, 4, 128, 128), F32),
            jax.ShapeDtypeStruct((4, ROWS), F32),
            jax.ShapeDtypeStruct((ROWS, 1024), BF16),
        ),
        in_specs=[ANY_SPEC] * 6,
        out_specs=(ANY_SPEC, VMEM_SPEC, VMEM_SPEC),
        scratch_shapes=[
            vm((ROWS, 4, 128, 128), F32), vm((4, ROWS, 128), F32), vm((4, ROWS, 128), F32), vm((4, 128, 128), F32),
            dma((5,)), dma((ROWS // SEQS,)), dma,
        ],
        compiler_params=pltpu.CompilerParams(vmem_limit_bytes=VMEM_LIMIT),
        name="memory_update",
    )(carried, keys, values, stab_new, memory, mixed)


def step_kernel(
    tok_hbm, gain1_hbm, wq_ref, wk_ref, wv_ref, wo_ref, wi_ref, wf_ref, mix_ref, dg_ref, du_ref, dd_ref,
    mem_ref, bias_hbm, stab_hbm, hgain_hbm, gain_hbm, route_hbm, weight_hbm, eg_ref, eu_ref, ed_ref, scale_hbm,
    out_ref, carr_ref, keys_ref, vt_ref, stab_new_ref,
    gainv, wiv, wfv, wbuf, gbuf, nbuf, abuf, pbuf, sbuf, tbuf, rbuf,
    memv, rows_ref, gates_ref, bias_ref, stab_ref, hgain_ref, rt, queries, gated_ref,
    tok_ref, gain_ref, route_ref, weight_ref, scale_ref,
    egv, euv, edv, dgv, duv, ddv, mixv, gx, asend, tb, ns, res, n2, sel, comb_hi, comb_lo, obuf, rx,
    xbuf, gacc, uacc, hbuf, yown, ysend, yrecv, yret, rret, da, dout, dr,
    load1_sem, w_send, w_recv, g_send, g_recv, a_send, a_recv, m_send, m_recv, p_send, p_recv, r_send, r_recv,
    dx_send, dx_recv, near_sem, late_sem,
    load_sem, gx_send, gx_recv, tb_send, tb_recv, x_send, x_recv, da_send, da_recv,
    y_send, y_recv, q_send, q_recv, dr_send, dr_recv, xo_send, xo_recv, d_send, d_recv, mem_sem, down_send, down_recv,
):
    chip, core, x, plane = own_place()
    z, y = plane // SIDE, plane % SIDE
    right = plane * SIDE + (x + 1) % SIDE
    left = plane * SIDE + (x + 3) % SIDE
    across = plane * SIDE + (x + 2) % SIDE
    xl, xr = (x + 3) % SIDE, (x + 1) % SIDE

    other, xa = 1 - core, (x + 2) % SIDE
    barrier = pltpu.get_barrier_semaphore()
    along_x, along_y, along_z = axis_peers(plane, x)
    for peer in along_z + along_x + along_y:
        pl.semaphore_signal(barrier, inc=1, device_id=(peer, core), device_id_type=MESH)
    pl.semaphore_signal(barrier, inc=1, device_id=(chip, other), device_id_type=MESH)

    def w_rows(xs):
        return pl.ds(pl.multiple_of(32 * xs, 32), 32)

    def half_rows(xs, half):
        return pl.ds(pl.multiple_of(32 * xs + 16 * half, 16), 16)

    for k, ref in enumerate((wq_ref, wk_ref, wv_ref, wo_ref)):
        load = pltpu.make_async_copy(ref, wbuf.at[w_rows(x), pl.ds(512 * k, 512)], load1_sem.at[0])
        load.start()
    small = [
        pltpu.make_async_copy(src, dst, load1_sem.at[2 + k])
        for k, (src, dst) in enumerate(((tok_hbm, tok_ref), (gain1_hbm, gainv), (wi_ref, wiv), (wf_ref, wfv)))
    ]
    for load in small:
        load.start()
    late = [
        pltpu.make_async_copy(src, dst, late_sem.at[k])
        for k, (src, dst) in enumerate((
            (route_hbm, route_ref), (weight_hbm, weight_ref), (bias_hbm, bias_ref), (stab_hbm, stab_ref),
            (hgain_hbm, hgain_ref), (gain_hbm, gain_ref), (scale_hbm, scale_ref),
        ))
    ]
    for load in small:
        load.wait()

    normed = rms_scale(tok_ref[...].astype(F32), gainv[...])
    nbuf[...] = normed.astype(BF16)
    place = (
        lax.broadcasted_iota(jnp.int32, (32, 128), 1) == lax.broadcasted_iota(jnp.int32, (32, 128), 0) + 32 * x
    ).astype(F32)
    gate_in = jnp.dot(wiv[...].astype(F32), place, preferred_element_type=F32)
    gate_fo = jnp.dot(wfv[...].astype(F32), place, preferred_element_type=F32)
    gbuf[x] = jnp.concatenate([gate_in, gate_fo], axis=0)
    drain(wbuf.at[w_rows(x), :], load1_sem.at[0])
    pl.semaphore_wait(barrier, 9 + 1)
    for peer in along_y:
        pl.semaphore_signal(near_sem, inc=1, device_id=(peer, core), device_id_type=MESH)

    def w_copy(k, kind, xs, part, device):
        rows = w_rows(xs) if part is None else half_rows(xs, part)
        block = wbuf.at[rows, pl.ds(512 * k, 512)]
        return remote(block, block, w_send, w_recv.at[k, kind], (device, core))

    for k in range(4):
        w_copy(k, 0, x, None, right).start()
        w_copy(k, 1, x, None, left).start()
    for peer in (right, left, across):
        remote(gbuf.at[x], gbuf.at[x], g_send, g_recv, (peer, core)).start()

    def token_copy(step):
        peer = plane_shift(plane, step)
        return remote(
            nbuf.at[:, pl.ds(pl.multiple_of(128 * peer, 128), 128)],
            abuf.at[pl.ds(pl.multiple_of(ROWS * plane, ROWS), ROWS), :],
            a_send, a_recv, (peer * SIDE + x, core),
        )

    def plane_peer(axis, step):
        if axis == 0:
            return (z + step) % SIDE, y
        return z, (y + step) % SIDE

    def device_of(zt, yt):
        return ((zt * SIDE + yt) * SIDE + x, core)

    def mix_first(axis, step):
        part = pl.ds(16 * axis, 16)
        return remote(
            mix_ref.at[part], mixv.at[z, y, part], m_send, m_recv.at[axis], device_of(*plane_peer(axis, step))
        )

    def mix_second(axis, step):
        part = pl.ds(16 * (1 - axis), 16)
        block = mixv.at[z, :, part] if axis == 0 else mixv.at[:, y, part]
        return remote(block, block, m_send, m_recv.at[2 + axis], device_of(*plane_peer(axis, step)))

    def start_tokens(step, carry):
        token_copy(step).start()
        return carry

    pl.semaphore_wait(near_sem, 3)
    lax.fori_loop(1, PLANE, start_tokens, 0)
    abuf[pl.ds(pl.multiple_of(ROWS * plane, ROWS), ROWS), :] = nbuf[:, pl.ds(pl.multiple_of(128 * plane, 128), 128)]
    for axis in range(2):
        for d in (2, 1, 3):
            mix_first(axis, d).start()
    mix_own = pltpu.make_async_copy(mix_ref, mixv.at[z, y], load1_sem.at[1])
    mix_own.start()

    dense = ((dg_ref, dgv), (du_ref, duv))

    def dense_copy(k, kind, xs, part, device):
        block = dense[k][1].at[2 * xs + core]
        if part is not None:
            block = block.at[pl.ds(16 * part, 16)]
        source = dense[k][0] if kind in (0, 1) else block
        return remote(source, block, dx_send.at[k], dx_recv.at[kind], device)

    def w_relay(k):
        w_copy(k, 0, x, None, right).wait_recv()
        w_copy(k, 2, xl, 0, right).start()
        w_copy(k, 1, x, None, left).wait_recv()
        w_copy(k, 3, xr, 1, left).start()

    for load in late:
        load.start()
    def mem_load(i):
        part = pl.ds(4 * i, 4)
        return pltpu.make_async_copy(mem_ref.at[part], memv.at[part], mem_sem.at[i])

    for i in range(4):
        mem_load(i).start()
    for k in range(3):
        own_load = pltpu.make_async_copy((dg_ref, du_ref, dd_ref)[k], (dgv, duv, ddv)[k].at[2 * x + core], load_sem.at[3 + k])
        own_load.start()
    late[0].wait()
    late[1].wait()
    spread = (
        lax.broadcasted_iota(jnp.int32, (ROWS, 128), 1) % ROWS == lax.broadcasted_iota(jnp.int32, (ROWS, 128), 0)
    ).astype(F32)
    route = jnp.dot(route_ref[...].astype(F32), spread, preferred_element_type=F32, precision=lax.Precision.HIGHEST)
    weight = jnp.dot(weight_ref[...], spread, preferred_element_type=F32, precision=lax.Precision.HIGHEST)
    expert = lax.broadcasted_iota(jnp.int32, (CHIPS, 128), 0).astype(F32)
    hit = jnp.zeros((CHIPS, 128), F32)
    chosen = jnp.zeros((CHIPS, 128), F32)
    for k in range(4):
        same = (route[k:k + 1, :] == expert).astype(F32)
        hit = hit + same
        chosen = chosen + same * weight[k:k + 1, :]
    col = lax.broadcasted_iota(jnp.int32, (128, 128), 1) % ROWS
    row = lax.broadcasted_iota(jnp.int32, (128, 128), 0)
    before = ((row < ROWS) & (row < col)).astype(F32)
    rank = jnp.dot(hit, before, preferred_element_type=F32)
    first = hit * (rank == 0.0).astype(F32)
    second = hit * (rank == 1.0).astype(F32)
    block_row = lax.broadcasted_iota(jnp.int32, (8, 128), 0)
    block_col = lax.broadcasted_iota(jnp.int32, (8, 128), 1) // ROWS
    diagonal = (block_row == block_col).astype(F32)

    def widened(top, bottom):
        low = top[:, None, :] * diagonal[None, :, :]
        high = bottom[:, None, :] * diagonal[None, :, :]
        return jnp.concatenate([low, high], axis=1).reshape(1024, 128)

    sel[...] = widened(first, second).astype(BF16)
    comb = widened(first * chosen, second * chosen).T
    comb_top = comb.astype(BF16)
    comb_hi[...] = comb_top
    comb_lo[...] = (comb - comb_top.astype(F32)).astype(BF16)
    for k in range(4):
        w_relay(k)
    for k in range(2):
        dense_copy(k, 0, x, None, (right, core)).start()
        dense_copy(k, 1, x, None, (left, core)).start()
    drain(abuf.at[pl.ds(0, 240), :], a_recv)
    drain(gbuf.at[pl.ds(0, 3)], g_recv)
    gate_w = (gbuf[0] + gbuf[1] + gbuf[2] + gbuf[3]).astype(BF16)
    gate_w = jnp.concatenate([gate_w.astype(F32), jnp.zeros((120, 128), F32)], axis=0).astype(BF16)
    def columns(k):
        return pl.ds(512 * k, 640 if k == 3 else 512)

    def first_sum(k, step):
        axis = (k + 1) % 2
        zt, yt = plane_peer(axis, step)
        src = pbuf.at[zt, :, :, columns(k)] if axis == 0 else pbuf.at[:, yt, :, columns(k)]
        own = z if axis == 0 else y
        return remote(src, sbuf.at[own, :, :, columns(k)], p_send, p_recv.at[k], device_of(zt, yt))

    def second_sum(k, step):
        axis = k % 2
        zt, yt = plane_peer(axis, step)
        target, own = (zt, z) if axis == 0 else (yt, y)
        return remote(
            tbuf.at[target, :, columns(k)], rbuf.at[own, :, columns(k)], r_send, r_recv.at[k], device_of(zt, yt)
        )

    for k in range(4):
        w_copy(k, 2, xl, 0, right).wait_recv()
        w_copy(k, 3, xr, 1, left).wait_recv()
        cols = slice(512 * k, 512 * k + 512)
        part = jnp.dot(abuf[...], wbuf[:, cols], preferred_element_type=F32).astype(BF16)
        pbuf[:, :, :, cols] = part.reshape(SIDE, SIDE, ROWS, 512)
        if k == 3:
            gates = lax.dot_general(abuf[...], gate_w, (((1,), (1,)), ((), ())), preferred_element_type=F32)
            high = gates.astype(BF16).astype(F32)
            part = (high + pltpu.roll(gates - high, 8, 1)).astype(BF16)
            pbuf[:, :, :, 2048:2176] = part.reshape(SIDE, SIDE, ROWS, 128)
        for d in (2, 1, 3):
            first_sum(k, d).start()
    loads = []
    for k, (src, dst) in enumerate(((eg_ref, egv), (eu_ref, euv), (ed_ref, edv))):
        loads.append(pltpu.make_async_copy(src.at[0], dst, load_sem.at[k]))
    for load in loads:
        load.start()
    mix_own.wait()
    for axis in range(2):
        drain(mixv.at[0, pl.ds(0, 3), pl.ds(0, 16)], m_recv.at[1 - axis])
        for d in (2, 1, 3):
            mix_second(axis, d).start()
    first_lanes = lax.broadcasted_iota(jnp.int32, (ROWS, 128), 1) < 8
    for k in range(4):
        cols = slice(512 * k, 2176 if k == 3 else 512 * k + 512)
        if k % 2 == 0:
            sbuf[y, :, :, cols] = pbuf[:, y, :, cols]
        else:
            sbuf[z, :, :, cols] = pbuf[z, :, :, cols]
        drain(sbuf.at[pl.ds(0, 3), :, :, columns(k)], p_recv.at[k])
        for t in range(SIDE):
            total = sbuf[0, t, :, cols].astype(F32)
            for s in range(1, SIDE):
                total = total + sbuf[s, t, :, cols].astype(F32)
            if k == 3:
                gates = total[:, 512:640]
                gates = jnp.where(first_lanes, gates + pltpu.roll(gates, 120, 1), 0.0)
                high = gates.astype(BF16).astype(F32)
                total = jnp.concatenate([total[:, :512], high + pltpu.roll(gates - high, 8, 1)], axis=1)
            tbuf[t, :, cols] = total.astype(BF16)
        for d in (2, 1, 3):
            second_sum(k, d).start()
        if k % 2 == 0:
            rbuf[z, :, cols] = tbuf[z, :, cols]
        else:
            rbuf[y, :, cols] = tbuf[y, :, cols]

    two, twohalf = dgv.at[pl.ds(0, 2)], dgv.at[pl.ds(0, 2), pl.ds(0, 16)]
    drain(two, dx_recv.at[0])
    for k in range(2):
        dense_copy(k, 2, xl, 0, (right, core)).start()
    drain(two, dx_recv.at[1])
    for k in range(2):
        dense_copy(k, 3, xr, 1, (left, core)).start()
    for k in range(4):
        cols = slice(512 * k, 512 * k + 512)
        drain(rbuf.at[pl.ds(0, 3), :, columns(k)], r_recv.at[k])
        total = rbuf[0, :, cols].astype(F32)
        for s in range(1, SIDE):
            total = total + rbuf[s, :, cols].astype(F32)
        rows_ref[:, cols] = total.astype(BF16)
    total = rbuf[0, :, 2048:2176].astype(F32)
    for s in range(1, SIDE):
        total = total + rbuf[s, :, 2048:2176].astype(F32)
    gates_ref[...] = total + pltpu.roll(total, 120, 1)

    for load in late[2:]:
        load.wait()
    stab_new, carried, written = memory_gates(gates_ref[...], bias_ref[...], stab_ref[...])
    for h in range(4):
        query = upright(rows_ref[:, head_cols(0, h)].astype(F32)).astype(BF16)
        queries[h] = jnp.concatenate([query, query], axis=0)
    lane_index = lax.broadcasted_iota(jnp.int32, (128, 128), 1)

    def read_part(i, carry):
        mem_load(i).wait()
        for h in range(4):
            stored = memv[pl.ds(4 * i, 4), h].reshape(512, 128)
            top = stored.astype(BF16)
            rest = (stored - top.astype(F32)).astype(BF16)
            read = jnp.dot(jnp.concatenate([top, rest], axis=1), queries[h], preferred_element_type=F32)
            reads = rt[h]
            for j in range(4):
                reads = jnp.where(lane_index == 4 * i + j, read[128 * j:128 * j + 128, :], reads)
            rt[h] = reads
        return carry

    rt[...] = jnp.zeros(rt.shape, F32)
    lax.fori_loop(0, 4, read_part, 0)
    for h in range(4):
        query = rows_ref[:, head_cols(0, h)].astype(F32)
        key = rows_ref[:, head_cols(1, h)].astype(F32) * (128 ** (-0.5))
        value = rows_ref[:, head_cols(2, h)].astype(F32)
        match = jnp.sum(key * query, axis=1, keepdims=True) * written[:, h:h + 1]
        readout = carried[:, h:h + 1] * rt[h].T[0:ROWS, :] + match * value
        gate = jax.nn.sigmoid(rows_ref[:, head_cols(3, h)].astype(F32))
        scaled = rms_scale(readout, hgain_ref[:, head_cols(0, h)])
        gated_ref[:, head_cols(0, h)] = (scaled * gate).astype(BF16)

    gx[pl.ds(pl.multiple_of(ROWS * x, ROWS), ROWS), :] = gated_ref[...]

    def gx_copy(d):
        rows = pl.ds(pl.multiple_of(ROWS * x, ROWS), ROWS)
        peer = plane * SIDE + (x + d) % SIDE
        return remote(gated_ref, gx.at[rows, :], gx_send, gx_recv, (peer, core))

    for d in range(1, SIDE):
        gx_copy(d).start()
    def down_copy(kind, xs, part, device):
        block = ddv.at[2 * xs + core]
        if part is not None:
            block = block.at[pl.ds(16 * part, 16)]
        if kind == 4:
            return remote(block, block, d_send.at[2], d_recv.at[2], (chip, other))
        return remote(dd_ref if kind < 2 else block, block, down_send, down_recv.at[kind], (device, core))

    stab_new_ref[...] = turned(stab_new)
    for h in range(4):
        key = rows_ref[:, head_cols(1, h)].astype(F32) * (128 ** (-0.5))
        carr_ref[h] = jnp.broadcast_to(carried[:, h:h + 1], (ROWS, 128))
        keys_ref[h] = key * written[:, h:h + 1]
        vt_ref[h] = upright(rows_ref[:, head_cols(2, h)].astype(F32))
    for axis in range(2):
        drain(mixv.at[pl.ds(0, 3), :, pl.ds(0, 16)], m_recv.at[2 + axis])
    drain(gx.at[pl.ds(0, 48), :], gx_recv)
    asend[...] = lax.dot_general(
        gx[...], mixv[...].reshape(512, 512), (((1,), (1,)), ((), ())), preferred_element_type=F32
    ).astype(BF16)

    def tb_copy(d, side):
        rows = pl.ds(pl.multiple_of(ROWS * ((x + d) % SIDE), ROWS), ROWS)
        peer = plane * SIDE + (x + d) % SIDE
        return remote(
            asend.at[rows, :], tb.at[core, x], tb_send, tb_recv,
            (peer, (core + side) % 2),
        )

    tb_list = [(0, 1)] + [(d, side) for d in (2, 1, 3) for side in (0, 1)]
    for d, side in tb_list:
        tb_copy(d, side).start()
    tb[core, x] = asend[pl.ds(pl.multiple_of(ROWS * x, ROWS), ROWS), :]
    down_copy(0, x, None, right).start()
    down_copy(1, x, None, left).start()
    tb_bytes = rx.at[pl.ds(0, 448), :]
    drain(tb_bytes, tb_recv)
    drain(twohalf, dx_recv.at[2])
    drain(twohalf, dx_recv.at[3])
    for k, (own, dst) in enumerate(((dg_ref, dgv), (du_ref, duv), (dd_ref, ddv))):
        for s in range(SIDE if k < 2 else 1):
            slot = dst.at[2 * ((x + s) % SIDE) + core]
            remote(own if s == 0 else slot, slot, d_send.at[k], d_recv.at[k], (chip, other)).start()
    attended = [tb[0, k].astype(F32) + tb[1, k].astype(F32) for k in range(SIDE)]
    lane = lax.broadcasted_iota(jnp.int32, (ROWS, 128), 1) // 32
    tiles = []
    for t in range(PLANE):
        tile = None
        for k in range(SIDE):
            part = attended[k][:, 128 * (t // 4):128 * (t // 4) + 128]
            shift = (32 * k - 32 * (t % 4)) % 128
            if shift:
                part = pltpu.roll(part, shift, 1)
            tile = part if tile is None else jnp.where(lane == k, part, tile)
        tiles.append(tile)
    residual = (tok_ref[...].astype(F32) + jnp.concatenate(tiles, axis=1)).astype(BF16)
    res[...] = residual
    normed = rms_scale(residual.astype(F32), gain_ref[...]).astype(BF16)
    ns[...] = normed
    def tile_rows(index):
        return pl.ds(pl.multiple_of(ROWS * index, ROWS), ROWS)

    parity = plane % 2
    half = plane // 2

    own_row = y // 2
    low, high = pl.ds(0, 1024), pl.ds(1024, 1024)

    def acts_first(axis, d):
        peer = (along_z, along_y)[axis][d]
        cols = (low, high)[axis]
        return remote(
            ns.at[:, cols], da.at[z, own_row, :, cols], da_send.at[0], da_recv.at[axis], (peer, parity)
        )

    def acts_second(axis, d):
        peer = (along_z, along_y)[axis][d]
        block = da.at[z, :, :, high] if axis == 0 else da.at[:, own_row, :, low]
        return remote(block, block, da_send.at[1 + axis], da_recv.at[2 + axis], (peer, core))

    for axis in range(2):
        @pl.when(core == axis)
        def _():
            for d in (1, 0, 2):
                acts_first(axis, d).start()

    @pl.when(parity == core)
    def _():
        da[z, own_row] = ns[...]

    for b in range(8):
        cols = pl.ds(pl.multiple_of(1024 * core + 128 * b, 128), 128)
        n2[16 * b:16 * b + 16, :] = ns[:, cols]
    for k in range(4):
        obuf[256 * k:256 * k + 256, :] = jnp.dot(
            sel[256 * k:256 * k + 256, :], n2[...], preferred_element_type=F32
        ).astype(BF16)

    def x_copy(peer):
        return remote(
            obuf.at[tile_rows(peer), :], rx.at[tile_rows(chip), :], x_send, x_recv, (peer, core)
        )

    each_chip(plane, x, lambda peer: x_copy(peer).start())
    rx[tile_rows(chip), :] = obuf[tile_rows(chip), :]

    down_copy(0, x, None, right).wait_recv()
    down_copy(2, xl, 0, right).start()
    down_copy(1, x, None, left).wait_recv()
    down_copy(3, xr, 1, left).start()
    down_copy(4, xl, None, chip).start()
    down_copy(4, xr, None, chip).start()
    row_of = da.at[0, 0, :, low]

    @pl.when(parity == core)
    def _():
        drain(row_of, da_recv.at[1])
        drain(da.at[pl.ds(0, 3), 0, :, low], da_recv.at[0])
        for d in (1, 0, 2):
            acts_second(1, d).start()

    @pl.when(parity != core)
    def _():
        drain(da.at[pl.ds(0, 2), 0, :, low], da_recv.at[1])

    for d in (1, 0, 2):
        acts_second(0, d).start()

    drain(rx.at[pl.ds(0, 1008), :], x_recv)
    row = lax.broadcasted_iota(jnp.int32, (256, 256), 0)
    col = lax.broadcasted_iota(jnp.int32, (256, 256), 1)
    gather = (col == ((row % 32) // 2) * 16 + (row % 2) * 8 + row // 32).astype(F32).astype(BF16)
    scatter = (row == ((col % 32) // 2) * 16 + (col % 2) * 8 + col // 32).astype(F32).astype(BF16)
    for g in range(4):
        mixed_up = jnp.dot(gather, rx[256 * g:256 * g + 256, :], preferred_element_type=F32).astype(BF16)
        for b in range(8):
            xbuf[core, 32 * g:32 * g + 32, 128 * b:128 * b + 128] = mixed_up[32 * b:32 * b + 32, :]
    swap = remote(xbuf.at[core], xbuf.at[core], xo_send, xo_recv, (chip, other))
    swap.start()
    loads[0].wait()
    loads[1].wait()

    def expert_up_near(t, carry):
        cols = pl.ds(pl.multiple_of(256 * t, 256), 256)
        depth = pl.ds(pl.multiple_of(1024 * core, 1024), 1024)
        gacc[:, cols] = jnp.dot(xbuf[core], egv[depth, cols], preferred_element_type=F32)
        uacc[:, cols] = jnp.dot(xbuf[core], euv[depth, cols], preferred_element_type=F32)
        return carry

    def expert_up_far(t, carry):
        cols = pl.ds(pl.multiple_of(256 * t, 256), 256)
        depth = pl.ds(pl.multiple_of(1024 * other, 1024), 1024)
        gate_pre = gacc[:, cols] + jnp.dot(xbuf[other], egv[depth, cols], preferred_element_type=F32)
        up_pre = uacc[:, cols] + jnp.dot(xbuf[other], euv[depth, cols], preferred_element_type=F32)
        gate_clamped = jnp.minimum(gate_pre, clamp_limit)
        up_clamped = jnp.clip(up_pre, -clamp_limit, clamp_limit)
        hbuf[:, cols] = (
            (up_clamped + 1.0) * gate_clamped * jax.nn.sigmoid(sigmoid_slope * gate_clamped)
        ).astype(BF16)
        return carry

    lax.fori_loop(0, 4, expert_up_near, 0)
    for k, dst in enumerate((dgv, duv)):
        drain(dst.at[0], load_sem.at[3 + k])
        drain(dst.at[pl.ds(0, 4)], d_recv.at[k])

    @pl.when(parity == core)
    def _():
        drain(da.at[:, 0, :, low], da_recv.at[3])

    @pl.when(parity != core)
    def _():
        drain(da.at[:, :, :, low], da_recv.at[3])

    drain(da.at[pl.ds(0, 3), :, :, low], da_recv.at[2])

    down_copy(2, xa, 0, right).wait_recv()
    down_copy(3, xa, 1, left).wait_recv()
    down_copy(4, xa, None, chip).start()
    dense_rows = da[...].reshape(128, 2048)
    over_last = (((1,), (1,)), ((), ()))
    gate_rows = lax.dot_general(dense_rows, dgv[...].reshape(256, 2048), over_last, preferred_element_type=F32)
    lift_rows = lax.dot_general(dense_rows, duv[...].reshape(256, 2048), over_last, preferred_element_type=F32)
    activity = (gate_rows / (1.0 + jnp.exp(-gate_rows)) * lift_rows).astype(BF16)
    drain(ddv.at[0], load_sem.at[5])
    drain(ddv.at[pl.ds(0, 4)], d_recv.at[2])
    down = ddv[...].reshape(256, 2048)
    for h in range(2):
        for t in range(2):
            lower = 1024 * h + 512 * t
            part = jnp.dot(activity, down[:, lower:lower + 512], preferred_element_type=F32).astype(BF16)
            dout[h, :, 512 * t:512 * t + 512] = part

    def dr_copy(index, h):
        target = 2 * index + core
        return remote(
            dout.at[h, tile_rows(index), :], dr.at[plane], dr_send, dr_recv,
            (target * SIDE + x, h),
        )

    def start_dr(index, carry):
        for h in range(2):
            @pl.when((2 * index + core != plane) | (core != h))
            def _():
                dr_copy(index, h).start()
        return carry

    lax.fori_loop(0, 8, start_dr, 0)

    @pl.when(parity == core)
    def _():
        dr[plane] = dout[core, tile_rows(half), :]

    swap.wait_recv()
    lax.fori_loop(0, 4, expert_up_far, 0)
    loads[2].wait()

    def y_copy(t):
        return remote(ysend.at[t], yrecv.at[t], y_send, y_recv, (chip, other))

    def expert_down_far(t, carry):
        cols = pl.ds(pl.multiple_of(1024 * other + 256 * t, 256), 256)
        ysend[t] = jnp.dot(hbuf[...], edv[:, cols], preferred_element_type=F32).astype(BF16)
        y_copy(t).start()
        return carry

    def expert_down_near(t, carry):
        cols = pl.ds(pl.multiple_of(1024 * core + 256 * t, 256), 256)
        yown[t] = jnp.dot(hbuf[...], edv[:, cols], preferred_element_type=F32).astype(BF16)
        return carry

    lax.fori_loop(0, 4, expert_down_far, 0)
    lax.fori_loop(0, 4, expert_down_near, 0)

    drain(yrecv, y_recv)
    for g in range(4):
        rows = slice(32 * g, 32 * g + 32)
        stacked = []
        for t in range(4):
            both = (yown[t, rows, :].astype(F32) + yrecv[t, rows, :].astype(F32)).astype(BF16)
            stacked += [both[:, :128], both[:, 128:]]
        yret[256 * g:256 * g + 256, :] = jnp.dot(
            scatter, jnp.concatenate(stacked, axis=0), preferred_element_type=F32
        ).astype(BF16)

    def q_copy(peer):
        return remote(
            yret.at[tile_rows(peer), :], rret.at[tile_rows(chip), :], q_send, q_recv, (peer, core)
        )

    each_chip(plane, x, lambda peer: q_copy(peer).start())
    rret[tile_rows(chip), :] = yret[tile_rows(chip), :]

    @pl.when(parity == core)
    def _():
        drain(dr.at[pl.ds(0, 15)], dr_recv)

    @pl.when(parity != core)
    def _():
        drain(dr, dr_recv)

    branch = dr[0].astype(F32)
    for s in range(1, PLANE):
        branch = branch + dr[s].astype(F32)

    drain(rret.at[pl.ds(0, 1008), :], q_recv)
    returned = rret[...]
    routed = jnp.dot(comb_hi[...], returned, preferred_element_type=F32) + jnp.dot(
        comb_lo[...], returned, preferred_element_type=F32
    )
    routed = jnp.concatenate([routed[16 * b:16 * b + 16, :] for b in range(8)], axis=1)
    own_cols = pl.ds(pl.multiple_of(1024 * core, 1024), 1024)
    out_ref[...] = (res[:, own_cols].astype(F32) + routed + branch * scale_ref[:, own_cols]).astype(BF16)

    drain(gx.at[pl.ds(0, 48), :], gx_send)
    drain(tb_bytes, tb_send)
    drain(rx.at[pl.ds(0, 1008), :], x_send)
    drain(rret.at[pl.ds(0, 1008), :], q_send)
    drain(yrecv, y_send)
    drain(xbuf.at[0], xo_send)
    for k, dst in enumerate((dgv, duv, ddv)):
        drain(dst.at[pl.ds(0, 4)], d_send.at[k])
    drain(ddv.at[pl.ds(0, 3)], down_send)

    drain(da.at[pl.ds(0, 3), 0, :, low], da_send.at[0])
    drain(da.at[pl.ds(0, 3), :, :, low], da_send.at[1])

    @pl.when(parity == core)
    def _():
        drain(da.at[pl.ds(0, 3)], da_send.at[2])

    @pl.when(parity == core)
    def _():
        drain(dr.at[pl.ds(0, 15)], dr_send)

    @pl.when(parity != core)
    def _():
        drain(dr, dr_send)
    drain(wbuf.at[pl.ds(0, 96), :], w_send)
    drain(gbuf.at[pl.ds(0, 3)], g_send)
    drain(abuf.at[pl.ds(0, 240), :], a_send)
    drain(mixv.at[pl.ds(0, 3), :, :], m_send)
    drain(mixv.at[0, pl.ds(0, 3)], m_send)
    drain(sbuf.at[pl.ds(0, 3)], p_send)
    drain(rbuf.at[pl.ds(0, 3)], r_send)
    for k in range(2):
        drain(dense[k][1].at[pl.ds(0, 3)], dx_send.at[k])


def decode_step(*operands):
    dma = pltpu.SemaphoreType.DMA
    vm = pltpu.VMEM
    return pl.pallas_call(
        step_kernel,
        out_shape=(
            jax.ShapeDtypeStruct((ROWS, 1024), BF16),
            jax.ShapeDtypeStruct((4, ROWS, 128), F32),
            jax.ShapeDtypeStruct((4, ROWS, 128), F32),
            jax.ShapeDtypeStruct((4, 128, 128), F32),
            jax.ShapeDtypeStruct((4, ROWS), F32),
        ),
        in_specs=[ANY_SPEC] * 23,
        out_specs=(VMEM_SPEC,) * 5,
        scratch_shapes=[
            vm((1, 2048), F32), vm((4, 32), BF16), vm((4, 32), BF16), vm((128, 2048), BF16), vm((4, 8, 128), F32),
            vm((ROWS, 2048), BF16), vm((256, 128), BF16),
            vm((SIDE, SIDE, ROWS, 2176), BF16), vm((SIDE, SIDE, ROWS, 2176), BF16),
            vm((SIDE, ROWS, 2176), BF16), vm((SIDE, ROWS, 2176), BF16),
            vm((ROWS, 4, 128, 128), F32), vm((ROWS, 2048), BF16), vm((ROWS, 128), F32), vm((1, 4), F32),
            vm((4, ROWS), F32), vm((1, 512), F32), vm((4, 128, 128), F32), vm((4, 256, 128), BF16),
            vm((ROWS, 512), BF16), vm((ROWS, 2048), BF16), vm((1, 2048), F32),
            vm((4, ROWS), jnp.int32), vm((4, ROWS), F32), vm((1, 2048), F32),
            vm((2048, 1024), BF16), vm((2048, 1024), BF16), vm((1024, 2048), BF16),
            vm((8, 32, 2048), BF16), vm((8, 32, 2048), BF16), vm((8, 32, 2048), BF16),
            vm((SIDE, SIDE, 32, 512), BF16),
            vm((64, 512), BF16), vm((64, 512), BF16), vm((2, 4, ROWS, 512), BF16),
            vm((ROWS, 2048), BF16), vm((ROWS, 2048), BF16), vm((128, 128), BF16),
            vm((1024, 128), BF16), vm((128, 1024), BF16), vm((128, 1024), BF16),
            vm((1024, 128), BF16), vm((1024, 128), BF16), vm((2, 128, 1024), BF16),
            vm((128, 1024), F32), vm((128, 1024), F32), vm((128, 1024), BF16),
            vm((4, 128, 256), BF16), vm((4, 128, 256), BF16), vm((4, 128, 256), BF16),
            vm((1024, 128), BF16), vm((1024, 128), BF16),
            vm((SIDE, 2, ROWS, 2048), BF16), vm((2, 128, 1024), BF16), vm((PLANE, ROWS, 1024), BF16),
            dma((6,)),
            dma, dma((4, 4)),
            dma, dma,
            dma, dma,
            dma, dma((4,)),
            dma, dma((4,)),
            dma, dma((4,)),
            dma((2,)), dma((4,)),
            pltpu.SemaphoreType.REGULAR, dma((7,)),
            dma((6,)),
            dma, dma,
            dma, dma,
            dma, dma,
            dma((3,)), dma((4,)),
            dma, dma,
            dma, dma,
            dma, dma,
            dma, dma,
            dma((3,)), dma((3,)),
            dma((4,)),
            dma, dma((4,)),
        ],
        compiler_params=pltpu.CompilerParams(
            collective_id=0, has_side_effects=True, vmem_limit_bytes=VMEM_LIMIT
        ),
        name="decode_step",
    )(*operands)


def body(
    tokens, norm_gain, query_weight, key_weight, value_weight, outgate_weight, input_weight, forget_weight,
    forget_bias, memory, stabilizer, head_gain, mix_weight, second_gain, route_experts, route_weight,
    expert_gate, expert_up, expert_down, dense_gate, dense_up, dense_down, branch_scale,
):
    mixed, carried, keys, values, stab_new = decode_step(
        tokens, norm_gain.reshape(1, -1), query_weight, key_weight, value_weight, outgate_weight,
        input_weight.T, forget_weight.T, mix_weight.T, dense_gate, dense_up, dense_down,
        memory, forget_bias.reshape(1, -1), stabilizer.T, head_gain.reshape(1, -1), second_gain.reshape(1, -1),
        route_experts.T, route_weight.T, expert_gate, expert_up, expert_down, branch_scale.reshape(1, -1),
    )
    memory_new, stab_new, mixed = memory_update(carried, keys, values, stab_new, memory, mixed)
    return mixed, memory_new, stab_new.T


def solution(mesh):
    in_specs = (
        P("ep", None), P(),
        P("ep", "tp"), P("ep", "tp"), P("ep", "tp"), P("ep", "tp"), P("ep", "tp"), P("ep", "tp"),
        P("tp"), P("ep", "tp", None, None), P("ep", "tp"), P("tp"), P("tp", "ep"), P(),
        P("ep", None), P("ep", None),
        P("ep", None, "tp"), P("ep", None, "tp"), P("ep", "tp", None),
        P(("ep", "tp"), None), P(("ep", "tp"), None), P(("ep", "tp"), None), P(),
    )
    out_specs = (P("ep", "tp"), P("ep", "tp", None, None), P("ep", "tp"))
    return jax.shard_map(body, mesh=mesh, in_specs=in_specs, out_specs=out_specs, check_vma=False)
```

```python
import jax
import jax.numpy as jnp
from jax import lax
from jax.experimental import pallas as pl
from jax.experimental.pallas import tpu as pltpu
from jax.sharding import PartitionSpec as P

norm_eps = 1e-05
clamp_limit = 7.0
sigmoid_slope = 1.702
F32 = jnp.float32
BF16 = jnp.bfloat16
MESH = pl.DeviceIdType.MESH
VMEM_SPEC = pl.BlockSpec(memory_space=pltpu.VMEM)
ANY_SPEC = pl.BlockSpec(memory_space=pl.ANY)
VMEM_LIMIT = 60 * 1024 * 1024

SIDE = 4
PLANE = 16
CHIPS = 64
ROWS = 16
SEQS = 2


def rms_scale(values, gain):
    mean_square = jnp.mean(values * values, axis=-1, keepdims=True)
    return values * lax.rsqrt(mean_square + norm_eps) * gain


def own_place():
    chip = lax.axis_index("ep")
    core = lax.axis_index("tp")
    return chip, core, chip % SIDE, chip // SIDE


def plane_shift(plane, step):
    z = (plane // SIDE + step // SIDE) % SIDE
    y = (plane % SIDE + step % SIDE) % SIDE
    return z * SIDE + y


def axis_peers(plane, x):
    z, y = plane // SIDE, plane % SIDE
    along_y = [((z * SIDE + (y + d) % SIDE) * SIDE + x) for d in range(1, SIDE)]
    along_z = [((((z + d) % SIDE) * SIDE + y) * SIDE + x) for d in range(1, SIDE)]
    along_x = [(plane * SIDE + (x + d) % SIDE) for d in range(1, SIDE)]
    return along_x, along_y, along_z


def each_chip(plane, x, act):
    xs = [(x + d) % SIDE for d in range(SIDE)]

    def on_plane(step, carry):
        base = plane_shift(plane, step) * SIDE
        for d in range(SIDE):
            act(base + xs[d])
        return carry

    lax.fori_loop(1, PLANE, on_plane, 0)
    for d in range(1, SIDE):
        act(plane * SIDE + xs[d])


def remote(src, dst, send, recv, device):
    return pltpu.make_async_remote_copy(
        src_ref=src, dst_ref=dst, send_sem=send, recv_sem=recv,
        device_id=device, device_id_type=MESH,
    )


def drain(ref, sem):
    pltpu.make_async_copy(ref, ref, sem).wait()


def identity(n):
    row = lax.broadcasted_iota(jnp.int32, (n, n), 0)
    return (row == lax.broadcasted_iota(jnp.int32, (n, n), 1)).astype(F32)


def turned(values):
    rows = values.shape[0]
    return lax.dot_general(
        identity(values.shape[1]), values, (((1,), (1,)), ((), ())),
        preferred_element_type=F32, precision=lax.Precision.HIGHEST,
    ).reshape(values.shape[1], rows)


def memory_gates(gates, bias, stab_t):
    stab = turned(stab_t)
    input_pre = gates[:, 0:4]
    forget = pltpu.roll(gates, 124, 1)[:, 0:4] + bias
    log_forget = jnp.minimum(forget, 0.0) - jnp.log1p(jnp.exp(-jnp.abs(forget)))
    stab_new = jnp.maximum(log_forget + stab, input_pre)
    return stab_new, jnp.exp(log_forget + stab - stab_new), jnp.exp(input_pre - stab_new)


def head_cols(part, h):
    return slice(512 * part + 128 * h, 512 * part + 128 * h + 128)


def upright(rows):
    return jnp.concatenate([rows, jnp.zeros((112, 128), F32)], axis=0).T


def memory_kernel(
    carr_hbm, keys_hbm, vt_hbm, stab_hbm, mem_ref, mixed_hbm,
    new_ref, stab_new_ref, mixed_ref,
    memv, carr, keys, vt, small_sem, load_sem, store_sem,
):
    small = [
        pltpu.make_async_copy(src, dst, small_sem.at[k])
        for k, (src, dst) in enumerate((
            (carr_hbm, carr), (keys_hbm, keys), (vt_hbm, vt), (stab_hbm, stab_new_ref), (mixed_hbm, mixed_ref),
        ))
    ]
    for copy in small:
        copy.start()

    def part(i):
        return pl.ds(SEQS * i, SEQS)

    def load(i):
        return pltpu.make_async_copy(mem_ref.at[part(i)], memv.at[part(i)], load_sem.at[i])

    def store(i):
        return pltpu.make_async_copy(memv.at[part(i)], new_ref.at[part(i)], store_sem)

    for i in range(3):
        load(i).start()
    for copy in small:
        copy.wait()
    def advance(i, carry):
        load(i).wait()

        @pl.when(i + 3 < ROWS // SEQS)
        def _():
            load(i + 3).start()

        for h in range(4):
            values = vt[h]
            for j in range(SEQS):
                place = pl.ds(SEQS * i + j, 1)
                memv[SEQS * i + j, h] = (
                    carr[h, place, :] * memv[SEQS * i + j, h] + values[:, j:j + 1] * keys[h, place, :]
                )
            vt[h] = pltpu.roll(values, 128 - SEQS, 1)
        store(i).start()
        return carry

    lax.fori_loop(0, ROWS // SEQS, advance, 0)
    drain(memv, store_sem)


def memory_update(carried, keys, values, stab_new, memory, mixed):
    dma = pltpu.SemaphoreType.DMA
    vm = pltpu.VMEM
    return pl.pallas_call(
        memory_kernel,
        out_shape=(
            jax.ShapeDtypeStruct((ROWS, 4, 128, 128), F32),
            jax.ShapeDtypeStruct((4, ROWS), F32),
            jax.ShapeDtypeStruct((ROWS, 1024), BF16),
        ),
        in_specs=[ANY_SPEC] * 6,
        out_specs=(ANY_SPEC, VMEM_SPEC, VMEM_SPEC),
        scratch_shapes=[
            vm((ROWS, 4, 128, 128), F32), vm((4, ROWS, 128), F32), vm((4, ROWS, 128), F32), vm((4, 128, 128), F32),
            dma((5,)), dma((ROWS // SEQS,)), dma,
        ],
        compiler_params=pltpu.CompilerParams(vmem_limit_bytes=VMEM_LIMIT),
        name="memory_update",
    )(carried, keys, values, stab_new, memory, mixed)


def step_kernel(
    tok_hbm, gain1_hbm, wq_ref, wk_ref, wv_ref, wo_ref, wi_ref, wf_ref, mix_ref, dg_ref, du_ref, dd_ref,
    mem_ref, bias_hbm, stab_hbm, hgain_hbm, gain_hbm, route_hbm, weight_hbm, eg_ref, eu_ref, ed_ref, scale_hbm,
    out_ref, carr_ref, keys_ref, vt_ref, stab_new_ref,
    gainv, wiv, wfv, wbuf, gbuf, nbuf, abuf, pbuf, sbuf, tbuf, rbuf,
    memv, rows_ref, gates_ref, bias_ref, stab_ref, hgain_ref, rt, queries, gated_ref,
    tok_ref, gain_ref, route_ref, weight_ref, scale_ref,
    egv, euv, edv, dgv, duv, ddv, mixv, gx, asend, tb, ns, res, n2, sel, comb_hi, comb_lo, obuf, rx,
    xbuf, gacc, uacc, hbuf, yown, ysend, yrecv, yret, rret, da, dout, dr,
    load1_sem, w_send, w_recv, g_send, g_recv, a_send, a_recv, m_send, m_recv, p_send, p_recv, r_send, r_recv,
    dx_send, dx_recv, near_sem, late_sem,
    load_sem, gx_send, gx_recv, tb_send, tb_recv, x_send, x_recv, da_send, da_recv,
    y_send, y_recv, q_send, q_recv, dr_send, dr_recv, xo_send, xo_recv, d_send, d_recv, mem_sem, down_send, down_recv,
):
    chip, core, x, plane = own_place()
    z, y = plane // SIDE, plane % SIDE
    right = plane * SIDE + (x + 1) % SIDE
    left = plane * SIDE + (x + 3) % SIDE
    across = plane * SIDE + (x + 2) % SIDE
    xl, xr = (x + 3) % SIDE, (x + 1) % SIDE

    other, xa = 1 - core, (x + 2) % SIDE
    barrier = pltpu.get_barrier_semaphore()
    along_x, along_y, along_z = axis_peers(plane, x)
    for peer in along_z + along_x + along_y:
        pl.semaphore_signal(barrier, inc=1, device_id=(peer, core), device_id_type=MESH)
    pl.semaphore_signal(barrier, inc=1, device_id=(chip, other), device_id_type=MESH)

    def w_rows(xs):
        return pl.ds(pl.multiple_of(32 * xs, 32), 32)

    def half_rows(xs, half):
        return pl.ds(pl.multiple_of(32 * xs + 16 * half, 16), 16)

    for k, ref in enumerate((wq_ref, wk_ref, wv_ref, wo_ref)):
        load = pltpu.make_async_copy(ref, wbuf.at[w_rows(x), pl.ds(512 * k, 512)], load1_sem.at[0])
        load.start()
    small = [
        pltpu.make_async_copy(src, dst, load1_sem.at[2 + k])
        for k, (src, dst) in enumerate(((tok_hbm, tok_ref), (gain1_hbm, gainv), (wi_ref, wiv), (wf_ref, wfv)))
    ]
    for load in small:
        load.start()
    late = [
        pltpu.make_async_copy(src, dst, late_sem.at[k])
        for k, (src, dst) in enumerate((
            (route_hbm, route_ref), (weight_hbm, weight_ref), (bias_hbm, bias_ref), (stab_hbm, stab_ref),
            (hgain_hbm, hgain_ref), (gain_hbm, gain_ref), (scale_hbm, scale_ref),
        ))
    ]
    for load in small:
        load.wait()

    normed = rms_scale(tok_ref[...].astype(F32), gainv[...])
    nbuf[...] = normed.astype(BF16)
    place = (
        lax.broadcasted_iota(jnp.int32, (32, 128), 1) == lax.broadcasted_iota(jnp.int32, (32, 128), 0) + 32 * x
    ).astype(F32)
    gate_in = jnp.dot(wiv[...].astype(F32), place, preferred_element_type=F32)
    gate_fo = jnp.dot(wfv[...].astype(F32), place, preferred_element_type=F32)
    gbuf[x] = jnp.concatenate([gate_in, gate_fo], axis=0)
    drain(wbuf.at[w_rows(x), :], load1_sem.at[0])
    pl.semaphore_wait(barrier, 9 + 1)
    for peer in along_y:
        pl.semaphore_signal(near_sem, inc=1, device_id=(peer, core), device_id_type=MESH)

    def w_copy(k, kind, xs, part, device):
        rows = w_rows(xs) if part is None else half_rows(xs, part)
        block = wbuf.at[rows, pl.ds(512 * k, 512)]
        return remote(block, block, w_send, w_recv.at[k, kind], (device, core))

    for k in range(4):
        w_copy(k, 0, x, None, right).start()
        w_copy(k, 1, x, None, left).start()
    for peer in (right, left, across):
        remote(gbuf.at[x], gbuf.at[x], g_send, g_recv, (peer, core)).start()

    def token_copy(step):
        peer = plane_shift(plane, step)
        return remote(
            nbuf.at[:, pl.ds(pl.multiple_of(128 * peer, 128), 128)],
            abuf.at[pl.ds(pl.multiple_of(ROWS * plane, ROWS), ROWS), :],
            a_send, a_recv, (peer * SIDE + x, core),
        )

    def plane_peer(axis, step):
        if axis == 0:
            return (z + step) % SIDE, y
        return z, (y + step) % SIDE

    def device_of(zt, yt):
        return ((zt * SIDE + yt) * SIDE + x, core)

    def mix_first(axis, step):
        part = pl.ds(16 * axis, 16)
        return remote(
            mix_ref.at[part], mixv.at[z, y, part], m_send, m_recv.at[axis], device_of(*plane_peer(axis, step))
        )

    def mix_second(axis, step):
        part = pl.ds(16 * (1 - axis), 16)
        block = mixv.at[z, :, part] if axis == 0 else mixv.at[:, y, part]
        return remote(block, block, m_send, m_recv.at[2 + axis], device_of(*plane_peer(axis, step)))

    def start_tokens(step, carry):
        token_copy(step).start()
        return carry

    pl.semaphore_wait(near_sem, 3)
    lax.fori_loop(1, PLANE, start_tokens, 0)
    abuf[pl.ds(pl.multiple_of(ROWS * plane, ROWS), ROWS), :] = nbuf[:, pl.ds(pl.multiple_of(128 * plane, 128), 128)]
    for axis in range(2):
        for d in (2, 1, 3):
            mix_first(axis, d).start()
    mix_own = pltpu.make_async_copy(mix_ref, mixv.at[z, y], load1_sem.at[1])
    mix_own.start()

    dense = ((dg_ref, dgv), (du_ref, duv))

    def dense_copy(k, kind, xs, part, device):
        block = dense[k][1].at[2 * xs + core]
        if part is not None:
            block = block.at[pl.ds(16 * part, 16)]
        source = dense[k][0] if kind in (0, 1) else block
        return remote(source, block, dx_send.at[k], dx_recv.at[kind], device)

    def w_relay(k):
        w_copy(k, 0, x, None, right).wait_recv()
        w_copy(k, 2, xl, 0, right).start()
        w_copy(k, 1, x, None, left).wait_recv()
        w_copy(k, 3, xr, 1, left).start()

    w_relay(0)
    w_relay(1)
    for load in late:
        load.start()
    def mem_load(i):
        part = pl.ds(4 * i, 4)
        return pltpu.make_async_copy(mem_ref.at[part], memv.at[part], mem_sem.at[i])

    for i in range(4):
        mem_load(i).start()
    for k in range(3):
        own_load = pltpu.make_async_copy((dg_ref, du_ref, dd_ref)[k], (dgv, duv, ddv)[k].at[2 * x + core], load_sem.at[3 + k])
        own_load.start()
    late[0].wait()
    late[1].wait()
    spread = (
        lax.broadcasted_iota(jnp.int32, (ROWS, 128), 1) % ROWS == lax.broadcasted_iota(jnp.int32, (ROWS, 128), 0)
    ).astype(F32)
    route = jnp.dot(route_ref[...].astype(F32), spread, preferred_element_type=F32, precision=lax.Precision.HIGHEST)
    weight = jnp.dot(weight_ref[...], spread, preferred_element_type=F32, precision=lax.Precision.HIGHEST)
    expert = lax.broadcasted_iota(jnp.int32, (CHIPS, 128), 0).astype(F32)
    hit = jnp.zeros((CHIPS, 128), F32)
    chosen = jnp.zeros((CHIPS, 128), F32)
    for k in range(4):
        same = (route[k:k + 1, :] == expert).astype(F32)
        hit = hit + same
        chosen = chosen + same * weight[k:k + 1, :]
    col = lax.broadcasted_iota(jnp.int32, (128, 128), 1) % ROWS
    row = lax.broadcasted_iota(jnp.int32, (128, 128), 0)
    before = ((row < ROWS) & (row < col)).astype(F32)
    rank = jnp.dot(hit, before, preferred_element_type=F32)
    first = hit * (rank == 0.0).astype(F32)
    second = hit * (rank == 1.0).astype(F32)
    block_row = lax.broadcasted_iota(jnp.int32, (8, 128), 0)
    block_col = lax.broadcasted_iota(jnp.int32, (8, 128), 1) // ROWS
    diagonal = (block_row == block_col).astype(F32)

    def widened(top, bottom):
        low = top[:, None, :] * diagonal[None, :, :]
        high = bottom[:, None, :] * diagonal[None, :, :]
        return jnp.concatenate([low, high], axis=1).reshape(1024, 128)

    sel[...] = widened(first, second).astype(BF16)
    comb = widened(first * chosen, second * chosen).T
    comb_top = comb.astype(BF16)
    comb_hi[...] = comb_top
    comb_lo[...] = (comb - comb_top.astype(F32)).astype(BF16)
    w_relay(2)
    w_relay(3)
    for k in range(2):
        dense_copy(k, 0, x, None, (right, core)).start()
        dense_copy(k, 1, x, None, (left, core)).start()
    drain(abuf.at[pl.ds(0, 240), :], a_recv)
    drain(gbuf.at[pl.ds(0, 3)], g_recv)
    gate_w = (gbuf[0] + gbuf[1] + gbuf[2] + gbuf[3]).astype(BF16)
    gate_w = jnp.concatenate([gate_w.astype(F32), jnp.zeros((120, 128), F32)], axis=0).astype(BF16)
    def columns(k):
        return pl.ds(512 * k, 640 if k == 3 else 512)

    def first_sum(k, step):
        axis = (k + 1) % 2
        zt, yt = plane_peer(axis, step)
        src = pbuf.at[zt, :, :, columns(k)] if axis == 0 else pbuf.at[:, yt, :, columns(k)]
        own = z if axis == 0 else y
        return remote(src, sbuf.at[own, :, :, columns(k)], p_send, p_recv.at[k], device_of(zt, yt))

    def second_sum(k, step):
        axis = k % 2
        zt, yt = plane_peer(axis, step)
        target, own = (zt, z) if axis == 0 else (yt, y)
        return remote(
            tbuf.at[target, :, columns(k)], rbuf.at[own, :, columns(k)], r_send, r_recv.at[k], device_of(zt, yt)
        )

    for k in range(4):
        w_copy(k, 2, xl, 0, right).wait_recv()
        w_copy(k, 3, xr, 1, left).wait_recv()
        cols = slice(512 * k, 512 * k + 512)
        part = jnp.dot(abuf[...], wbuf[:, cols], preferred_element_type=F32).astype(BF16)
        pbuf[:, :, :, cols] = part.reshape(SIDE, SIDE, ROWS, 512)
        if k == 3:
            gates = lax.dot_general(abuf[...], gate_w, (((1,), (1,)), ((), ())), preferred_element_type=F32)
            high = gates.astype(BF16).astype(F32)
            part = (high + pltpu.roll(gates - high, 8, 1)).astype(BF16)
            pbuf[:, :, :, 2048:2176] = part.reshape(SIDE, SIDE, ROWS, 128)
        for d in (2, 1, 3):
            first_sum(k, d).start()
    loads = []
    for k, (src, dst) in enumerate(((eg_ref, egv), (eu_ref, euv), (ed_ref, edv))):
        loads.append(pltpu.make_async_copy(src.at[0], dst, load_sem.at[k]))
    for load in loads:
        load.start()
    first_lanes = lax.broadcasted_iota(jnp.int32, (ROWS, 128), 1) < 8
    for k in range(4):
        cols = slice(512 * k, 2176 if k == 3 else 512 * k + 512)
        if k % 2 == 0:
            sbuf[y, :, :, cols] = pbuf[:, y, :, cols]
        else:
            sbuf[z, :, :, cols] = pbuf[z, :, :, cols]
        drain(sbuf.at[pl.ds(0, 3), :, :, columns(k)], p_recv.at[k])
        for t in range(SIDE):
            total = sbuf[0, t, :, cols].astype(F32)
            for s in range(1, SIDE):
                total = total + sbuf[s, t, :, cols].astype(F32)
            if k == 3:
                gates = total[:, 512:640]
                gates = jnp.where(first_lanes, gates + pltpu.roll(gates, 120, 1), 0.0)
                high = gates.astype(BF16).astype(F32)
                total = jnp.concatenate([total[:, :512], high + pltpu.roll(gates - high, 8, 1)], axis=1)
            tbuf[t, :, cols] = total.astype(BF16)
        for d in (2, 1, 3):
            second_sum(k, d).start()
        if k % 2 == 0:
            rbuf[z, :, cols] = tbuf[z, :, cols]
        else:
            rbuf[y, :, cols] = tbuf[y, :, cols]

    mix_own.wait()
    for axis in range(2):
        drain(mixv.at[0, pl.ds(0, 3), pl.ds(0, 16)], m_recv.at[1 - axis])
        for d in (2, 1, 3):
            mix_second(axis, d).start()
    def down_copy(kind, xs, part, device):
        block = ddv.at[2 * xs + core]
        if part is not None:
            block = block.at[pl.ds(16 * part, 16)]
        if kind == 4:
            return remote(block, block, d_send.at[2], d_recv.at[2], (chip, other))
        return remote(dd_ref if kind < 2 else block, block, down_send, down_recv.at[kind], (device, core))

    two, twohalf = dgv.at[pl.ds(0, 2)], dgv.at[pl.ds(0, 2), pl.ds(0, 16)]
    drain(two, dx_recv.at[0])
    for k in range(2):
        dense_copy(k, 2, xl, 0, (right, core)).start()
    drain(two, dx_recv.at[1])
    for k in range(2):
        dense_copy(k, 3, xr, 1, (left, core)).start()
    down_copy(0, x, None, right).start()
    down_copy(1, x, None, left).start()
    def row_sum(k):
        cols = slice(512 * k, 512 * k + 512)
        drain(rbuf.at[pl.ds(0, 3), :, columns(k)], r_recv.at[k])
        total = rbuf[0, :, cols].astype(F32)
        for s in range(1, SIDE):
            total = total + rbuf[s, :, cols].astype(F32)
        rows_ref[:, cols] = total.astype(BF16)

    row_sum(0)
    for h in range(4):
        query = upright(rows_ref[:, head_cols(0, h)].astype(F32)).astype(BF16)
        queries[h] = jnp.concatenate([query, query], axis=0)
    lane_index = lax.broadcasted_iota(jnp.int32, (128, 128), 1)

    def read_part(i, carry):
        mem_load(i).wait()
        for h in range(4):
            stored = memv[pl.ds(4 * i, 4), h].reshape(512, 128)
            top = stored.astype(BF16)
            rest = (stored - top.astype(F32)).astype(BF16)
            read = jnp.dot(jnp.concatenate([top, rest], axis=1), queries[h], preferred_element_type=F32)
            reads = rt[h]
            for j in range(4):
                reads = jnp.where(lane_index == 4 * i + j, read[128 * j:128 * j + 128, :], reads)
            rt[h] = reads
        return carry

    rt[...] = jnp.zeros(rt.shape, F32)
    lax.fori_loop(0, 4, read_part, 0)
    for k in range(1, 4):
        row_sum(k)
    total = rbuf[0, :, 2048:2176].astype(F32)
    for s in range(1, SIDE):
        total = total + rbuf[s, :, 2048:2176].astype(F32)
    gates_ref[...] = total + pltpu.roll(total, 120, 1)

    for load in late[2:]:
        load.wait()
    stab_new, carried, written = memory_gates(gates_ref[...], bias_ref[...], stab_ref[...])
    for h in range(4):
        query = rows_ref[:, head_cols(0, h)].astype(F32)
        key = rows_ref[:, head_cols(1, h)].astype(F32) * (128 ** (-0.5))
        value = rows_ref[:, head_cols(2, h)].astype(F32)
        match = jnp.sum(key * query, axis=1, keepdims=True) * written[:, h:h + 1]
        readout = carried[:, h:h + 1] * rt[h].T[0:ROWS, :] + match * value
        gate = jax.nn.sigmoid(rows_ref[:, head_cols(3, h)].astype(F32))
        scaled = rms_scale(readout, hgain_ref[:, head_cols(0, h)])
        gated_ref[:, head_cols(0, h)] = (scaled * gate).astype(BF16)

    gx[pl.ds(pl.multiple_of(ROWS * x, ROWS), ROWS), :] = gated_ref[...]

    def gx_copy(d):
        rows = pl.ds(pl.multiple_of(ROWS * x, ROWS), ROWS)
        peer = plane * SIDE + (x + d) % SIDE
        return remote(gated_ref, gx.at[rows, :], gx_send, gx_recv, (peer, core))

    for d in range(1, SIDE):
        gx_copy(d).start()
    stab_new_ref[...] = turned(stab_new)
    for h in range(4):
        key = rows_ref[:, head_cols(1, h)].astype(F32) * (128 ** (-0.5))
        carr_ref[h] = jnp.broadcast_to(carried[:, h:h + 1], (ROWS, 128))
        keys_ref[h] = key * written[:, h:h + 1]
        vt_ref[h] = upright(rows_ref[:, head_cols(2, h)].astype(F32))
    for axis in range(2):
        drain(mixv.at[pl.ds(0, 3), :, pl.ds(0, 16)], m_recv.at[2 + axis])
    drain(gx.at[pl.ds(0, 48), :], gx_recv)
    asend[...] = lax.dot_general(
        gx[...], mixv[...].reshape(512, 512), (((1,), (1,)), ((), ())), preferred_element_type=F32
    ).astype(BF16)

    def tb_copy(d, side):
        rows = pl.ds(pl.multiple_of(ROWS * ((x + d) % SIDE), ROWS), ROWS)
        peer = plane * SIDE + (x + d) % SIDE
        return remote(
            asend.at[rows, :], tb.at[core, x], tb_send, tb_recv,
            (peer, (core + side) % 2),
        )

    tb_list = [(0, 1)] + [(d, side) for d in (2, 1, 3) for side in (0, 1)]
    for d, side in tb_list:
        tb_copy(d, side).start()
    tb[core, x] = asend[pl.ds(pl.multiple_of(ROWS * x, ROWS), ROWS), :]
    tb_bytes = rx.at[pl.ds(0, 448), :]
    drain(tb_bytes, tb_recv)
    drain(twohalf, dx_recv.at[2])
    drain(twohalf, dx_recv.at[3])
    for k, (own, dst) in enumerate(((dg_ref, dgv), (du_ref, duv), (dd_ref, ddv))):
        for s in range(SIDE if k < 2 else 1):
            slot = dst.at[2 * ((x + s) % SIDE) + core]
            remote(own if s == 0 else slot, slot, d_send.at[k], d_recv.at[k], (chip, other)).start()
    attended = [tb[0, k].astype(F32) + tb[1, k].astype(F32) for k in range(SIDE)]
    lane = lax.broadcasted_iota(jnp.int32, (ROWS, 128), 1) // 32
    tiles = []
    for t in range(PLANE):
        tile = None
        for k in range(SIDE):
            part = attended[k][:, 128 * (t // 4):128 * (t // 4) + 128]
            shift = (32 * k - 32 * (t % 4)) % 128
            if shift:
                part = pltpu.roll(part, shift, 1)
            tile = part if tile is None else jnp.where(lane == k, part, tile)
        tiles.append(tile)
    residual = (tok_ref[...].astype(F32) + jnp.concatenate(tiles, axis=1)).astype(BF16)
    res[...] = residual
    normed = rms_scale(residual.astype(F32), gain_ref[...]).astype(BF16)
    ns[...] = normed
    def tile_rows(index):
        return pl.ds(pl.multiple_of(ROWS * index, ROWS), ROWS)

    parity = plane % 2
    half = plane // 2

    own_row = y // 2
    low, high = pl.ds(0, 1024), pl.ds(1024, 1024)

    def acts_first(axis, d):
        peer = (along_z, along_y)[axis][d]
        cols = (low, high)[axis]
        return remote(
            ns.at[:, cols], da.at[z, own_row, :, cols], da_send.at[0], da_recv.at[axis], (peer, parity)
        )

    def acts_second(axis, d):
        peer = (along_z, along_y)[axis][d]
        block = da.at[z, :, :, high] if axis == 0 else da.at[:, own_row, :, low]
        return remote(block, block, da_send.at[1 + axis], da_recv.at[2 + axis], (peer, core))

    for axis in range(2):
        @pl.when(core == axis)
        def _():
            for d in (1, 0, 2):
                acts_first(axis, d).start()

    @pl.when(parity == core)
    def _():
        da[z, own_row] = ns[...]

    for b in range(8):
        cols = pl.ds(pl.multiple_of(1024 * core + 128 * b, 128), 128)
        n2[16 * b:16 * b + 16, :] = ns[:, cols]
    for k in range(4):
        obuf[256 * k:256 * k + 256, :] = jnp.dot(
            sel[256 * k:256 * k + 256, :], n2[...], preferred_element_type=F32
        ).astype(BF16)

    def x_copy(peer):
        return remote(
            obuf.at[tile_rows(peer), :], rx.at[tile_rows(chip), :], x_send, x_recv, (peer, core)
        )

    each_chip(plane, x, lambda peer: x_copy(peer).start())
    rx[tile_rows(chip), :] = obuf[tile_rows(chip), :]

    down_copy(0, x, None, right).wait_recv()
    down_copy(2, xl, 0, right).start()
    down_copy(1, x, None, left).wait_recv()
    down_copy(3, xr, 1, left).start()
    down_copy(4, xl, None, chip).start()
    down_copy(4, xr, None, chip).start()
    row_of = da.at[0, 0, :, low]

    @pl.when(parity == core)
    def _():
        drain(row_of, da_recv.at[1])
        drain(da.at[pl.ds(0, 3), 0, :, low], da_recv.at[0])
        for d in (1, 0, 2):
            acts_second(1, d).start()

    @pl.when(parity != core)
    def _():
        drain(da.at[pl.ds(0, 2), 0, :, low], da_recv.at[1])

    for d in (1, 0, 2):
        acts_second(0, d).start()

    drain(rx.at[pl.ds(0, 1008), :], x_recv)
    row = lax.broadcasted_iota(jnp.int32, (256, 256), 0)
    col = lax.broadcasted_iota(jnp.int32, (256, 256), 1)
    gather = (col == ((row % 32) // 2) * 16 + (row % 2) * 8 + row // 32).astype(F32).astype(BF16)
    scatter = (row == ((col % 32) // 2) * 16 + (col % 2) * 8 + col // 32).astype(F32).astype(BF16)
    for g in range(4):
        mixed_up = jnp.dot(gather, rx[256 * g:256 * g + 256, :], preferred_element_type=F32).astype(BF16)
        for b in range(8):
            xbuf[core, 32 * g:32 * g + 32, 128 * b:128 * b + 128] = mixed_up[32 * b:32 * b + 32, :]
    swap = remote(xbuf.at[core], xbuf.at[core], xo_send, xo_recv, (chip, other))
    swap.start()
    loads[0].wait()
    loads[1].wait()

    def expert_up_near(t, carry):
        cols = pl.ds(pl.multiple_of(256 * t, 256), 256)
        depth = pl.ds(pl.multiple_of(1024 * core, 1024), 1024)
        gacc[:, cols] = jnp.dot(xbuf[core], egv[depth, cols], preferred_element_type=F32)
        uacc[:, cols] = jnp.dot(xbuf[core], euv[depth, cols], preferred_element_type=F32)
        return carry

    def expert_up_far(t, carry):
        cols = pl.ds(pl.multiple_of(256 * t, 256), 256)
        depth = pl.ds(pl.multiple_of(1024 * other, 1024), 1024)
        gate_pre = gacc[:, cols] + jnp.dot(xbuf[other], egv[depth, cols], preferred_element_type=F32)
        up_pre = uacc[:, cols] + jnp.dot(xbuf[other], euv[depth, cols], preferred_element_type=F32)
        gate_clamped = jnp.minimum(gate_pre, clamp_limit)
        up_clamped = jnp.clip(up_pre, -clamp_limit, clamp_limit)
        hbuf[:, cols] = (
            (up_clamped + 1.0) * gate_clamped * jax.nn.sigmoid(sigmoid_slope * gate_clamped)
        ).astype(BF16)
        return carry

    lax.fori_loop(0, 4, expert_up_near, 0)
    for k, dst in enumerate((dgv, duv)):
        drain(dst.at[0], load_sem.at[3 + k])
        drain(dst.at[pl.ds(0, 4)], d_recv.at[k])

    @pl.when(parity == core)
    def _():
        drain(da.at[:, 0, :, low], da_recv.at[3])

    @pl.when(parity != core)
    def _():
        drain(da.at[:, :, :, low], da_recv.at[3])

    drain(da.at[pl.ds(0, 3), :, :, low], da_recv.at[2])

    down_copy(2, xa, 0, right).wait_recv()
    down_copy(3, xa, 1, left).wait_recv()
    down_copy(4, xa, None, chip).start()
    dense_rows = da[...].reshape(128, 2048)
    over_last = (((1,), (1,)), ((), ()))
    gate_rows = lax.dot_general(dense_rows, dgv[...].reshape(256, 2048), over_last, preferred_element_type=F32)
    lift_rows = lax.dot_general(dense_rows, duv[...].reshape(256, 2048), over_last, preferred_element_type=F32)
    activity = (gate_rows / (1.0 + jnp.exp(-gate_rows)) * lift_rows).astype(BF16)
    drain(ddv.at[0], load_sem.at[5])
    drain(ddv.at[pl.ds(0, 4)], d_recv.at[2])
    down = ddv[...].reshape(256, 2048)
    for h in range(2):
        for t in range(2):
            lower = 1024 * h + 512 * t
            part = jnp.dot(activity, down[:, lower:lower + 512], preferred_element_type=F32).astype(BF16)
            dout[h, :, 512 * t:512 * t + 512] = part

    def dr_copy(index, h):
        target = 2 * index + core
        return remote(
            dout.at[h, tile_rows(index), :], dr.at[plane], dr_send, dr_recv,
            (target * SIDE + x, h),
        )

    def start_dr(index, carry):
        for h in range(2):
            @pl.when((2 * index + core != plane) | (core != h))
            def _():
                dr_copy(index, h).start()
        return carry

    lax.fori_loop(0, 8, start_dr, 0)

    @pl.when(parity == core)
    def _():
        dr[plane] = dout[core, tile_rows(half), :]

    swap.wait_recv()
    lax.fori_loop(0, 4, expert_up_far, 0)
    loads[2].wait()

    def y_copy(t):
        return remote(ysend.at[t], yrecv.at[t], y_send, y_recv, (chip, other))

    def expert_down_far(t, carry):
        cols = pl.ds(pl.multiple_of(1024 * other + 256 * t, 256), 256)
        ysend[t] = jnp.dot(hbuf[...], edv[:, cols], preferred_element_type=F32).astype(BF16)
        y_copy(t).start()
        return carry

    def expert_down_near(t, carry):
        cols = pl.ds(pl.multiple_of(1024 * core + 256 * t, 256), 256)
        yown[t] = jnp.dot(hbuf[...], edv[:, cols], preferred_element_type=F32).astype(BF16)
        return carry

    lax.fori_loop(0, 4, expert_down_far, 0)
    lax.fori_loop(0, 4, expert_down_near, 0)

    drain(yrecv, y_recv)
    for g in range(4):
        rows = slice(32 * g, 32 * g + 32)
        stacked = []
        for t in range(4):
            both = (yown[t, rows, :].astype(F32) + yrecv[t, rows, :].astype(F32)).astype(BF16)
            stacked += [both[:, :128], both[:, 128:]]
        yret[256 * g:256 * g + 256, :] = jnp.dot(
            scatter, jnp.concatenate(stacked, axis=0), preferred_element_type=F32
        ).astype(BF16)

    def q_copy(peer):
        return remote(
            yret.at[tile_rows(peer), :], rret.at[tile_rows(chip), :], q_send, q_recv, (peer, core)
        )

    each_chip(plane, x, lambda peer: q_copy(peer).start())
    rret[tile_rows(chip), :] = yret[tile_rows(chip), :]

    @pl.when(parity == core)
    def _():
        drain(dr.at[pl.ds(0, 15)], dr_recv)

    @pl.when(parity != core)
    def _():
        drain(dr, dr_recv)

    branch = dr[0].astype(F32)
    for s in range(1, PLANE):
        branch = branch + dr[s].astype(F32)

    drain(rret.at[pl.ds(0, 1008), :], q_recv)
    returned = rret[...]
    routed = jnp.dot(comb_hi[...], returned, preferred_element_type=F32) + jnp.dot(
        comb_lo[...], returned, preferred_element_type=F32
    )
    routed = jnp.concatenate([routed[16 * b:16 * b + 16, :] for b in range(8)], axis=1)
    own_cols = pl.ds(pl.multiple_of(1024 * core, 1024), 1024)
    out_ref[...] = (res[:, own_cols].astype(F32) + routed + branch * scale_ref[:, own_cols]).astype(BF16)

    drain(gx.at[pl.ds(0, 48), :], gx_send)
    drain(tb_bytes, tb_send)
    drain(rx.at[pl.ds(0, 1008), :], x_send)
    drain(rret.at[pl.ds(0, 1008), :], q_send)
    drain(yrecv, y_send)
    drain(xbuf.at[0], xo_send)
    for k, dst in enumerate((dgv, duv, ddv)):
        drain(dst.at[pl.ds(0, 4)], d_send.at[k])
    drain(ddv.at[pl.ds(0, 3)], down_send)

    drain(da.at[pl.ds(0, 3), 0, :, low], da_send.at[0])
    drain(da.at[pl.ds(0, 3), :, :, low], da_send.at[1])

    @pl.when(parity == core)
    def _():
        drain(da.at[pl.ds(0, 3)], da_send.at[2])

    @pl.when(parity == core)
    def _():
        drain(dr.at[pl.ds(0, 15)], dr_send)

    @pl.when(parity != core)
    def _():
        drain(dr, dr_send)
    drain(wbuf.at[pl.ds(0, 96), :], w_send)
    drain(gbuf.at[pl.ds(0, 3)], g_send)
    drain(abuf.at[pl.ds(0, 240), :], a_send)
    drain(mixv.at[pl.ds(0, 3), :, :], m_send)
    drain(mixv.at[0, pl.ds(0, 3)], m_send)
    drain(sbuf.at[pl.ds(0, 3)], p_send)
    drain(rbuf.at[pl.ds(0, 3)], r_send)
    for k in range(2):
        drain(dense[k][1].at[pl.ds(0, 3)], dx_send.at[k])


def decode_step(*operands):
    dma = pltpu.SemaphoreType.DMA
    vm = pltpu.VMEM
    return pl.pallas_call(
        step_kernel,
        out_shape=(
            jax.ShapeDtypeStruct((ROWS, 1024), BF16),
            jax.ShapeDtypeStruct((4, ROWS, 128), F32),
            jax.ShapeDtypeStruct((4, ROWS, 128), F32),
            jax.ShapeDtypeStruct((4, 128, 128), F32),
            jax.ShapeDtypeStruct((4, ROWS), F32),
        ),
        in_specs=[ANY_SPEC] * 23,
        out_specs=(VMEM_SPEC,) * 5,
        scratch_shapes=[
            vm((1, 2048), F32), vm((4, 32), BF16), vm((4, 32), BF16), vm((128, 2048), BF16), vm((4, 8, 128), F32),
            vm((ROWS, 2048), BF16), vm((256, 128), BF16),
            vm((SIDE, SIDE, ROWS, 2176), BF16), vm((SIDE, SIDE, ROWS, 2176), BF16),
            vm((SIDE, ROWS, 2176), BF16), vm((SIDE, ROWS, 2176), BF16),
            vm((ROWS, 4, 128, 128), F32), vm((ROWS, 2048), BF16), vm((ROWS, 128), F32), vm((1, 4), F32),
            vm((4, ROWS), F32), vm((1, 512), F32), vm((4, 128, 128), F32), vm((4, 256, 128), BF16),
            vm((ROWS, 512), BF16), vm((ROWS, 2048), BF16), vm((1, 2048), F32),
            vm((4, ROWS), jnp.int32), vm((4, ROWS), F32), vm((1, 2048), F32),
            vm((2048, 1024), BF16), vm((2048, 1024), BF16), vm((1024, 2048), BF16),
            vm((8, 32, 2048), BF16), vm((8, 32, 2048), BF16), vm((8, 32, 2048), BF16),
            vm((SIDE, SIDE, 32, 512), BF16),
            vm((64, 512), BF16), vm((64, 512), BF16), vm((2, 4, ROWS, 512), BF16),
            vm((ROWS, 2048), BF16), vm((ROWS, 2048), BF16), vm((128, 128), BF16),
            vm((1024, 128), BF16), vm((128, 1024), BF16), vm((128, 1024), BF16),
            vm((1024, 128), BF16), vm((1024, 128), BF16), vm((2, 128, 1024), BF16),
            vm((128, 1024), F32), vm((128, 1024), F32), vm((128, 1024), BF16),
            vm((4, 128, 256), BF16), vm((4, 128, 256), BF16), vm((4, 128, 256), BF16),
            vm((1024, 128), BF16), vm((1024, 128), BF16),
            vm((SIDE, 2, ROWS, 2048), BF16), vm((2, 128, 1024), BF16), vm((PLANE, ROWS, 1024), BF16),
            dma((6,)),
            dma, dma((4, 4)),
            dma, dma,
            dma, dma,
            dma, dma((4,)),
            dma, dma((4,)),
            dma, dma((4,)),
            dma((2,)), dma((4,)),
            pltpu.SemaphoreType.REGULAR, dma((7,)),
            dma((6,)),
            dma, dma,
            dma, dma,
            dma, dma,
            dma((3,)), dma((4,)),
            dma, dma,
            dma, dma,
            dma, dma,
            dma, dma,
            dma((3,)), dma((3,)),
            dma((4,)),
            dma, dma((4,)),
        ],
        compiler_params=pltpu.CompilerParams(
            collective_id=0, has_side_effects=True, vmem_limit_bytes=VMEM_LIMIT
        ),
        name="decode_step",
    )(*operands)


def body(
    tokens, norm_gain, query_weight, key_weight, value_weight, outgate_weight, input_weight, forget_weight,
    forget_bias, memory, stabilizer, head_gain, mix_weight, second_gain, route_experts, route_weight,
    expert_gate, expert_up, expert_down, dense_gate, dense_up, dense_down, branch_scale,
):
    mixed, carried, keys, values, stab_new = decode_step(
        tokens, norm_gain.reshape(1, -1), query_weight, key_weight, value_weight, outgate_weight,
        input_weight.T, forget_weight.T, mix_weight.T, dense_gate, dense_up, dense_down,
        memory, forget_bias.reshape(1, -1), stabilizer.T, head_gain.reshape(1, -1), second_gain.reshape(1, -1),
        route_experts.T, route_weight.T, expert_gate, expert_up, expert_down, branch_scale.reshape(1, -1),
    )
    memory_new, stab_new, mixed = memory_update(carried, keys, values, stab_new, memory, mixed)
    return mixed, memory_new, stab_new.T


def solution(mesh):
    in_specs = (
        P("ep", None), P(),
        P("ep", "tp"), P("ep", "tp"), P("ep", "tp"), P("ep", "tp"), P("ep", "tp"), P("ep", "tp"),
        P("tp"), P("ep", "tp", None, None), P("ep", "tp"), P("tp"), P("tp", "ep"), P(),
        P("ep", None), P("ep", None),
        P("ep", None, "tp"), P("ep", None, "tp"), P("ep", "tp", None),
        P(("ep", "tp"), None), P(("ep", "tp"), None), P(("ep", "tp"), None), P(),
    )
    out_specs = (P("ep", "tp"), P("ep", "tp", None, None), P("ep", "tp"))
    return jax.shard_map(body, mesh=mesh, in_specs=in_specs, out_specs=out_specs, check_vma=False)
```

```python
import jax
import jax.numpy as jnp
from jax import lax
from jax.experimental import pallas as pl
from jax.experimental.pallas import tpu as pltpu
from jax.sharding import PartitionSpec as P

norm_eps = 1e-05
clamp_limit = 7.0
sigmoid_slope = 1.702
F32 = jnp.float32
BF16 = jnp.bfloat16
MESH = pl.DeviceIdType.MESH
VMEM_SPEC = pl.BlockSpec(memory_space=pltpu.VMEM)
ANY_SPEC = pl.BlockSpec(memory_space=pl.ANY)
VMEM_LIMIT = 60 * 1024 * 1024

SIDE = 4
PLANE = 16
CHIPS = 64
ROWS = 16
SEQS = 2


def rms_scale(values, gain):
    mean_square = jnp.mean(values * values, axis=-1, keepdims=True)
    return values * lax.rsqrt(mean_square + norm_eps) * gain


def own_place():
    chip = lax.axis_index("ep")
    core = lax.axis_index("tp")
    return chip, core, chip % SIDE, chip // SIDE


def plane_shift(plane, step):
    z = (plane // SIDE + step // SIDE) % SIDE
    y = (plane % SIDE + step % SIDE) % SIDE
    return z * SIDE + y


def axis_peers(plane, x):
    z, y = plane // SIDE, plane % SIDE
    along_y = [((z * SIDE + (y + d) % SIDE) * SIDE + x) for d in range(1, SIDE)]
    along_z = [((((z + d) % SIDE) * SIDE + y) * SIDE + x) for d in range(1, SIDE)]
    along_x = [(plane * SIDE + (x + d) % SIDE) for d in range(1, SIDE)]
    return along_x, along_y, along_z


def each_chip(plane, x, act):
    xs = [(x + d) % SIDE for d in range(SIDE)]

    def on_plane(step, carry):
        base = plane_shift(plane, step) * SIDE
        for d in range(SIDE):
            act(base + xs[d])
        return carry

    lax.fori_loop(1, PLANE, on_plane, 0)
    for d in range(1, SIDE):
        act(plane * SIDE + xs[d])


def remote(src, dst, send, recv, device):
    return pltpu.make_async_remote_copy(
        src_ref=src, dst_ref=dst, send_sem=send, recv_sem=recv,
        device_id=device, device_id_type=MESH,
    )


def drain(ref, sem):
    pltpu.make_async_copy(ref, ref, sem).wait()


def identity(n):
    row = lax.broadcasted_iota(jnp.int32, (n, n), 0)
    return (row == lax.broadcasted_iota(jnp.int32, (n, n), 1)).astype(F32)


def turned(values):
    rows = values.shape[0]
    return lax.dot_general(
        identity(values.shape[1]), values, (((1,), (1,)), ((), ())),
        preferred_element_type=F32, precision=lax.Precision.HIGHEST,
    ).reshape(values.shape[1], rows)


def memory_gates(gates, bias, stab_t):
    stab = turned(stab_t)
    input_pre = gates[:, 0:4]
    forget = pltpu.roll(gates, 124, 1)[:, 0:4] + bias
    log_forget = jnp.minimum(forget, 0.0) - jnp.log1p(jnp.exp(-jnp.abs(forget)))
    stab_new = jnp.maximum(log_forget + stab, input_pre)
    return stab_new, jnp.exp(log_forget + stab - stab_new), jnp.exp(input_pre - stab_new)


def head_cols(part, h):
    return slice(512 * part + 128 * h, 512 * part + 128 * h + 128)


def upright(rows):
    return jnp.concatenate([rows, jnp.zeros((112, 128), F32)], axis=0).T


def memory_kernel(
    carr_hbm, keys_hbm, vt_hbm, stab_hbm, mem_ref, mixed_hbm,
    new_ref, stab_new_ref, mixed_ref,
    memv, carr, keys, vt, small_sem, load_sem, store_sem,
):
    small = [
        pltpu.make_async_copy(src, dst, small_sem.at[k])
        for k, (src, dst) in enumerate((
            (carr_hbm, carr), (keys_hbm, keys), (vt_hbm, vt), (stab_hbm, stab_new_ref), (mixed_hbm, mixed_ref),
        ))
    ]
    for copy in small:
        copy.start()

    def part(i):
        return pl.ds(SEQS * i, SEQS)

    def load(i):
        return pltpu.make_async_copy(mem_ref.at[part(i)], memv.at[part(i)], load_sem.at[i])

    def store(i):
        return pltpu.make_async_copy(memv.at[part(i)], new_ref.at[part(i)], store_sem)

    for i in range(3):
        load(i).start()
    for copy in small:
        copy.wait()
    row = lax.broadcasted_iota(jnp.int32, (32, 128), 0) % ROWS

    def advance(i, carry):
        load(i).wait()

        @pl.when(i + 3 < ROWS // SEQS)
        def _():
            load(i + 3).start()

        for h in range(4):
            chosen = [jnp.where(row == SEQS * i + j, keys[h], 0.0) for j in range(SEQS)]
            outer = jnp.dot(
                vt[h, :, 0:32], jnp.concatenate(chosen, axis=1).astype(BF16), preferred_element_type=F32
            )
            for j in range(SEQS):
                place = SEQS * i + j
                memv[place, h] = carr[h, pl.ds(place, 1), :] * memv[place, h] + outer[:, 128 * j:128 * j + 128]
        store(i).start()
        return carry

    lax.fori_loop(0, ROWS // SEQS, advance, 0)
    drain(memv, store_sem)


def memory_update(carried, keys, values, stab_new, memory, mixed):
    dma = pltpu.SemaphoreType.DMA
    vm = pltpu.VMEM
    return pl.pallas_call(
        memory_kernel,
        out_shape=(
            jax.ShapeDtypeStruct((ROWS, 4, 128, 128), F32),
            jax.ShapeDtypeStruct((4, ROWS), F32),
            jax.ShapeDtypeStruct((ROWS, 1024), BF16),
        ),
        in_specs=[ANY_SPEC] * 6,
        out_specs=(ANY_SPEC, VMEM_SPEC, VMEM_SPEC),
        scratch_shapes=[
            vm((ROWS, 4, 128, 128), F32), vm((4, ROWS, 128), F32), vm((4, 32, 128), F32), vm((4, 128, 128), BF16),
            dma((5,)), dma((ROWS // SEQS,)), dma,
        ],
        compiler_params=pltpu.CompilerParams(vmem_limit_bytes=VMEM_LIMIT),
        name="memory_update",
    )(carried, keys, values, stab_new, memory, mixed)


def step_kernel(
    tok_hbm, gain1_hbm, wq_ref, wk_ref, wv_ref, wo_ref, wi_ref, wf_ref, mix_ref, dg_ref, du_ref, dd_ref,
    mem_ref, bias_hbm, stab_hbm, hgain_hbm, gain_hbm, route_hbm, weight_hbm, eg_ref, eu_ref, ed_ref, scale_hbm,
    out_ref, carr_ref, keys_ref, vt_ref, stab_new_ref,
    gainv, wiv, wfv, wbuf, gbuf, nbuf, abuf, pbuf, sbuf, tbuf, rbuf,
    memv, rows_ref, gates_ref, bias_ref, stab_ref, hgain_ref, rt, queries, gated_ref,
    tok_ref, gain_ref, route_ref, weight_ref, scale_ref,
    egv, euv, edv, dgv, duv, ddv, mixv, gx, asend, tb, ns, res, n2, sel, comb_hi, comb_lo, obuf, rx,
    xbuf, gacc, uacc, hbuf, yown, ysend, yrecv, yret, rret, da, dout, dr, zsum, ysum, zout, yout,
    load1_sem, w_send, w_recv, g_send, g_recv, a_send, a_recv, m_send, m_recv, p_send, p_recv, r_send, r_recv,
    dx_send, dx_recv, near_sem, late_sem,
    load_sem, gx_send, gx_recv, tb_send, tb_recv, x_send, x_recv, da_send, da_recv,
    y_send, y_recv, q_send, q_recv, dr_send, dr_recv, xo_send, xo_recv, d_send, d_recv, mem_sem, down_send, down_recv,
    rp_send, rp_recv,
):
    chip, core, x, plane = own_place()
    z, y = plane // SIDE, plane % SIDE
    right = plane * SIDE + (x + 1) % SIDE
    left = plane * SIDE + (x + 3) % SIDE
    across = plane * SIDE + (x + 2) % SIDE
    xl, xr = (x + 3) % SIDE, (x + 1) % SIDE

    other, xa = 1 - core, (x + 2) % SIDE
    barrier = pltpu.get_barrier_semaphore()
    along_x, along_y, along_z = axis_peers(plane, x)
    for peer in along_z + along_x + along_y:
        pl.semaphore_signal(barrier, inc=1, device_id=(peer, core), device_id_type=MESH)
    pl.semaphore_signal(barrier, inc=1, device_id=(chip, other), device_id_type=MESH)

    def w_rows(xs):
        return pl.ds(pl.multiple_of(32 * xs, 32), 32)

    def half_rows(xs, half):
        return pl.ds(pl.multiple_of(32 * xs + 16 * half, 16), 16)

    for k, ref in enumerate((wq_ref, wk_ref, wv_ref, wo_ref)):
        load = pltpu.make_async_copy(ref, wbuf.at[w_rows(x), pl.ds(512 * k, 512)], load1_sem.at[0])
        load.start()
    small = [
        pltpu.make_async_copy(src, dst, load1_sem.at[2 + k])
        for k, (src, dst) in enumerate(((tok_hbm, tok_ref), (gain1_hbm, gainv), (wi_ref, wiv), (wf_ref, wfv)))
    ]
    for load in small:
        load.start()
    late = [
        pltpu.make_async_copy(src, dst, late_sem.at[k])
        for k, (src, dst) in enumerate((
            (route_hbm, route_ref), (weight_hbm, weight_ref), (bias_hbm, bias_ref), (stab_hbm, stab_ref),
            (hgain_hbm, hgain_ref), (gain_hbm, gain_ref), (scale_hbm, scale_ref),
        ))
    ]
    for load in small:
        load.wait()

    normed = rms_scale(tok_ref[...].astype(F32), gainv[...])
    nbuf[...] = normed.astype(BF16)
    place = (
        lax.broadcasted_iota(jnp.int32, (32, 128), 1) == lax.broadcasted_iota(jnp.int32, (32, 128), 0) + 32 * x
    ).astype(F32)
    gate_in = jnp.dot(wiv[...].astype(F32), place, preferred_element_type=F32)
    gate_fo = jnp.dot(wfv[...].astype(F32), place, preferred_element_type=F32)
    gbuf[x] = jnp.concatenate([gate_in, gate_fo], axis=0)
    drain(wbuf.at[w_rows(x), :], load1_sem.at[0])
    pl.semaphore_wait(barrier, 9 + 1)
    for peer in along_y:
        pl.semaphore_signal(near_sem, inc=1, device_id=(peer, core), device_id_type=MESH)

    def w_copy(k, kind, xs, part, device):
        rows = w_rows(xs) if part is None else half_rows(xs, part)
        block = wbuf.at[rows, pl.ds(512 * k, 512)]
        return remote(block, block, w_send, w_recv.at[k, kind], (device, core))

    for k in range(4):
        w_copy(k, 0, x, None, right).start()
        w_copy(k, 1, x, None, left).start()
    for peer in (right, left, across):
        remote(gbuf.at[x], gbuf.at[x], g_send, g_recv, (peer, core)).start()

    def token_copy(step):
        peer = plane_shift(plane, step)
        return remote(
            nbuf.at[:, pl.ds(pl.multiple_of(128 * peer, 128), 128)],
            abuf.at[pl.ds(pl.multiple_of(ROWS * plane, ROWS), ROWS), :],
            a_send, a_recv, (peer * SIDE + x, core),
        )

    def plane_peer(axis, step):
        if axis == 0:
            return (z + step) % SIDE, y
        return z, (y + step) % SIDE

    def device_of(zt, yt):
        return ((zt * SIDE + yt) * SIDE + x, core)

    def mix_first(axis, step):
        part = pl.ds(16 * axis, 16)
        return remote(
            mix_ref.at[part], mixv.at[z, y, part], m_send, m_recv.at[axis], device_of(*plane_peer(axis, step))
        )

    def mix_second(axis, step):
        part = pl.ds(16 * (1 - axis), 16)
        block = mixv.at[z, :, part] if axis == 0 else mixv.at[:, y, part]
        return remote(block, block, m_send, m_recv.at[2 + axis], device_of(*plane_peer(axis, step)))

    def start_tokens(step, carry):
        token_copy(step).start()
        return carry

    pl.semaphore_wait(near_sem, 3)
    lax.fori_loop(1, PLANE, start_tokens, 0)
    abuf[pl.ds(pl.multiple_of(ROWS * plane, ROWS), ROWS), :] = nbuf[:, pl.ds(pl.multiple_of(128 * plane, 128), 128)]
    for axis in range(2):
        for d in (2, 1, 3):
            mix_first(axis, d).start()
    mix_own = pltpu.make_async_copy(mix_ref, mixv.at[z, y], load1_sem.at[1])
    mix_own.start()

    dense = ((dg_ref, dgv), (du_ref, duv))

    def dense_copy(k, kind, xs, part, device):
        block = dense[k][1].at[2 * xs + core]
        if part is not None:
            block = block.at[pl.ds(16 * part, 16)]
        source = dense[k][0] if kind in (0, 1) else block
        return remote(source, block, dx_send.at[k], dx_recv.at[kind], device)

    def w_relay(k):
        w_copy(k, 0, x, None, right).wait_recv()
        w_copy(k, 2, xl, 0, right).start()
        w_copy(k, 1, x, None, left).wait_recv()
        w_copy(k, 3, xr, 1, left).start()

    w_relay(0)
    w_relay(1)
    for load in late:
        load.start()
    def mem_load(i):
        part = pl.ds(4 * i, 4)
        return pltpu.make_async_copy(mem_ref.at[part], memv.at[part], mem_sem.at[i])

    for i in range(4):
        mem_load(i).start()
    for k in range(3):
        own_load = pltpu.make_async_copy((dg_ref, du_ref, dd_ref)[k], (dgv, duv, ddv)[k].at[2 * x + core], load_sem.at[3 + k])
        own_load.start()
    late[0].wait()
    late[1].wait()
    spread = (
        lax.broadcasted_iota(jnp.int32, (ROWS, 128), 1) % ROWS == lax.broadcasted_iota(jnp.int32, (ROWS, 128), 0)
    ).astype(F32)
    route = jnp.dot(route_ref[...].astype(F32), spread, preferred_element_type=F32, precision=lax.Precision.HIGHEST)
    weight = jnp.dot(weight_ref[...], spread, preferred_element_type=F32, precision=lax.Precision.HIGHEST)
    expert = lax.broadcasted_iota(jnp.int32, (CHIPS, 128), 0).astype(F32)
    hit = jnp.zeros((CHIPS, 128), F32)
    chosen = jnp.zeros((CHIPS, 128), F32)
    for k in range(4):
        same = (route[k:k + 1, :] == expert).astype(F32)
        hit = hit + same
        chosen = chosen + same * weight[k:k + 1, :]
    col = lax.broadcasted_iota(jnp.int32, (128, 128), 1) % ROWS
    row = lax.broadcasted_iota(jnp.int32, (128, 128), 0)
    before = ((row < ROWS) & (row < col)).astype(F32)
    rank = jnp.dot(hit, before, preferred_element_type=F32)
    first = hit * (rank == 0.0).astype(F32)
    second = hit * (rank == 1.0).astype(F32)
    block_row = lax.broadcasted_iota(jnp.int32, (8, 128), 0)
    block_col = lax.broadcasted_iota(jnp.int32, (8, 128), 1) // ROWS
    diagonal = (block_row == block_col).astype(F32)

    def widened(top, bottom):
        low = top[:, None, :] * diagonal[None, :, :]
        high = bottom[:, None, :] * diagonal[None, :, :]
        return jnp.concatenate([low, high], axis=1).reshape(1024, 128)

    sel[...] = widened(first, second).astype(BF16)
    comb = widened(first * chosen, second * chosen).T
    comb_top = comb.astype(BF16)
    comb_hi[...] = comb_top
    comb_lo[...] = (comb - comb_top.astype(F32)).astype(BF16)
    w_relay(2)
    w_relay(3)
    for k in range(2):
        dense_copy(k, 0, x, None, (right, core)).start()
        dense_copy(k, 1, x, None, (left, core)).start()
    drain(abuf.at[pl.ds(0, 240), :], a_recv)
    drain(gbuf.at[pl.ds(0, 3)], g_recv)
    gate_w = (gbuf[0] + gbuf[1] + gbuf[2] + gbuf[3]).astype(BF16)
    gate_w = jnp.concatenate([gate_w.astype(F32), jnp.zeros((120, 128), F32)], axis=0).astype(BF16)
    def columns(k):
        return pl.ds(512 * k, 640 if k == 3 else 512)

    def first_sum(k, step):
        axis = (k + 1) % 2
        zt, yt = plane_peer(axis, step)
        src = pbuf.at[zt, :, :, columns(k)] if axis == 0 else pbuf.at[:, yt, :, columns(k)]
        own = z if axis == 0 else y
        return remote(src, sbuf.at[own, :, :, columns(k)], p_send, p_recv.at[k], device_of(zt, yt))

    def second_sum(k, step):
        axis = k % 2
        zt, yt = plane_peer(axis, step)
        target, own = (zt, z) if axis == 0 else (yt, y)
        return remote(
            tbuf.at[target, :, columns(k)], rbuf.at[own, :, columns(k)], r_send, r_recv.at[k], device_of(zt, yt)
        )

    for k in range(4):
        w_copy(k, 2, xl, 0, right).wait_recv()
        w_copy(k, 3, xr, 1, left).wait_recv()
        cols = slice(512 * k, 512 * k + 512)
        part = jnp.dot(abuf[...], wbuf[:, cols], preferred_element_type=F32).astype(BF16)
        pbuf[:, :, :, cols] = part.reshape(SIDE, SIDE, ROWS, 512)
        if k == 3:
            gates = lax.dot_general(abuf[...], gate_w, (((1,), (1,)), ((), ())), preferred_element_type=F32)
            high = gates.astype(BF16).astype(F32)
            part = (high + pltpu.roll(gates - high, 8, 1)).astype(BF16)
            pbuf[:, :, :, 2048:2176] = part.reshape(SIDE, SIDE, ROWS, 128)
        for d in (2, 1, 3):
            first_sum(k, d).start()
    loads = []
    for k, (src, dst) in enumerate(((eg_ref, egv), (eu_ref, euv), (ed_ref, edv))):
        loads.append(pltpu.make_async_copy(src.at[0], dst, load_sem.at[k]))
    for load in loads:
        load.start()
    first_lanes = lax.broadcasted_iota(jnp.int32, (ROWS, 128), 1) < 8
    for k in range(4):
        cols = slice(512 * k, 2176 if k == 3 else 512 * k + 512)
        if k % 2 == 0:
            sbuf[y, :, :, cols] = pbuf[:, y, :, cols]
        else:
            sbuf[z, :, :, cols] = pbuf[z, :, :, cols]
        drain(sbuf.at[pl.ds(0, 3), :, :, columns(k)], p_recv.at[k])
        for t in range(SIDE):
            total = sbuf[0, t, :, cols].astype(F32)
            for s in range(1, SIDE):
                total = total + sbuf[s, t, :, cols].astype(F32)
            if k == 3:
                gates = total[:, 512:640]
                gates = jnp.where(first_lanes, gates + pltpu.roll(gates, 120, 1), 0.0)
                high = gates.astype(BF16).astype(F32)
                total = jnp.concatenate([total[:, :512], high + pltpu.roll(gates - high, 8, 1)], axis=1)
            tbuf[t, :, cols] = total.astype(BF16)
        for d in (2, 1, 3):
            second_sum(k, d).start()
        if k % 2 == 0:
            rbuf[z, :, cols] = tbuf[z, :, cols]
        else:
            rbuf[y, :, cols] = tbuf[y, :, cols]

    mix_own.wait()
    for axis in range(2):
        drain(mixv.at[0, pl.ds(0, 3), pl.ds(0, 16)], m_recv.at[1 - axis])
        for d in (2, 1, 3):
            mix_second(axis, d).start()
    def down_copy(kind, xs, part, device):
        block = ddv.at[2 * xs + core]
        if part is not None:
            block = block.at[pl.ds(16 * part, 16)]
        if kind == 4:
            return remote(block, block, d_send.at[2], d_recv.at[2], (chip, other))
        return remote(dd_ref if kind < 2 else block, block, down_send, down_recv.at[kind], (device, core))

    two, twohalf = dgv.at[pl.ds(0, 2)], dgv.at[pl.ds(0, 2), pl.ds(0, 16)]
    drain(two, dx_recv.at[0])
    for k in range(2):
        dense_copy(k, 2, xl, 0, (right, core)).start()
    drain(two, dx_recv.at[1])
    for k in range(2):
        dense_copy(k, 3, xr, 1, (left, core)).start()
    down_copy(0, x, None, right).start()
    down_copy(1, x, None, left).start()
    def row_sum(k):
        cols = slice(512 * k, 512 * k + 512)
        drain(rbuf.at[pl.ds(0, 3), :, columns(k)], r_recv.at[k])
        total = rbuf[0, :, cols].astype(F32)
        for s in range(1, SIDE):
            total = total + rbuf[s, :, cols].astype(F32)
        rows_ref[:, cols] = total.astype(BF16)

    row_sum(0)
    for h in range(4):
        query = upright(rows_ref[:, head_cols(0, h)].astype(F32)).astype(BF16)
        queries[h] = jnp.concatenate([query, query], axis=0)
    lane_index = lax.broadcasted_iota(jnp.int32, (128, 128), 1)

    def read_part(i, carry):
        mem_load(i).wait()
        for h in range(4):
            stored = memv[pl.ds(4 * i, 4), h].reshape(512, 128)
            top = stored.astype(BF16)
            rest = (stored - top.astype(F32)).astype(BF16)
            read = jnp.dot(jnp.concatenate([top, rest], axis=1), queries[h], preferred_element_type=F32)
            reads = rt[h]
            for j in range(4):
                reads = jnp.where(lane_index == 4 * i + j, read[128 * j:128 * j + 128, :], reads)
            rt[h] = reads
        return carry

    rt[...] = jnp.zeros(rt.shape, F32)
    lax.fori_loop(0, 4, read_part, 0)
    for k in range(1, 4):
        row_sum(k)
    total = rbuf[0, :, 2048:2176].astype(F32)
    for s in range(1, SIDE):
        total = total + rbuf[s, :, 2048:2176].astype(F32)
    gates_ref[...] = total + pltpu.roll(total, 120, 1)

    for load in late[2:]:
        load.wait()
    stab_new, carried, written = memory_gates(gates_ref[...], bias_ref[...], stab_ref[...])
    for h in range(4):
        query = rows_ref[:, head_cols(0, h)].astype(F32)
        key = rows_ref[:, head_cols(1, h)].astype(F32) * (128 ** (-0.5))
        value = rows_ref[:, head_cols(2, h)].astype(F32)
        match = jnp.sum(key * query, axis=1, keepdims=True) * written[:, h:h + 1]
        readout = carried[:, h:h + 1] * rt[h].T[0:ROWS, :] + match * value
        gate = jax.nn.sigmoid(rows_ref[:, head_cols(3, h)].astype(F32))
        scaled = rms_scale(readout, hgain_ref[:, head_cols(0, h)])
        gated_ref[:, head_cols(0, h)] = (scaled * gate).astype(BF16)

    gx[pl.ds(pl.multiple_of(ROWS * x, ROWS), ROWS), :] = gated_ref[...]

    def gx_copy(d):
        rows = pl.ds(pl.multiple_of(ROWS * x, ROWS), ROWS)
        peer = plane * SIDE + (x + d) % SIDE
        return remote(gated_ref, gx.at[rows, :], gx_send, gx_recv, (peer, core))

    for d in range(1, SIDE):
        gx_copy(d).start()
    stab_new_ref[...] = turned(stab_new)
    for h in range(4):
        key = rows_ref[:, head_cols(1, h)].astype(F32) * (128 ** (-0.5))
        carr_ref[h] = jnp.broadcast_to(carried[:, h:h + 1], (ROWS, 128))
        key = key * written[:, h:h + 1]
        top = key.astype(BF16).astype(F32)
        keys_ref[h] = jnp.concatenate([top, key - top], axis=0)
        value = rows_ref[:, head_cols(2, h)].astype(F32)
        vt_ref[h] = jnp.concatenate([value, value, jnp.zeros((96, 128), F32)], axis=0).T.astype(BF16)
    for axis in range(2):
        drain(mixv.at[pl.ds(0, 3), :, pl.ds(0, 16)], m_recv.at[2 + axis])
    drain(gx.at[pl.ds(0, 48), :], gx_recv)
    asend[...] = lax.dot_general(
        gx[...], mixv[...].reshape(512, 512), (((1,), (1,)), ((), ())), preferred_element_type=F32
    ).astype(BF16)

    def tb_copy(d, side):
        rows = pl.ds(pl.multiple_of(ROWS * ((x + d) % SIDE), ROWS), ROWS)
        peer = plane * SIDE + (x + d) % SIDE
        return remote(
            asend.at[rows, :], tb.at[core, x], tb_send, tb_recv,
            (peer, (core + side) % 2),
        )

    tb_list = [(0, 1)] + [(d, side) for d in (2, 1, 3) for side in (0, 1)]
    for d, side in tb_list:
        tb_copy(d, side).start()
    tb[core, x] = asend[pl.ds(pl.multiple_of(ROWS * x, ROWS), ROWS), :]
    tb_bytes = rx.at[pl.ds(0, 448), :]
    drain(tb_bytes, tb_recv)
    drain(twohalf, dx_recv.at[2])
    drain(twohalf, dx_recv.at[3])
    for k, (own, dst) in enumerate(((dg_ref, dgv), (du_ref, duv), (dd_ref, ddv))):
        for s in range(SIDE if k < 2 else 1):
            slot = dst.at[2 * ((x + s) % SIDE) + core]
            remote(own if s == 0 else slot, slot, d_send.at[k], d_recv.at[k], (chip, other)).start()
    attended = [tb[0, k].astype(F32) + tb[1, k].astype(F32) for k in range(SIDE)]
    lane = lax.broadcasted_iota(jnp.int32, (ROWS, 128), 1) // 32
    tiles = []
    for t in range(PLANE):
        tile = None
        for k in range(SIDE):
            part = attended[k][:, 128 * (t // 4):128 * (t // 4) + 128]
            shift = (32 * k - 32 * (t % 4)) % 128
            if shift:
                part = pltpu.roll(part, shift, 1)
            tile = part if tile is None else jnp.where(lane == k, part, tile)
        tiles.append(tile)
    residual = (tok_ref[...].astype(F32) + jnp.concatenate(tiles, axis=1)).astype(BF16)
    res[...] = residual
    normed = rms_scale(residual.astype(F32), gain_ref[...]).astype(BF16)
    ns[...] = normed
    def tile_rows(index):
        return pl.ds(pl.multiple_of(ROWS * index, ROWS), ROWS)

    parity = plane % 2

    own_row = y // 2
    low, high = pl.ds(0, 1024), pl.ds(1024, 1024)

    def acts_first(axis, d):
        peer = (along_z, along_y)[axis][d]
        cols = (low, high)[axis]
        return remote(
            ns.at[:, cols], da.at[z, own_row, :, cols], da_send.at[0], da_recv.at[axis], (peer, parity)
        )

    def acts_second(axis, d):
        peer = (along_z, along_y)[axis][d]
        block = da.at[z, :, :, high] if axis == 0 else da.at[:, own_row, :, low]
        return remote(block, block, da_send.at[1 + axis], da_recv.at[2 + axis], (peer, core))

    for axis in range(2):
        @pl.when(core == axis)
        def _():
            for d in (1, 0, 2):
                acts_first(axis, d).start()

    @pl.when(parity == core)
    def _():
        da[z, own_row] = ns[...]

    for b in range(8):
        cols = pl.ds(pl.multiple_of(1024 * core + 128 * b, 128), 128)
        n2[16 * b:16 * b + 16, :] = ns[:, cols]
    for k in range(4):
        obuf[256 * k:256 * k + 256, :] = jnp.dot(
            sel[256 * k:256 * k + 256, :], n2[...], preferred_element_type=F32
        ).astype(BF16)

    def x_copy(peer):
        return remote(
            obuf.at[tile_rows(peer), :], rx.at[tile_rows(chip), :], x_send, x_recv, (peer, core)
        )

    each_chip(plane, x, lambda peer: x_copy(peer).start())
    rx[tile_rows(chip), :] = obuf[tile_rows(chip), :]

    down_copy(0, x, None, right).wait_recv()
    down_copy(2, xl, 0, right).start()
    down_copy(1, x, None, left).wait_recv()
    down_copy(3, xr, 1, left).start()
    down_copy(4, xl, None, chip).start()
    down_copy(4, xr, None, chip).start()
    row_of = da.at[0, 0, :, low]

    @pl.when(parity == core)
    def _():
        drain(row_of, da_recv.at[1])
        drain(da.at[pl.ds(0, 3), 0, :, low], da_recv.at[0])
        for d in (1, 0, 2):
            acts_second(1, d).start()

    @pl.when(parity != core)
    def _():
        drain(da.at[pl.ds(0, 2), 0, :, low], da_recv.at[1])

    for d in (1, 0, 2):
        acts_second(0, d).start()

    drain(rx.at[pl.ds(0, 1008), :], x_recv)
    row = lax.broadcasted_iota(jnp.int32, (256, 256), 0)
    col = lax.broadcasted_iota(jnp.int32, (256, 256), 1)
    gather = (col == ((row % 32) // 2) * 16 + (row % 2) * 8 + row // 32).astype(F32).astype(BF16)
    scatter = (row == ((col % 32) // 2) * 16 + (col % 2) * 8 + col // 32).astype(F32).astype(BF16)
    for g in range(4):
        mixed_up = jnp.dot(gather, rx[256 * g:256 * g + 256, :], preferred_element_type=F32).astype(BF16)
        for b in range(8):
            xbuf[core, 32 * g:32 * g + 32, 128 * b:128 * b + 128] = mixed_up[32 * b:32 * b + 32, :]
    swap = remote(xbuf.at[core], xbuf.at[core], xo_send, xo_recv, (chip, other))
    swap.start()
    loads[0].wait()
    loads[1].wait()

    def expert_up_near(t, carry):
        cols = pl.ds(pl.multiple_of(256 * t, 256), 256)
        depth = pl.ds(pl.multiple_of(1024 * core, 1024), 1024)
        gacc[:, cols] = jnp.dot(xbuf[core], egv[depth, cols], preferred_element_type=F32)
        uacc[:, cols] = jnp.dot(xbuf[core], euv[depth, cols], preferred_element_type=F32)
        return carry

    def expert_up_far(t, carry):
        cols = pl.ds(pl.multiple_of(256 * t, 256), 256)
        depth = pl.ds(pl.multiple_of(1024 * other, 1024), 1024)
        gate_pre = gacc[:, cols] + jnp.dot(xbuf[other], egv[depth, cols], preferred_element_type=F32)
        up_pre = uacc[:, cols] + jnp.dot(xbuf[other], euv[depth, cols], preferred_element_type=F32)
        gate_clamped = jnp.minimum(gate_pre, clamp_limit)
        up_clamped = jnp.clip(up_pre, -clamp_limit, clamp_limit)
        hbuf[:, cols] = (
            (up_clamped + 1.0) * gate_clamped * jax.nn.sigmoid(sigmoid_slope * gate_clamped)
        ).astype(BF16)
        return carry

    lax.fori_loop(0, 4, expert_up_near, 0)
    for k, dst in enumerate((dgv, duv)):
        drain(dst.at[0], load_sem.at[3 + k])
        drain(dst.at[pl.ds(0, 4)], d_recv.at[k])

    @pl.when(parity == core)
    def _():
        drain(da.at[:, 0, :, low], da_recv.at[3])

    @pl.when(parity != core)
    def _():
        drain(da.at[:, :, :, low], da_recv.at[3])

    drain(da.at[pl.ds(0, 3), :, :, low], da_recv.at[2])

    down_copy(2, xa, 0, right).wait_recv()
    down_copy(3, xa, 1, left).wait_recv()
    down_copy(4, xa, None, chip).start()
    dense_rows = da[...].reshape(128, 2048)
    over_last = (((1,), (1,)), ((), ()))
    gate_rows = lax.dot_general(dense_rows, dgv[...].reshape(256, 2048), over_last, preferred_element_type=F32)
    lift_rows = lax.dot_general(dense_rows, duv[...].reshape(256, 2048), over_last, preferred_element_type=F32)
    activity = (gate_rows / (1.0 + jnp.exp(-gate_rows)) * lift_rows).astype(BF16)
    drain(ddv.at[0], load_sem.at[5])
    drain(ddv.at[pl.ds(0, 4)], d_recv.at[2])
    down = ddv[...].reshape(256, 2048)
    for h in range(2):
        for t in range(2):
            lower = 1024 * h + 512 * t
            part = jnp.dot(activity, down[:, lower:lower + 512], preferred_element_type=F32).astype(BF16)
            dout[h, :, :, :, 512 * t:512 * t + 512] = part.reshape(SIDE, 2, ROWS, 512)

    for d in range(3):
        zt = (z + d + 1) % SIDE
        remote(dout.at[0, zt], zsum.at[z], rp_send.at[0], rp_recv.at[0], (along_z[d], core)).start()
    zsum[z] = dout[0, z]
    for i in range(2):
        yt = 2 * i + core
        target = (z * SIDE + yt) * SIDE + x

        @pl.when(yt != y)
        def _():
            remote(dout.at[1, :, i], ysum.at[y], rp_send.at[1], rp_recv.at[1], (target, core)).start()

        @pl.when(yt == y)
        def _():
            ysum[y] = dout[1, :, i]

    swap.wait_recv()
    lax.fori_loop(0, 4, expert_up_far, 0)
    loads[2].wait()

    def y_copy(t):
        return remote(ysend.at[t], yrecv.at[t], y_send, y_recv, (chip, other))

    def expert_down_far(t, carry):
        cols = pl.ds(pl.multiple_of(1024 * other + 256 * t, 256), 256)
        ysend[t] = jnp.dot(hbuf[...], edv[:, cols], preferred_element_type=F32).astype(BF16)
        y_copy(t).start()
        return carry

    def expert_down_near(t, carry):
        cols = pl.ds(pl.multiple_of(1024 * core + 256 * t, 256), 256)
        yown[t] = jnp.dot(hbuf[...], edv[:, cols], preferred_element_type=F32).astype(BF16)
        return carry

    lax.fori_loop(0, 4, expert_down_far, 0)
    lax.fori_loop(0, 4, expert_down_near, 0)

    drain(yrecv, y_recv)
    for g in range(4):
        rows = slice(32 * g, 32 * g + 32)
        stacked = []
        for t in range(4):
            both = (yown[t, rows, :].astype(F32) + yrecv[t, rows, :].astype(F32)).astype(BF16)
            stacked += [both[:, :128], both[:, 128:]]
        yret[256 * g:256 * g + 256, :] = jnp.dot(
            scatter, jnp.concatenate(stacked, axis=0), preferred_element_type=F32
        ).astype(BF16)

    def q_copy(peer):
        return remote(
            yret.at[tile_rows(peer), :], rret.at[tile_rows(chip), :], q_send, q_recv, (peer, core)
        )

    each_chip(plane, x, lambda peer: q_copy(peer).start())
    rret[tile_rows(chip), :] = yret[tile_rows(chip), :]

    drain(zsum.at[pl.ds(0, 3)], rp_recv.at[0])
    for i in range(2):
        total = zsum[0, i].astype(F32)
        for s in range(1, SIDE):
            total = total + zsum[s, i].astype(F32)
        zout[i] = total.astype(BF16)
    for i in range(2):
        yt = 2 * i + core
        target = (z * SIDE + yt) * SIDE + x

        @pl.when((yt != y) | (core != 0))
        def _():
            remote(zout.at[i], dr.at[y], dr_send.at[0], dr_recv, (target, 0)).start()

        @pl.when((yt == y) & (core == 0))
        def _():
            dr[y] = zout[i]

    @pl.when(parity == core)
    def _():
        drain(ysum.at[pl.ds(0, 3)], rp_recv.at[1])
        for t in range(SIDE):
            total = ysum[0, t].astype(F32)
            for s in range(1, SIDE):
                total = total + ysum[s, t].astype(F32)
            yout[t] = total.astype(BF16)
        for d in range(3):
            zt = (z + d + 1) % SIDE
            remote(yout.at[zt], dr.at[z], dr_send.at[1], dr_recv, (along_z[d], 1)).start()

        @pl.when(core == 0)
        def _():
            remote(yout.at[z], dr.at[z], dr_send.at[1], dr_recv, (chip, 1)).start()

        @pl.when(core != 0)
        def _():
            dr[z] = yout[z]

    @pl.when(parity == core)
    def _():
        drain(dr.at[pl.ds(0, 3)], dr_recv)

    @pl.when(parity != core)
    def _():
        drain(dr, dr_recv)

    branch = dr[0].astype(F32)
    for s in range(1, SIDE):
        branch = branch + dr[s].astype(F32)

    drain(rret.at[pl.ds(0, 1008), :], q_recv)
    returned = rret[...]
    routed = jnp.dot(comb_hi[...], returned, preferred_element_type=F32) + jnp.dot(
        comb_lo[...], returned, preferred_element_type=F32
    )
    routed = jnp.concatenate([routed[16 * b:16 * b + 16, :] for b in range(8)], axis=1)
    own_cols = pl.ds(pl.multiple_of(1024 * core, 1024), 1024)
    out_ref[...] = (res[:, own_cols].astype(F32) + routed + branch * scale_ref[:, own_cols]).astype(BF16)

    drain(gx.at[pl.ds(0, 48), :], gx_send)
    drain(tb_bytes, tb_send)
    drain(rx.at[pl.ds(0, 1008), :], x_send)
    drain(rret.at[pl.ds(0, 1008), :], q_send)
    drain(yrecv, y_send)
    drain(xbuf.at[0], xo_send)
    for k, dst in enumerate((dgv, duv, ddv)):
        drain(dst.at[pl.ds(0, 4)], d_send.at[k])
    drain(ddv.at[pl.ds(0, 3)], down_send)

    drain(da.at[pl.ds(0, 3), 0, :, low], da_send.at[0])
    drain(da.at[pl.ds(0, 3), :, :, low], da_send.at[1])

    @pl.when(parity == core)
    def _():
        drain(da.at[pl.ds(0, 3)], da_send.at[2])

    drain(zsum.at[pl.ds(0, 3)], rp_send.at[0])

    @pl.when(parity == core)
    def _():
        drain(ysum.at[0], rp_send.at[1])

        @pl.when(core == 0)
        def _():
            drain(dr.at[0], dr_send.at[0])
            drain(dr, dr_send.at[1])

        @pl.when(core != 0)
        def _():
            drain(dr.at[pl.ds(0, 2)], dr_send.at[0])
            drain(dr.at[pl.ds(0, 3)], dr_send.at[1])

    @pl.when(parity != core)
    def _():
        drain(ysum.at[pl.ds(0, 2)], rp_send.at[1])
        drain(dr.at[pl.ds(0, 2)], dr_send.at[0])
    drain(wbuf.at[pl.ds(0, 96), :], w_send)
    drain(gbuf.at[pl.ds(0, 3)], g_send)
    drain(abuf.at[pl.ds(0, 240), :], a_send)
    drain(mixv.at[pl.ds(0, 3), :, :], m_send)
    drain(mixv.at[0, pl.ds(0, 3)], m_send)
    drain(sbuf.at[pl.ds(0, 3)], p_send)
    drain(rbuf.at[pl.ds(0, 3)], r_send)
    for k in range(2):
        drain(dense[k][1].at[pl.ds(0, 3)], dx_send.at[k])


def decode_step(*operands):
    dma = pltpu.SemaphoreType.DMA
    vm = pltpu.VMEM
    return pl.pallas_call(
        step_kernel,
        out_shape=(
            jax.ShapeDtypeStruct((ROWS, 1024), BF16),
            jax.ShapeDtypeStruct((4, ROWS, 128), F32),
            jax.ShapeDtypeStruct((4, 32, 128), F32),
            jax.ShapeDtypeStruct((4, 128, 128), BF16),
            jax.ShapeDtypeStruct((4, ROWS), F32),
        ),
        in_specs=[ANY_SPEC] * 23,
        out_specs=(VMEM_SPEC,) * 5,
        scratch_shapes=[
            vm((1, 2048), F32), vm((4, 32), BF16), vm((4, 32), BF16), vm((128, 2048), BF16), vm((4, 8, 128), F32),
            vm((ROWS, 2048), BF16), vm((256, 128), BF16),
            vm((SIDE, SIDE, ROWS, 2176), BF16), vm((SIDE, SIDE, ROWS, 2176), BF16),
            vm((SIDE, ROWS, 2176), BF16), vm((SIDE, ROWS, 2176), BF16),
            vm((ROWS, 4, 128, 128), F32), vm((ROWS, 2048), BF16), vm((ROWS, 128), F32), vm((1, 4), F32),
            vm((4, ROWS), F32), vm((1, 512), F32), vm((4, 128, 128), F32), vm((4, 256, 128), BF16),
            vm((ROWS, 512), BF16), vm((ROWS, 2048), BF16), vm((1, 2048), F32),
            vm((4, ROWS), jnp.int32), vm((4, ROWS), F32), vm((1, 2048), F32),
            vm((2048, 1024), BF16), vm((2048, 1024), BF16), vm((1024, 2048), BF16),
            vm((8, 32, 2048), BF16), vm((8, 32, 2048), BF16), vm((8, 32, 2048), BF16),
            vm((SIDE, SIDE, 32, 512), BF16),
            vm((64, 512), BF16), vm((64, 512), BF16), vm((2, 4, ROWS, 512), BF16),
            vm((ROWS, 2048), BF16), vm((ROWS, 2048), BF16), vm((128, 128), BF16),
            vm((1024, 128), BF16), vm((128, 1024), BF16), vm((128, 1024), BF16),
            vm((1024, 128), BF16), vm((1024, 128), BF16), vm((2, 128, 1024), BF16),
            vm((128, 1024), F32), vm((128, 1024), F32), vm((128, 1024), BF16),
            vm((4, 128, 256), BF16), vm((4, 128, 256), BF16), vm((4, 128, 256), BF16),
            vm((1024, 128), BF16), vm((1024, 128), BF16),
            vm((SIDE, 2, ROWS, 2048), BF16), vm((2, SIDE, 2, ROWS, 1024), BF16), vm((SIDE, ROWS, 1024), BF16),
            vm((SIDE, 2, ROWS, 1024), BF16), vm((SIDE, SIDE, ROWS, 1024), BF16),
            vm((2, ROWS, 1024), BF16), vm((SIDE, ROWS, 1024), BF16),
            dma((6,)),
            dma, dma((4, 4)),
            dma, dma,
            dma, dma,
            dma, dma((4,)),
            dma, dma((4,)),
            dma, dma((4,)),
            dma((2,)), dma((4,)),
            pltpu.SemaphoreType.REGULAR, dma((7,)),
            dma((6,)),
            dma, dma,
            dma, dma,
            dma, dma,
            dma((3,)), dma((4,)),
            dma, dma,
            dma, dma,
            dma((2,)), dma,
            dma, dma,
            dma((3,)), dma((3,)),
            dma((4,)),
            dma, dma((4,)),
            dma((2,)), dma((2,)),
        ],
        compiler_params=pltpu.CompilerParams(
            collective_id=0, has_side_effects=True, vmem_limit_bytes=VMEM_LIMIT
        ),
        name="decode_step",
    )(*operands)


def body(
    tokens, norm_gain, query_weight, key_weight, value_weight, outgate_weight, input_weight, forget_weight,
    forget_bias, memory, stabilizer, head_gain, mix_weight, second_gain, route_experts, route_weight,
    expert_gate, expert_up, expert_down, dense_gate, dense_up, dense_down, branch_scale,
):
    mixed, carried, keys, values, stab_new = decode_step(
        tokens, norm_gain.reshape(1, -1), query_weight, key_weight, value_weight, outgate_weight,
        input_weight.T, forget_weight.T, mix_weight.T, dense_gate, dense_up, dense_down,
        memory, forget_bias.reshape(1, -1), stabilizer.T, head_gain.reshape(1, -1), second_gain.reshape(1, -1),
        route_experts.T, route_weight.T, expert_gate, expert_up, expert_down, branch_scale.reshape(1, -1),
    )
    memory_new, stab_new, mixed = memory_update(carried, keys, values, stab_new, memory, mixed)
    return mixed, memory_new, stab_new.T


def solution(mesh):
    in_specs = (
        P("ep", None), P(),
        P("ep", "tp"), P("ep", "tp"), P("ep", "tp"), P("ep", "tp"), P("ep", "tp"), P("ep", "tp"),
        P("tp"), P("ep", "tp", None, None), P("ep", "tp"), P("tp"), P("tp", "ep"), P(),
        P("ep", None), P("ep", None),
        P("ep", None, "tp"), P("ep", None, "tp"), P("ep", "tp", None),
        P(("ep", "tp"), None), P(("ep", "tp"), None), P(("ep", "tp"), None), P(),
    )
    out_specs = (P("ep", "tp"), P("ep", "tp", None, None), P("ep", "tp"))
    return jax.shard_map(body, mesh=mesh, in_specs=in_specs, out_specs=out_specs, check_vma=False)
```

```python
import jax
import jax.numpy as jnp
from jax import lax
from jax.experimental import pallas as pl
from jax.experimental.pallas import tpu as pltpu
from jax.sharding import PartitionSpec as P

norm_eps = 1e-05
clamp_limit = 7.0
sigmoid_slope = 1.702
F32 = jnp.float32
BF16 = jnp.bfloat16
MESH = pl.DeviceIdType.MESH
VMEM_SPEC = pl.BlockSpec(memory_space=pltpu.VMEM)
ANY_SPEC = pl.BlockSpec(memory_space=pl.ANY)
VMEM_LIMIT = 60 * 1024 * 1024

SIDE = 4
PLANE = 16
CHIPS = 64
ROWS = 16
SEQS = 2


def rms_scale(values, gain):
    mean_square = jnp.mean(values * values, axis=-1, keepdims=True)
    return values * lax.rsqrt(mean_square + norm_eps) * gain


def own_place():
    chip = lax.axis_index("ep")
    core = lax.axis_index("tp")
    return chip, core, chip % SIDE, chip // SIDE


def plane_shift(plane, step):
    z = (plane // SIDE + step // SIDE) % SIDE
    y = (plane % SIDE + step % SIDE) % SIDE
    return z * SIDE + y


def axis_peers(plane, x):
    z, y = plane // SIDE, plane % SIDE
    along_y = [((z * SIDE + (y + d) % SIDE) * SIDE + x) for d in range(1, SIDE)]
    along_z = [((((z + d) % SIDE) * SIDE + y) * SIDE + x) for d in range(1, SIDE)]
    along_x = [(plane * SIDE + (x + d) % SIDE) for d in range(1, SIDE)]
    return along_x, along_y, along_z


def each_chip(plane, x, act):
    xs = [(x + d) % SIDE for d in range(SIDE)]

    def on_plane(step, carry):
        base = plane_shift(plane, step) * SIDE
        for d in range(SIDE):
            act(base + xs[d])
        return carry

    lax.fori_loop(1, PLANE, on_plane, 0)
    for d in range(1, SIDE):
        act(plane * SIDE + xs[d])


def remote(src, dst, send, recv, device):
    return pltpu.make_async_remote_copy(
        src_ref=src, dst_ref=dst, send_sem=send, recv_sem=recv,
        device_id=device, device_id_type=MESH,
    )


def drain(ref, sem):
    pltpu.make_async_copy(ref, ref, sem).wait()


def identity(n):
    row = lax.broadcasted_iota(jnp.int32, (n, n), 0)
    return (row == lax.broadcasted_iota(jnp.int32, (n, n), 1)).astype(F32)


def turned(values):
    rows = values.shape[0]
    return lax.dot_general(
        identity(values.shape[1]), values, (((1,), (1,)), ((), ())),
        preferred_element_type=F32, precision=lax.Precision.HIGHEST,
    ).reshape(values.shape[1], rows)


def memory_gates(gates, bias, stab_t):
    stab = turned(stab_t)
    input_pre = gates[:, 0:4]
    forget = pltpu.roll(gates, 124, 1)[:, 0:4] + bias
    log_forget = jnp.minimum(forget, 0.0) - jnp.log1p(jnp.exp(-jnp.abs(forget)))
    stab_new = jnp.maximum(log_forget + stab, input_pre)
    return stab_new, jnp.exp(log_forget + stab - stab_new), jnp.exp(input_pre - stab_new)


def head_cols(part, h):
    return slice(512 * part + 128 * h, 512 * part + 128 * h + 128)


def upright(rows):
    return jnp.concatenate([rows, jnp.zeros((112, 128), F32)], axis=0).T


def memory_kernel(
    carr_hbm, keys_hbm, vt_hbm, stab_hbm, mem_ref, mixed_hbm,
    new_ref, stab_new_ref, mixed_ref,
    memv, carr, keys, vt, small_sem, load_sem, store_sem,
):
    small = [
        pltpu.make_async_copy(src, dst, small_sem.at[k])
        for k, (src, dst) in enumerate((
            (carr_hbm, carr), (keys_hbm, keys), (vt_hbm, vt), (stab_hbm, stab_new_ref), (mixed_hbm, mixed_ref),
        ))
    ]
    for copy in small:
        copy.start()

    def part(i):
        return pl.ds(SEQS * i, SEQS)

    def load(i):
        return pltpu.make_async_copy(mem_ref.at[part(i)], memv.at[part(i)], load_sem.at[i])

    def store(i):
        return pltpu.make_async_copy(memv.at[part(i)], new_ref.at[part(i)], store_sem)

    for i in range(6):
        load(i).start()
    for copy in small:
        copy.wait()
    row = lax.broadcasted_iota(jnp.int32, (32, 128), 0) % ROWS

    def advance(i, carry):
        load(i).wait()

        @pl.when(i + 6 < ROWS // SEQS)
        def _():
            load(i + 6).start()

        for h in range(4):
            chosen = [jnp.where(row == SEQS * i + j, keys[h], 0.0) for j in range(SEQS)]
            outer = jnp.dot(
                vt[h, :, 0:32], jnp.concatenate(chosen, axis=1).astype(BF16), preferred_element_type=F32
            )
            for j in range(SEQS):
                place = SEQS * i + j
                memv[place, h] = carr[h, pl.ds(place, 1), :] * memv[place, h] + outer[:, 128 * j:128 * j + 128]
        store(i).start()
        return carry

    lax.fori_loop(0, ROWS // SEQS, advance, 0)
    drain(memv, store_sem)


def memory_update(carried, keys, values, stab_new, memory, mixed):
    dma = pltpu.SemaphoreType.DMA
    vm = pltpu.VMEM
    return pl.pallas_call(
        memory_kernel,
        out_shape=(
            jax.ShapeDtypeStruct((ROWS, 4, 128, 128), F32),
            jax.ShapeDtypeStruct((4, ROWS), F32),
            jax.ShapeDtypeStruct((ROWS, 1024), BF16),
        ),
        in_specs=[ANY_SPEC] * 6,
        out_specs=(ANY_SPEC, VMEM_SPEC, VMEM_SPEC),
        scratch_shapes=[
            vm((ROWS, 4, 128, 128), F32), vm((4, ROWS, 128), F32), vm((4, 32, 128), F32), vm((4, 128, 128), BF16),
            dma((5,)), dma((ROWS // SEQS,)), dma,
        ],
        compiler_params=pltpu.CompilerParams(vmem_limit_bytes=VMEM_LIMIT),
        name="memory_update",
    )(carried, keys, values, stab_new, memory, mixed)


def step_kernel(
    tok_hbm, gain1_hbm, wq_ref, wk_ref, wv_ref, wo_ref, wi_ref, wf_ref, mix_ref, dg_ref, du_ref, dd_ref,
    mem_ref, bias_hbm, stab_hbm, hgain_hbm, gain_hbm, route_hbm, weight_hbm, eg_ref, eu_ref, ed_ref, scale_hbm,
    out_ref, carr_ref, keys_ref, vt_ref, stab_new_ref,
    gainv, wiv, wfv, wbuf, gbuf, nbuf, abuf, pbuf, sbuf, tbuf, rbuf,
    memv, rows_ref, gates_ref, bias_ref, stab_ref, hgain_ref, rt, queries, gated_ref,
    tok_ref, gain_ref, route_ref, weight_ref, scale_ref,
    egv, euv, edv, dgv, duv, ddv, mixv, gx, asend, tb, ns, res, n2, sel, comb_hi, comb_lo, obuf, rx,
    xbuf, gacc, uacc, hbuf, yown, ysend, yrecv, yret, rret, da, dout, dr, zsum, ysum, zout, yout,
    load1_sem, w_send, w_recv, g_send, g_recv, a_send, a_recv, m_send, m_recv, p_send, p_recv, r_send, r_recv,
    dx_send, dx_recv, near_sem, late_sem,
    load_sem, gx_send, gx_recv, tb_send, tb_recv, x_send, x_recv, da_send, da_recv,
    y_send, y_recv, q_send, q_recv, dr_send, dr_recv, xo_send, xo_recv, d_send, d_recv, mem_sem, down_send, down_recv,
    rp_send, rp_recv,
):
    chip, core, x, plane = own_place()
    z, y = plane // SIDE, plane % SIDE
    right = plane * SIDE + (x + 1) % SIDE
    left = plane * SIDE + (x + 3) % SIDE
    across = plane * SIDE + (x + 2) % SIDE
    xl, xr = (x + 3) % SIDE, (x + 1) % SIDE

    other, xa = 1 - core, (x + 2) % SIDE
    barrier = pltpu.get_barrier_semaphore()
    along_x, along_y, along_z = axis_peers(plane, x)
    for peer in along_z + along_x + along_y:
        pl.semaphore_signal(barrier, inc=1, device_id=(peer, core), device_id_type=MESH)
    pl.semaphore_signal(barrier, inc=1, device_id=(chip, other), device_id_type=MESH)

    def w_rows(xs):
        return pl.ds(pl.multiple_of(32 * xs, 32), 32)

    def half_rows(xs, half):
        return pl.ds(pl.multiple_of(32 * xs + 16 * half, 16), 16)

    for k, ref in enumerate((wq_ref, wk_ref, wv_ref, wo_ref)):
        load = pltpu.make_async_copy(ref, wbuf.at[w_rows(x), pl.ds(512 * k, 512)], load1_sem.at[0])
        load.start()
    small = [
        pltpu.make_async_copy(src, dst, load1_sem.at[2 + k])
        for k, (src, dst) in enumerate(((tok_hbm, tok_ref), (gain1_hbm, gainv), (wi_ref, wiv), (wf_ref, wfv)))
    ]
    for load in small:
        load.start()
    late = [
        pltpu.make_async_copy(src, dst, late_sem.at[k])
        for k, (src, dst) in enumerate((
            (route_hbm, route_ref), (weight_hbm, weight_ref), (bias_hbm, bias_ref), (stab_hbm, stab_ref),
            (hgain_hbm, hgain_ref), (gain_hbm, gain_ref), (scale_hbm, scale_ref),
        ))
    ]
    for load in small:
        load.wait()

    normed = rms_scale(tok_ref[...].astype(F32), gainv[...])
    nbuf[...] = normed.astype(BF16)
    place = (
        lax.broadcasted_iota(jnp.int32, (32, 128), 1) == lax.broadcasted_iota(jnp.int32, (32, 128), 0) + 32 * x
    ).astype(F32)
    gate_in = jnp.dot(wiv[...].astype(F32), place, preferred_element_type=F32)
    gate_fo = jnp.dot(wfv[...].astype(F32), place, preferred_element_type=F32)
    gbuf[x] = jnp.concatenate([gate_in, gate_fo], axis=0)
    drain(wbuf.at[w_rows(x), :], load1_sem.at[0])
    pl.semaphore_wait(barrier, 9 + 1)
    for peer in along_y:
        pl.semaphore_signal(near_sem, inc=1, device_id=(peer, core), device_id_type=MESH)

    def w_copy(k, kind, xs, part, device):
        rows = w_rows(xs) if part is None else half_rows(xs, part)
        block = wbuf.at[rows, pl.ds(512 * k, 512)]
        return remote(block, block, w_send, w_recv.at[k, kind], (device, core))

    for k in range(4):
        w_copy(k, 0, x, None, right).start()
        w_copy(k, 1, x, None, left).start()
    for peer in (right, left, across):
        remote(gbuf.at[x], gbuf.at[x], g_send, g_recv, (peer, core)).start()

    def token_copy(step):
        peer = plane_shift(plane, step)
        return remote(
            nbuf.at[:, pl.ds(pl.multiple_of(128 * peer, 128), 128)],
            abuf.at[pl.ds(pl.multiple_of(ROWS * plane, ROWS), ROWS), :],
            a_send, a_recv, (peer * SIDE + x, core),
        )

    def plane_peer(axis, step):
        if axis == 0:
            return (z + step) % SIDE, y
        return z, (y + step) % SIDE

    def device_of(zt, yt):
        return ((zt * SIDE + yt) * SIDE + x, core)

    def mix_first(axis, step):
        part = pl.ds(16 * axis, 16)
        return remote(
            mix_ref.at[part], mixv.at[z, y, part], m_send, m_recv.at[axis], device_of(*plane_peer(axis, step))
        )

    def mix_second(axis, step):
        part = pl.ds(16 * (1 - axis), 16)
        block = mixv.at[z, :, part] if axis == 0 else mixv.at[:, y, part]
        return remote(block, block, m_send, m_recv.at[2 + axis], device_of(*plane_peer(axis, step)))

    def start_tokens(step, carry):
        token_copy(step).start()
        return carry

    pl.semaphore_wait(near_sem, 3)
    lax.fori_loop(1, PLANE, start_tokens, 0)
    abuf[pl.ds(pl.multiple_of(ROWS * plane, ROWS), ROWS), :] = nbuf[:, pl.ds(pl.multiple_of(128 * plane, 128), 128)]
    for axis in range(2):
        for d in (2, 1, 3):
            mix_first(axis, d).start()
    mix_own = pltpu.make_async_copy(mix_ref, mixv.at[z, y], load1_sem.at[1])
    mix_own.start()

    dense = ((dg_ref, dgv), (du_ref, duv))

    def dense_copy(k, kind, xs, part, device):
        block = dense[k][1].at[2 * xs + core]
        if part is not None:
            block = block.at[pl.ds(16 * part, 16)]
        source = dense[k][0] if kind in (0, 1) else block
        return remote(source, block, dx_send.at[k], dx_recv.at[kind], device)

    def w_relay(k):
        w_copy(k, 0, x, None, right).wait_recv()
        w_copy(k, 2, xl, 0, right).start()
        w_copy(k, 1, x, None, left).wait_recv()
        w_copy(k, 3, xr, 1, left).start()

    w_relay(0)
    w_relay(1)
    for load in late:
        load.start()
    def mem_load(i):
        part = pl.ds(4 * i, 4)
        return pltpu.make_async_copy(mem_ref.at[part], memv.at[part], mem_sem.at[i])

    for i in range(4):
        mem_load(i).start()
    for k in range(3):
        own_load = pltpu.make_async_copy((dg_ref, du_ref, dd_ref)[k], (dgv, duv, ddv)[k].at[2 * x + core], load_sem.at[3 + k])
        own_load.start()
    late[0].wait()
    late[1].wait()
    spread = (
        lax.broadcasted_iota(jnp.int32, (ROWS, 128), 1) % ROWS == lax.broadcasted_iota(jnp.int32, (ROWS, 128), 0)
    ).astype(F32)
    route = jnp.dot(route_ref[...].astype(F32), spread, preferred_element_type=F32, precision=lax.Precision.HIGHEST)
    weight = jnp.dot(weight_ref[...], spread, preferred_element_type=F32, precision=lax.Precision.HIGHEST)
    expert = lax.broadcasted_iota(jnp.int32, (CHIPS, 128), 0).astype(F32)
    hit = jnp.zeros((CHIPS, 128), F32)
    chosen = jnp.zeros((CHIPS, 128), F32)
    for k in range(4):
        same = (route[k:k + 1, :] == expert).astype(F32)
        hit = hit + same
        chosen = chosen + same * weight[k:k + 1, :]
    col = lax.broadcasted_iota(jnp.int32, (128, 128), 1) % ROWS
    row = lax.broadcasted_iota(jnp.int32, (128, 128), 0)
    before = ((row < ROWS) & (row < col)).astype(F32)
    rank = jnp.dot(hit, before, preferred_element_type=F32)
    first = hit * (rank == 0.0).astype(F32)
    second = hit * (rank == 1.0).astype(F32)
    block_row = lax.broadcasted_iota(jnp.int32, (8, 128), 0)
    block_col = lax.broadcasted_iota(jnp.int32, (8, 128), 1) // ROWS
    diagonal = (block_row == block_col).astype(F32)

    def widened(top, bottom):
        low = top[:, None, :] * diagonal[None, :, :]
        high = bottom[:, None, :] * diagonal[None, :, :]
        return jnp.concatenate([low, high], axis=1).reshape(1024, 128)

    sel[...] = widened(first, second).astype(BF16)
    comb = widened(first * chosen, second * chosen).T
    comb_top = comb.astype(BF16)
    comb_hi[...] = comb_top
    comb_lo[...] = (comb - comb_top.astype(F32)).astype(BF16)
    w_relay(2)
    w_relay(3)
    for k in range(2):
        dense_copy(k, 0, x, None, (right, core)).start()
        dense_copy(k, 1, x, None, (left, core)).start()
    drain(abuf.at[pl.ds(0, 240), :], a_recv)
    drain(gbuf.at[pl.ds(0, 3)], g_recv)
    gate_w = (gbuf[0] + gbuf[1] + gbuf[2] + gbuf[3]).astype(BF16)
    gate_w = jnp.concatenate([gate_w.astype(F32), jnp.zeros((120, 128), F32)], axis=0).astype(BF16)
    def columns(k):
        return pl.ds(512 * k, 640 if k == 3 else 512)

    def first_sum(k, step):
        axis = (k + 1) % 2
        zt, yt = plane_peer(axis, step)
        src = pbuf.at[zt, :, :, columns(k)] if axis == 0 else pbuf.at[:, yt, :, columns(k)]
        own = z if axis == 0 else y
        return remote(src, sbuf.at[own, :, :, columns(k)], p_send, p_recv.at[k], device_of(zt, yt))

    def second_sum(k, step):
        axis = k % 2
        zt, yt = plane_peer(axis, step)
        target, own = (zt, z) if axis == 0 else (yt, y)
        return remote(
            tbuf.at[target, :, columns(k)], rbuf.at[own, :, columns(k)], r_send, r_recv.at[k], device_of(zt, yt)
        )

    for k in range(4):
        w_copy(k, 2, xl, 0, right).wait_recv()
        w_copy(k, 3, xr, 1, left).wait_recv()
        cols = slice(512 * k, 512 * k + 512)
        part = jnp.dot(abuf[...], wbuf[:, cols], preferred_element_type=F32).astype(BF16)
        pbuf[:, :, :, cols] = part.reshape(SIDE, SIDE, ROWS, 512)
        if k == 3:
            gates = lax.dot_general(abuf[...], gate_w, (((1,), (1,)), ((), ())), preferred_element_type=F32)
            high = gates.astype(BF16).astype(F32)
            part = (high + pltpu.roll(gates - high, 8, 1)).astype(BF16)
            pbuf[:, :, :, 2048:2176] = part.reshape(SIDE, SIDE, ROWS, 128)
        for d in (2, 1, 3):
            first_sum(k, d).start()
    loads = []
    for k, (src, dst) in enumerate(((eg_ref, egv), (eu_ref, euv), (ed_ref, edv))):
        loads.append(pltpu.make_async_copy(src.at[0], dst, load_sem.at[k]))
    for load in loads:
        load.start()
    first_lanes = lax.broadcasted_iota(jnp.int32, (ROWS, 128), 1) < 8
    for k in range(4):
        cols = slice(512 * k, 2176 if k == 3 else 512 * k + 512)
        if k % 2 == 0:
            sbuf[y, :, :, cols] = pbuf[:, y, :, cols]
        else:
            sbuf[z, :, :, cols] = pbuf[z, :, :, cols]
        drain(sbuf.at[pl.ds(0, 3), :, :, columns(k)], p_recv.at[k])
        for t in range(SIDE):
            total = sbuf[0, t, :, cols].astype(F32)
            for s in range(1, SIDE):
                total = total + sbuf[s, t, :, cols].astype(F32)
            if k == 3:
                gates = total[:, 512:640]
                gates = jnp.where(first_lanes, gates + pltpu.roll(gates, 120, 1), 0.0)
                high = gates.astype(BF16).astype(F32)
                total = jnp.concatenate([total[:, :512], high + pltpu.roll(gates - high, 8, 1)], axis=1)
            tbuf[t, :, cols] = total.astype(BF16)
        for d in (2, 1, 3):
            second_sum(k, d).start()
        if k % 2 == 0:
            rbuf[z, :, cols] = tbuf[z, :, cols]
        else:
            rbuf[y, :, cols] = tbuf[y, :, cols]

    mix_own.wait()
    for axis in range(2):
        drain(mixv.at[0, pl.ds(0, 3), pl.ds(0, 16)], m_recv.at[1 - axis])
        for d in (2, 1, 3):
            mix_second(axis, d).start()
    def down_copy(kind, xs, part, device):
        block = ddv.at[2 * xs + core]
        if part is not None:
            block = block.at[pl.ds(16 * part, 16)]
        if kind == 4:
            return remote(block, block, d_send.at[2], d_recv.at[2], (chip, other))
        return remote(dd_ref if kind < 2 else block, block, down_send, down_recv.at[kind], (device, core))

    two, twohalf = dgv.at[pl.ds(0, 2)], dgv.at[pl.ds(0, 2), pl.ds(0, 16)]
    drain(two, dx_recv.at[0])
    for k in range(2):
        dense_copy(k, 2, xl, 0, (right, core)).start()
    drain(two, dx_recv.at[1])
    for k in range(2):
        dense_copy(k, 3, xr, 1, (left, core)).start()
    down_copy(0, x, None, right).start()
    down_copy(1, x, None, left).start()
    def row_sum(k):
        cols = slice(512 * k, 512 * k + 512)
        drain(rbuf.at[pl.ds(0, 3), :, columns(k)], r_recv.at[k])
        total = rbuf[0, :, cols].astype(F32)
        for s in range(1, SIDE):
            total = total + rbuf[s, :, cols].astype(F32)
        rows_ref[:, cols] = total.astype(BF16)

    row_sum(0)
    for h in range(4):
        query = upright(rows_ref[:, head_cols(0, h)].astype(F32)).astype(BF16)
        queries[h] = jnp.concatenate([query, query], axis=0)
    lane_index = lax.broadcasted_iota(jnp.int32, (128, 128), 1)

    def read_part(i, carry):
        mem_load(i).wait()
        for h in range(4):
            stored = memv[pl.ds(4 * i, 4), h].reshape(512, 128)
            top = stored.astype(BF16)
            rest = (stored - top.astype(F32)).astype(BF16)
            read = jnp.dot(jnp.concatenate([top, rest], axis=1), queries[h], preferred_element_type=F32)
            reads = rt[h]
            for j in range(4):
                reads = jnp.where(lane_index == 4 * i + j, read[128 * j:128 * j + 128, :], reads)
            rt[h] = reads
        return carry

    rt[...] = jnp.zeros(rt.shape, F32)
    lax.fori_loop(0, 4, read_part, 0)
    for k in range(1, 4):
        row_sum(k)
    total = rbuf[0, :, 2048:2176].astype(F32)
    for s in range(1, SIDE):
        total = total + rbuf[s, :, 2048:2176].astype(F32)
    gates_ref[...] = total + pltpu.roll(total, 120, 1)

    for load in late[2:]:
        load.wait()
    stab_new, carried, written = memory_gates(gates_ref[...], bias_ref[...], stab_ref[...])
    for h in range(4):
        query = rows_ref[:, head_cols(0, h)].astype(F32)
        key = rows_ref[:, head_cols(1, h)].astype(F32) * (128 ** (-0.5))
        value = rows_ref[:, head_cols(2, h)].astype(F32)
        match = jnp.sum(key * query, axis=1, keepdims=True) * written[:, h:h + 1]
        readout = carried[:, h:h + 1] * rt[h].T[0:ROWS, :] + match * value
        gate = jax.nn.sigmoid(rows_ref[:, head_cols(3, h)].astype(F32))
        scaled = rms_scale(readout, hgain_ref[:, head_cols(0, h)])
        gated_ref[:, head_cols(0, h)] = (scaled * gate).astype(BF16)

    gx[pl.ds(pl.multiple_of(ROWS * x, ROWS), ROWS), :] = gated_ref[...]

    def gx_copy(d):
        rows = pl.ds(pl.multiple_of(ROWS * x, ROWS), ROWS)
        peer = plane * SIDE + (x + d) % SIDE
        return remote(gated_ref, gx.at[rows, :], gx_send, gx_recv, (peer, core))

    for d in range(1, SIDE):
        gx_copy(d).start()
    stab_new_ref[...] = turned(stab_new)
    for h in range(4):
        key = rows_ref[:, head_cols(1, h)].astype(F32) * (128 ** (-0.5))
        carr_ref[h] = jnp.broadcast_to(carried[:, h:h + 1], (ROWS, 128))
        key = key * written[:, h:h + 1]
        top = key.astype(BF16).astype(F32)
        keys_ref[h] = jnp.concatenate([top, key - top], axis=0)
        value = rows_ref[:, head_cols(2, h)].astype(F32)
        vt_ref[h] = jnp.concatenate([value, value, jnp.zeros((96, 128), F32)], axis=0).T.astype(BF16)
    for axis in range(2):
        drain(mixv.at[pl.ds(0, 3), :, pl.ds(0, 16)], m_recv.at[2 + axis])
    drain(gx.at[pl.ds(0, 48), :], gx_recv)
    asend[...] = lax.dot_general(
        gx[...], mixv[...].reshape(512, 512), (((1,), (1,)), ((), ())), preferred_element_type=F32
    ).astype(BF16)

    def tb_copy(d, side):
        rows = pl.ds(pl.multiple_of(ROWS * ((x + d) % SIDE), ROWS), ROWS)
        peer = plane * SIDE + (x + d) % SIDE
        return remote(
            asend.at[rows, :], tb.at[core, x], tb_send, tb_recv,
            (peer, (core + side) % 2),
        )

    tb_list = [(0, 1)] + [(d, side) for d in (2, 1, 3) for side in (0, 1)]
    for d, side in tb_list:
        tb_copy(d, side).start()
    tb[core, x] = asend[pl.ds(pl.multiple_of(ROWS * x, ROWS), ROWS), :]
    tb_bytes = rx.at[pl.ds(0, 448), :]
    drain(tb_bytes, tb_recv)
    drain(twohalf, dx_recv.at[2])
    drain(twohalf, dx_recv.at[3])
    for k, (own, dst) in enumerate(((dg_ref, dgv), (du_ref, duv), (dd_ref, ddv))):
        for s in range(SIDE if k < 2 else 1):
            slot = dst.at[2 * ((x + s) % SIDE) + core]
            remote(own if s == 0 else slot, slot, d_send.at[k], d_recv.at[k], (chip, other)).start()
    attended = [tb[0, k].astype(F32) + tb[1, k].astype(F32) for k in range(SIDE)]
    lane = lax.broadcasted_iota(jnp.int32, (ROWS, 128), 1) // 32
    tiles = []
    for t in range(PLANE):
        tile = None
        for k in range(SIDE):
            part = attended[k][:, 128 * (t // 4):128 * (t // 4) + 128]
            shift = (32 * k - 32 * (t % 4)) % 128
            if shift:
                part = pltpu.roll(part, shift, 1)
            tile = part if tile is None else jnp.where(lane == k, part, tile)
        tiles.append(tile)
    residual = (tok_ref[...].astype(F32) + jnp.concatenate(tiles, axis=1)).astype(BF16)
    res[...] = residual
    normed = rms_scale(residual.astype(F32), gain_ref[...]).astype(BF16)
    ns[...] = normed
    def tile_rows(index):
        return pl.ds(pl.multiple_of(ROWS * index, ROWS), ROWS)

    parity = plane % 2

    own_row = y // 2
    low, high = pl.ds(0, 1024), pl.ds(1024, 1024)

    def acts_first(axis, d):
        peer = (along_z, along_y)[axis][d]
        cols = (low, high)[axis]
        return remote(
            ns.at[:, cols], da.at[z, own_row, :, cols], da_send.at[0], da_recv.at[axis], (peer, parity)
        )

    def acts_second(axis, d):
        peer = (along_z, along_y)[axis][d]
        block = da.at[z, :, :, high] if axis == 0 else da.at[:, own_row, :, low]
        return remote(block, block, da_send.at[1 + axis], da_recv.at[2 + axis], (peer, core))

    for axis in range(2):
        @pl.when(core == axis)
        def _():
            for d in (1, 0, 2):
                acts_first(axis, d).start()

    @pl.when(parity == core)
    def _():
        da[z, own_row] = ns[...]

    for b in range(8):
        cols = pl.ds(pl.multiple_of(1024 * core + 128 * b, 128), 128)
        n2[16 * b:16 * b + 16, :] = ns[:, cols]
    for k in range(4):
        obuf[256 * k:256 * k + 256, :] = jnp.dot(
            sel[256 * k:256 * k + 256, :], n2[...], preferred_element_type=F32
        ).astype(BF16)

    def x_copy(peer):
        return remote(
            obuf.at[tile_rows(peer), :], rx.at[tile_rows(chip), :], x_send, x_recv, (peer, core)
        )

    each_chip(plane, x, lambda peer: x_copy(peer).start())
    rx[tile_rows(chip), :] = obuf[tile_rows(chip), :]

    down_copy(0, x, None, right).wait_recv()
    down_copy(2, xl, 0, right).start()
    down_copy(1, x, None, left).wait_recv()
    down_copy(3, xr, 1, left).start()
    down_copy(4, xl, None, chip).start()
    down_copy(4, xr, None, chip).start()
    row_of = da.at[0, 0, :, low]

    @pl.when(parity == core)
    def _():
        drain(row_of, da_recv.at[1])
        drain(da.at[pl.ds(0, 3), 0, :, low], da_recv.at[0])
        for d in (1, 0, 2):
            acts_second(1, d).start()

    @pl.when(parity != core)
    def _():
        drain(da.at[pl.ds(0, 2), 0, :, low], da_recv.at[1])

    for d in (1, 0, 2):
        acts_second(0, d).start()

    drain(rx.at[pl.ds(0, 1008), :], x_recv)
    row = lax.broadcasted_iota(jnp.int32, (256, 256), 0)
    col = lax.broadcasted_iota(jnp.int32, (256, 256), 1)
    gather = (col == ((row % 32) // 2) * 16 + (row % 2) * 8 + row // 32).astype(F32).astype(BF16)
    scatter = (row == ((col % 32) // 2) * 16 + (col % 2) * 8 + col // 32).astype(F32).astype(BF16)
    for g in range(4):
        mixed_up = jnp.dot(gather, rx[256 * g:256 * g + 256, :], preferred_element_type=F32).astype(BF16)
        for b in range(8):
            xbuf[core, 32 * g:32 * g + 32, 128 * b:128 * b + 128] = mixed_up[32 * b:32 * b + 32, :]
    swap = remote(xbuf.at[core], xbuf.at[core], xo_send, xo_recv, (chip, other))
    swap.start()
    loads[0].wait()
    loads[1].wait()

    def expert_up_near(t, carry):
        cols = pl.ds(pl.multiple_of(256 * t, 256), 256)
        depth = pl.ds(pl.multiple_of(1024 * core, 1024), 1024)
        gacc[:, cols] = jnp.dot(xbuf[core], egv[depth, cols], preferred_element_type=F32)
        uacc[:, cols] = jnp.dot(xbuf[core], euv[depth, cols], preferred_element_type=F32)
        return carry

    def expert_up_far(t, carry):
        cols = pl.ds(pl.multiple_of(256 * t, 256), 256)
        depth = pl.ds(pl.multiple_of(1024 * other, 1024), 1024)
        gate_pre = gacc[:, cols] + jnp.dot(xbuf[other], egv[depth, cols], preferred_element_type=F32)
        up_pre = uacc[:, cols] + jnp.dot(xbuf[other], euv[depth, cols], preferred_element_type=F32)
        gate_clamped = jnp.minimum(gate_pre, clamp_limit)
        up_clamped = jnp.clip(up_pre, -clamp_limit, clamp_limit)
        hbuf[:, cols] = (
            (up_clamped + 1.0) * gate_clamped * jax.nn.sigmoid(sigmoid_slope * gate_clamped)
        ).astype(BF16)
        return carry

    lax.fori_loop(0, 4, expert_up_near, 0)
    for k, dst in enumerate((dgv, duv)):
        drain(dst.at[0], load_sem.at[3 + k])
        drain(dst.at[pl.ds(0, 4)], d_recv.at[k])

    @pl.when(parity == core)
    def _():
        drain(da.at[:, 0, :, low], da_recv.at[3])

    @pl.when(parity != core)
    def _():
        drain(da.at[:, :, :, low], da_recv.at[3])

    drain(da.at[pl.ds(0, 3), :, :, low], da_recv.at[2])

    down_copy(2, xa, 0, right).wait_recv()
    down_copy(3, xa, 1, left).wait_recv()
    down_copy(4, xa, None, chip).start()
    dense_rows = da[...].reshape(128, 2048)
    over_last = (((1,), (1,)), ((), ()))
    gate_rows = lax.dot_general(dense_rows, dgv[...].reshape(256, 2048), over_last, preferred_element_type=F32)
    lift_rows = lax.dot_general(dense_rows, duv[...].reshape(256, 2048), over_last, preferred_element_type=F32)
    activity = (gate_rows / (1.0 + jnp.exp(-gate_rows)) * lift_rows).astype(BF16)
    drain(ddv.at[0], load_sem.at[5])
    drain(ddv.at[pl.ds(0, 4)], d_recv.at[2])
    down = ddv[...].reshape(256, 2048)
    for h in range(2):
        for t in range(2):
            lower = 1024 * h + 512 * t
            part = jnp.dot(activity, down[:, lower:lower + 512], preferred_element_type=F32).astype(BF16)
            dout[h, :, :, :, 512 * t:512 * t + 512] = part.reshape(SIDE, 2, ROWS, 512)

    for d in range(3):
        zt = (z + d + 1) % SIDE
        remote(dout.at[0, zt], zsum.at[z], rp_send.at[0], rp_recv.at[0], (along_z[d], core)).start()
    zsum[z] = dout[0, z]
    for i in range(2):
        yt = 2 * i + core
        target = (z * SIDE + yt) * SIDE + x

        @pl.when(yt != y)
        def _():
            remote(dout.at[1, :, i], ysum.at[y], rp_send.at[1], rp_recv.at[1], (target, core)).start()

        @pl.when(yt == y)
        def _():
            ysum[y] = dout[1, :, i]

    swap.wait_recv()
    lax.fori_loop(0, 4, expert_up_far, 0)
    loads[2].wait()

    def y_copy(t):
        return remote(ysend.at[t], yrecv.at[t], y_send, y_recv, (chip, other))

    def expert_down_far(t, carry):
        cols = pl.ds(pl.multiple_of(1024 * other + 256 * t, 256), 256)
        ysend[t] = jnp.dot(hbuf[...], edv[:, cols], preferred_element_type=F32).astype(BF16)
        y_copy(t).start()
        return carry

    def expert_down_near(t, carry):
        cols = pl.ds(pl.multiple_of(1024 * core + 256 * t, 256), 256)
        yown[t] = jnp.dot(hbuf[...], edv[:, cols], preferred_element_type=F32).astype(BF16)
        return carry

    lax.fori_loop(0, 4, expert_down_far, 0)
    lax.fori_loop(0, 4, expert_down_near, 0)

    drain(yrecv, y_recv)
    for g in range(4):
        rows = slice(32 * g, 32 * g + 32)
        stacked = []
        for t in range(4):
            both = (yown[t, rows, :].astype(F32) + yrecv[t, rows, :].astype(F32)).astype(BF16)
            stacked += [both[:, :128], both[:, 128:]]
        yret[256 * g:256 * g + 256, :] = jnp.dot(
            scatter, jnp.concatenate(stacked, axis=0), preferred_element_type=F32
        ).astype(BF16)

    def q_copy(peer):
        return remote(
            yret.at[tile_rows(peer), :], rret.at[tile_rows(chip), :], q_send, q_recv, (peer, core)
        )

    each_chip(plane, x, lambda peer: q_copy(peer).start())
    rret[tile_rows(chip), :] = yret[tile_rows(chip), :]

    drain(zsum.at[pl.ds(0, 3)], rp_recv.at[0])
    for i in range(2):
        total = zsum[0, i].astype(F32)
        for s in range(1, SIDE):
            total = total + zsum[s, i].astype(F32)
        zout[i] = total.astype(BF16)
    for i in range(2):
        yt = 2 * i + core
        target = (z * SIDE + yt) * SIDE + x

        @pl.when((yt != y) | (core != 0))
        def _():
            remote(zout.at[i], dr.at[y], dr_send.at[0], dr_recv, (target, 0)).start()

        @pl.when((yt == y) & (core == 0))
        def _():
            dr[y] = zout[i]

    @pl.when(parity == core)
    def _():
        drain(ysum.at[pl.ds(0, 3)], rp_recv.at[1])
        for t in range(SIDE):
            total = ysum[0, t].astype(F32)
            for s in range(1, SIDE):
                total = total + ysum[s, t].astype(F32)
            yout[t] = total.astype(BF16)
        for d in range(3):
            zt = (z + d + 1) % SIDE
            remote(yout.at[zt], dr.at[z], dr_send.at[1], dr_recv, (along_z[d], 1)).start()

        @pl.when(core == 0)
        def _():
            remote(yout.at[z], dr.at[z], dr_send.at[1], dr_recv, (chip, 1)).start()

        @pl.when(core != 0)
        def _():
            dr[z] = yout[z]

    @pl.when(parity == core)
    def _():
        drain(dr.at[pl.ds(0, 3)], dr_recv)

    @pl.when(parity != core)
    def _():
        drain(dr, dr_recv)

    branch = dr[0].astype(F32)
    for s in range(1, SIDE):
        branch = branch + dr[s].astype(F32)

    drain(rret.at[pl.ds(0, 1008), :], q_recv)
    returned = rret[...]
    routed = jnp.dot(comb_hi[...], returned, preferred_element_type=F32) + jnp.dot(
        comb_lo[...], returned, preferred_element_type=F32
    )
    routed = jnp.concatenate([routed[16 * b:16 * b + 16, :] for b in range(8)], axis=1)
    own_cols = pl.ds(pl.multiple_of(1024 * core, 1024), 1024)
    out_ref[...] = (res[:, own_cols].astype(F32) + routed + branch * scale_ref[:, own_cols]).astype(BF16)

    drain(gx.at[pl.ds(0, 48), :], gx_send)
    drain(tb_bytes, tb_send)
    drain(rx.at[pl.ds(0, 1008), :], x_send)
    drain(rret.at[pl.ds(0, 1008), :], q_send)
    drain(yrecv, y_send)
    drain(xbuf.at[0], xo_send)
    for k, dst in enumerate((dgv, duv, ddv)):
        drain(dst.at[pl.ds(0, 4)], d_send.at[k])
    drain(ddv.at[pl.ds(0, 3)], down_send)

    drain(da.at[pl.ds(0, 3), 0, :, low], da_send.at[0])
    drain(da.at[pl.ds(0, 3), :, :, low], da_send.at[1])

    @pl.when(parity == core)
    def _():
        drain(da.at[pl.ds(0, 3)], da_send.at[2])

    drain(zsum.at[pl.ds(0, 3)], rp_send.at[0])

    @pl.when(parity == core)
    def _():
        drain(ysum.at[0], rp_send.at[1])

        @pl.when(core == 0)
        def _():
            drain(dr.at[0], dr_send.at[0])
            drain(dr, dr_send.at[1])

        @pl.when(core != 0)
        def _():
            drain(dr.at[pl.ds(0, 2)], dr_send.at[0])
            drain(dr.at[pl.ds(0, 3)], dr_send.at[1])

    @pl.when(parity != core)
    def _():
        drain(ysum.at[pl.ds(0, 2)], rp_send.at[1])
        drain(dr.at[pl.ds(0, 2)], dr_send.at[0])
    drain(wbuf.at[pl.ds(0, 96), :], w_send)
    drain(gbuf.at[pl.ds(0, 3)], g_send)
    drain(abuf.at[pl.ds(0, 240), :], a_send)
    drain(mixv.at[pl.ds(0, 3), :, :], m_send)
    drain(mixv.at[0, pl.ds(0, 3)], m_send)
    drain(sbuf.at[pl.ds(0, 3)], p_send)
    drain(rbuf.at[pl.ds(0, 3)], r_send)
    for k in range(2):
        drain(dense[k][1].at[pl.ds(0, 3)], dx_send.at[k])


def decode_step(*operands):
    dma = pltpu.SemaphoreType.DMA
    vm = pltpu.VMEM
    return pl.pallas_call(
        step_kernel,
        out_shape=(
            jax.ShapeDtypeStruct((ROWS, 1024), BF16),
            jax.ShapeDtypeStruct((4, ROWS, 128), F32),
            jax.ShapeDtypeStruct((4, 32, 128), F32),
            jax.ShapeDtypeStruct((4, 128, 128), BF16),
            jax.ShapeDtypeStruct((4, ROWS), F32),
        ),
        in_specs=[ANY_SPEC] * 23,
        out_specs=(VMEM_SPEC,) * 5,
        scratch_shapes=[
            vm((1, 2048), F32), vm((4, 32), BF16), vm((4, 32), BF16), vm((128, 2048), BF16), vm((4, 8, 128), F32),
            vm((ROWS, 2048), BF16), vm((256, 128), BF16),
            vm((SIDE, SIDE, ROWS, 2176), BF16), vm((SIDE, SIDE, ROWS, 2176), BF16),
            vm((SIDE, ROWS, 2176), BF16), vm((SIDE, ROWS, 2176), BF16),
            vm((ROWS, 4, 128, 128), F32), vm((ROWS, 2048), BF16), vm((ROWS, 128), F32), vm((1, 4), F32),
            vm((4, ROWS), F32), vm((1, 512), F32), vm((4, 128, 128), F32), vm((4, 256, 128), BF16),
            vm((ROWS, 512), BF16), vm((ROWS, 2048), BF16), vm((1, 2048), F32),
            vm((4, ROWS), jnp.int32), vm((4, ROWS), F32), vm((1, 2048), F32),
            vm((2048, 1024), BF16), vm((2048, 1024), BF16), vm((1024, 2048), BF16),
            vm((8, 32, 2048), BF16), vm((8, 32, 2048), BF16), vm((8, 32, 2048), BF16),
            vm((SIDE, SIDE, 32, 512), BF16),
            vm((64, 512), BF16), vm((64, 512), BF16), vm((2, 4, ROWS, 512), BF16),
            vm((ROWS, 2048), BF16), vm((ROWS, 2048), BF16), vm((128, 128), BF16),
            vm((1024, 128), BF16), vm((128, 1024), BF16), vm((128, 1024), BF16),
            vm((1024, 128), BF16), vm((1024, 128), BF16), vm((2, 128, 1024), BF16),
            vm((128, 1024), F32), vm((128, 1024), F32), vm((128, 1024), BF16),
            vm((4, 128, 256), BF16), vm((4, 128, 256), BF16), vm((4, 128, 256), BF16),
            vm((1024, 128), BF16), vm((1024, 128), BF16),
            vm((SIDE, 2, ROWS, 2048), BF16), vm((2, SIDE, 2, ROWS, 1024), BF16), vm((SIDE, ROWS, 1024), BF16),
            vm((SIDE, 2, ROWS, 1024), BF16), vm((SIDE, SIDE, ROWS, 1024), BF16),
            vm((2, ROWS, 1024), BF16), vm((SIDE, ROWS, 1024), BF16),
            dma((6,)),
            dma, dma((4, 4)),
            dma, dma,
            dma, dma,
            dma, dma((4,)),
            dma, dma((4,)),
            dma, dma((4,)),
            dma((2,)), dma((4,)),
            pltpu.SemaphoreType.REGULAR, dma((7,)),
            dma((6,)),
            dma, dma,
            dma, dma,
            dma, dma,
            dma((3,)), dma((4,)),
            dma, dma,
            dma, dma,
            dma((2,)), dma,
            dma, dma,
            dma((3,)), dma((3,)),
            dma((4,)),
            dma, dma((4,)),
            dma((2,)), dma((2,)),
        ],
        compiler_params=pltpu.CompilerParams(
            collective_id=0, has_side_effects=True, vmem_limit_bytes=VMEM_LIMIT
        ),
        name="decode_step",
    )(*operands)


def body(
    tokens, norm_gain, query_weight, key_weight, value_weight, outgate_weight, input_weight, forget_weight,
    forget_bias, memory, stabilizer, head_gain, mix_weight, second_gain, route_experts, route_weight,
    expert_gate, expert_up, expert_down, dense_gate, dense_up, dense_down, branch_scale,
):
    mixed, carried, keys, values, stab_new = decode_step(
        tokens, norm_gain.reshape(1, -1), query_weight, key_weight, value_weight, outgate_weight,
        input_weight.T, forget_weight.T, mix_weight.T, dense_gate, dense_up, dense_down,
        memory, forget_bias.reshape(1, -1), stabilizer.T, head_gain.reshape(1, -1), second_gain.reshape(1, -1),
        route_experts.T, route_weight.T, expert_gate, expert_up, expert_down, branch_scale.reshape(1, -1),
    )
    memory_new, stab_new, mixed = memory_update(carried, keys, values, stab_new, memory, mixed)
    return mixed, memory_new, stab_new.T


def solution(mesh):
    in_specs = (
        P("ep", None), P(),
        P("ep", "tp"), P("ep", "tp"), P("ep", "tp"), P("ep", "tp"), P("ep", "tp"), P("ep", "tp"),
        P("tp"), P("ep", "tp", None, None), P("ep", "tp"), P("tp"), P("tp", "ep"), P(),
        P("ep", None), P("ep", None),
        P("ep", None, "tp"), P("ep", None, "tp"), P("ep", "tp", None),
        P(("ep", "tp"), None), P(("ep", "tp"), None), P(("ep", "tp"), None), P(),
    )
    out_specs = (P("ep", "tp"), P("ep", "tp", None, None), P("ep", "tp"))
    return jax.shard_map(body, mesh=mesh, in_specs=in_specs, out_specs=out_specs, check_vma=False)
```
